32 devices in a mesh: sp: 8 (over z, x), tp: 4 (over y, core).
Axes of the slice: x: 2, y: 2, z: 4, core: 2. Of those that a mesh axis runs over, the one named last changes fastest.
Arguments:
- residual: bfloat16 [2048, 2048], P(('sp', 'tp')), may hold values from -6 to 6
- query_wide: bfloat16 [2048, 512], P('sp', 'tp'), may hold values from -8 to 8
- key_wide: bfloat16 [2048, 512], P('sp', 'tp'), may hold values from -8 to 8
- value_wide: bfloat16 [2048, 512], P('sp', 'tp'), may hold values from -6 to 6
- query_narrow: bfloat16 [2048, 512], P('sp', 'tp'), may hold values from -8 to 8
- key_narrow: bfloat16 [2048, 512], P('sp', 'tp'), may hold values from -8 to 8
- value_narrow: bfloat16 [2048, 512], P('sp', 'tp'), may hold values from -6 to 6
- gate_wide: float32 [2048, 4], P('sp', 'tp'), may hold values from -2 to 20
- gate_narrow: float32 [2048, 8], P('sp', 'tp'), may hold values from -2 to 20
- out_wide: bfloat16 [512, 2048], replicated, may hold values from -0.1875 to 0.1875
- out_narrow: bfloat16 [512, 2048], replicated, may hold values from -0.1875 to 0.1875
- norm_gain: float32 [2048], replicated, may hold values from 0.1 to 1.9
- routing: int32 [2048, 2], P(('sp', 'tp')), may hold values from 0 to 7, as said below
- route_weight: float32 [2048, 2], P(('sp', 'tp')), may hold values from 0.3 to 1.5
- gate_weight: bfloat16 [8, 2048, 1024], P('sp', None, 'tp'), may hold values from -0.125 to 0.125
- up_weight: bfloat16 [8, 2048, 1024], P('sp', None, 'tp'), may hold values from -0.125 to 0.125
- down_weight: bfloat16 [8, 1024, 2048], P('sp', 'tp'), may hold values from -0.1875 to 0.1875
Outputs:
- result: bfloat16 [2048, 2048], P(('sp', 'tp'))
The draws below stay inside these ranges and needn't reach their ends.
Inputs may be any that keep to these rules, and one draw needn't show every extreme that they name: `routing`: each row names 2 different experts of one group (experts g * 2 to g * 2 + 1). In each aligned block of 64 rows (the rows of one device) no expert is named by more than 32 rows; one group, the same for all blocks, has each of its experts named by exactly 32 rows of every block.
All inputs are finite; a program needn't handle non-finite values.
Results may differ from the reference program's by a relative error of at most 0.017.
Values may be sent and summed in bfloat16 or wider, within the bound.
A program may use at most 128 MiB of HBM per device.

```python
import math
import jax
import jax.numpy as jnp
from jax import lax

D = 2048
WIDE = 4
HW = 128
NARROW = 8
HN = 64
FFE = 1024
GROUPS = 4
TOP = 2
TOK_DEV = 256
TOKENS = 2048
EXPERTS = 8
EPG = 2
ROWS_DEV = 64
CAP = 32
N_TP = 4


def projected(key, breadth, salt_value):
    values = 1.7 * jax.random.normal(jax.random.fold_in(key, salt_value), (TOKENS, breadth), jnp.float32)
    values = jnp.clip(values, -8.0, 8.0)
    return values.astype(jnp.bfloat16)


def forget(key, head_count, salt_value):
    seeded = jax.random.fold_in(key, salt_value)
    order_key, drift_key, jitter_key = jax.random.split(seeded, 3)
    ranking = jax.random.permutation(order_key, head_count)
    keeping = head_count // 2
    baseline = jnp.where(ranking < keeping, jnp.log(1.0 * TOKENS), jnp.log(40.0))
    shards = TOKENS // TOK_DEV
    drift_part = jax.random.uniform(drift_key, (shards, 1, head_count), jnp.float32, -0.8, 0.8)
    drift_part = jnp.broadcast_to(drift_part, (shards, TOK_DEV, head_count)).reshape(TOKENS, head_count)
    jitter = jnp.clip(jax.random.normal(jitter_key, (TOKENS, head_count), jnp.float32), -4.0, 4.0)
    return (baseline[None, :] + drift_part + jitter).astype(jnp.float32)


def draw_query_wide(key, part):
    return projected(key, WIDE * HW, 11)


def draw_key_wide(key, part):
    return projected(key, WIDE * HW, 12)


def draw_query_narrow(key, part):
    return projected(key, NARROW * HN, 21)


def draw_key_narrow(key, part):
    return projected(key, NARROW * HN, 22)


def draw_gate_wide(key, part):
    return forget(key, WIDE, 31)


def draw_gate_narrow(key, part):
    return forget(key, NARROW, 32)


def route_block(key, full_group):
    cut_key, label_key, row_key = jax.random.split(key, 3)
    half_rows = ROWS_DEV // 2
    ordinal = jnp.arange(ROWS_DEV, dtype=jnp.int32)
    cut_points = jnp.sort(jax.random.randint(cut_key, (GROUPS - 2,), 0, half_rows + 1))
    remainder = ordinal - half_rows
    other_group = jnp.sum((remainder[:, None] >= cut_points[None, :]).astype(jnp.int32), axis=1)
    group_starts = jnp.concatenate([jnp.zeros((1,), jnp.int32), cut_points.astype(jnp.int32)])
    in_full = ordinal < half_rows
    ranking = jnp.where(in_full, ordinal, remainder - group_starts[other_group])
    chosen_group = jnp.where(in_full, full_group, (full_group + 1 + other_group) % GROUPS)

    def labels_of(group_number):
        return jax.random.permutation(jax.random.fold_in(label_key, group_number), EPG)
    labels = jax.vmap(labels_of)(jnp.arange(GROUPS, dtype=jnp.int32))
    slot_number = TOP * ranking[:, None] + jnp.arange(TOP, dtype=jnp.int32)[None, :]
    local_expert = labels[chosen_group[:, None], slot_number % EPG]
    expert_ids = (chosen_group[:, None] * EPG + local_expert).astype(jnp.int32)
    shuffled = jax.random.permutation(row_key, ROWS_DEV)
    return jnp.zeros((ROWS_DEV, TOP), jnp.int32).at[shuffled].set(expert_ids)


def draw_routing(key, part):
    seeded = jax.random.fold_in(key, 4242)
    full_group = jax.random.randint(jax.random.fold_in(seeded, 1), (), 0, GROUPS)

    def one_block(block_number):
        return route_block(jax.random.fold_in(seeded, block_number + 2), full_group)
    blocks = jax.vmap(one_block)(jnp.arange(TOKENS // ROWS_DEV, dtype=jnp.int32))
    return blocks.reshape(TOKENS, TOP)


def block_scale(own_key, dims, cuts, low, largest):
    loudness, own = 1.0, jax.random.fold_in(own_key, 6)
    for axis_at, shards_of in cuts:
        heights = jnp.exp(jax.random.uniform(jax.random.fold_in(own, axis_at), (shards_of,), jnp.float32, low / len(cuts), largest / len(cuts)))
        loudness = loudness * jnp.repeat(heights, dims[axis_at] // shards_of).reshape([-1 if axis == axis_at else 1 for axis in range(len(dims))])
    return loudness


def bell_draw(stream_key, shape, scale, most, cuts=(), kind=jnp.bfloat16):
    array = jax.random.normal(stream_key, shape, jnp.float32) * scale
    if len(cuts) > 0:
        array = block_scale(stream_key, shape, cuts, -0.22, 0.18) * array
    return jnp.clip(array, min=-most, max=most).astype(kind)


def setup_inputs(seed: int = 0) -> dict:
    key_list = jax.random.split(jax.random.key(seed), 18)
    return {
        "residual": bell_draw(key_list[0], (TOKENS, D), 1.0, 6.0, ((0, 32),)),
        "query_wide": draw_query_wide(jax.random.fold_in(key_list[17], 71), 0),
        "key_wide": draw_key_wide(jax.random.fold_in(key_list[17], 71), 0),
        "value_wide": bell_draw(key_list[3], (TOKENS, WIDE * HW), 1.0, 6.0, ((0, 8), (1, 4))),
        "query_narrow": draw_query_narrow(jax.random.fold_in(key_list[17], 71), 0),
        "key_narrow": draw_key_narrow(jax.random.fold_in(key_list[17], 71), 0),
        "value_narrow": bell_draw(key_list[6], (TOKENS, NARROW * HN), 1.0, 6.0, ((0, 8), (1, 4))),
        "gate_wide": draw_gate_wide(jax.random.fold_in(key_list[17], 71), 0),
        "gate_narrow": draw_gate_narrow(jax.random.fold_in(key_list[17], 71), 0),
        "out_wide": bell_draw(key_list[9], (WIDE * HW, D), (WIDE * HW + NARROW * HN) ** -0.5, 0.1875),
        "out_narrow": bell_draw(key_list[10], (NARROW * HN, D), (WIDE * HW + NARROW * HN) ** -0.5, 0.1875),
        "norm_gain": jnp.clip(1.0 + 0.18 * jax.random.normal(key_list[11], (D,), jnp.float32), 0.1, 1.9),
        "routing": draw_routing(jax.random.fold_in(key_list[17], 71), 0),
        "route_weight": jnp.clip(jnp.exp(math.log(1.5) - 1.60943787 * jax.random.uniform(key_list[13], (TOKENS, TOP), jnp.float32) ** block_scale(key_list[13], (TOKENS, TOP), ((0, 32),), -0.2, 0.2)), 0.3, 1.5),
        "gate_weight": bell_draw(key_list[14], (EXPERTS, D, FFE), D ** -0.5, 0.125, ((0, 8), (2, 4))),
        "up_weight": bell_draw(key_list[15], (EXPERTS, D, FFE), D ** -0.5, 0.125, ((0, 8), (2, 4))),
        "down_weight": bell_draw(key_list[16], (EXPERTS, FFE, D), FFE ** -0.5, 0.1875, ((0, 8), (1, 4))),
    }


epsilon = 1e-06

def attend(queries, keys, values, gates, head_width):
    length = queries.shape[0]
    head_count = gates.shape[1]
    decay = jnp.cumsum(jax.nn.log_sigmoid(gates.astype(jnp.float32)), axis=0)
    grid_query = queries.reshape(length, head_count, head_width).astype(jnp.float32)
    grid_key = keys.reshape(length, head_count, head_width).astype(jnp.float32)
    grid_value = values.reshape(length, head_count, head_width).astype(jnp.float32)
    block_size = math.gcd(length, 512)
    key_place = jnp.arange(length, dtype=jnp.int32)

    def one_block(position):
        begin = (position * block_size).astype(jnp.int32)
        part_query = lax.dynamic_slice_in_dim(grid_query, begin, block_size, 0)
        part_decay = lax.dynamic_slice_in_dim(decay, begin, block_size, 0)
        scores = jnp.einsum('thd,phd->htp', part_query, grid_key) * head_width ** (-0.5)
        scores = scores + part_decay.T[:, :, None] - decay.T[:, None, :]
        query_place = begin + jnp.arange(block_size, dtype=jnp.int32)
        scores = jnp.where(key_place[None, None, :] <= query_place[None, :, None], scores, -jnp.inf)
        weights = jnp.exp(scores - lax.optimization_barrier(jnp.max(scores, axis=2, keepdims=True)))
        weight_sum = lax.optimization_barrier(jnp.sum(weights, axis=2))
        rounded = lax.optimization_barrier(weights.astype(jnp.bfloat16)).astype(jnp.float32)
        mixed_heads = jnp.einsum('htp,phd->htd', rounded, grid_value) / weight_sum[:, :, None]
        return jnp.transpose(mixed_heads, (1, 0, 2)).reshape(block_size, head_count * head_width).astype(jnp.bfloat16)
    blocks = lax.map(one_block, jnp.arange(length // block_size, dtype=jnp.int32))
    return blocks.reshape(length, head_count * head_width)

def experts_apply(normed, routing, route_weight, gate_weight, up_weight, down_weight):
    length = normed.shape[0]
    chosen_count = routing.shape[1]
    expert_count = gate_weight.shape[0]
    flat_routes = routing.reshape(-1).astype(jnp.int32)
    matches = (flat_routes[:, None] == jnp.arange(expert_count, dtype=jnp.int32)[None, :]).astype(jnp.int32)
    ranking = lax.optimization_barrier(jnp.sum((jnp.cumsum(matches, axis=0) - matches) * matches, axis=1)).astype(jnp.int32)
    capacity_all = length // ROWS_DEV * CAP
    lookup = jnp.full((expert_count, capacity_all), length * chosen_count, jnp.int32)
    lookup = lookup.at[flat_routes, ranking].set(jnp.arange(length * chosen_count, dtype=jnp.int32))
    flat_weights = route_weight.reshape(-1)

    def one_expert(carried, pieces):
        copies, gate_part, up_part, down_part = pieces
        positions = (copies // chosen_count).astype(jnp.int32)
        chosen_rows = jnp.take(normed, positions, axis=0, mode='clip')
        gate_value = jnp.dot(chosen_rows, gate_part, preferred_element_type=jnp.float32)
        up_value = jnp.dot(chosen_rows, up_part, preferred_element_type=jnp.float32)
        hidden = (jax.nn.silu(gate_value) * up_value).astype(jnp.bfloat16)
        hidden_blocks = hidden.reshape(capacity_all, N_TP, -1).astype(jnp.float32)
        down_blocks = down_part.reshape(N_TP, -1, down_part.shape[1]).astype(jnp.float32)
        partial_out = jnp.einsum('lnf,nfd->nld', hidden_blocks, down_blocks)
        partial_out = lax.optimization_barrier(partial_out.astype(jnp.bfloat16)).astype(jnp.float32)
        expert_out = lax.optimization_barrier(jnp.sum(partial_out, axis=0)).astype(jnp.bfloat16)
        scale = jnp.take(flat_weights, copies, mode='fill', fill_value=0.0)
        carried = carried.at[positions].add(scale[:, None] * expert_out.astype(jnp.float32), mode='drop')
        return (carried, None)
    start = jnp.zeros((length, normed.shape[1]), jnp.float32)
    total, _ = lax.scan(one_expert, start, (lookup, gate_weight, up_weight, down_weight))
    return total

def reference(residual, query_wide, key_wide, value_wide, query_narrow, key_narrow, value_narrow, gate_wide, gate_narrow, out_wide, out_narrow, norm_gain, routing, route_weight, gate_weight, up_weight, down_weight):
    att_wide = attend(query_wide, key_wide, value_wide, gate_wide, HW)
    att_narrow = attend(query_narrow, key_narrow, value_narrow, gate_narrow, HN)
    mixed = jnp.dot(att_wide, out_wide, preferred_element_type=jnp.float32)
    mixed = mixed + jnp.dot(att_narrow, out_narrow, preferred_element_type=jnp.float32)
    middle = (residual.astype(jnp.float32) + mixed).astype(jnp.bfloat16)
    middle_wide = middle.astype(jnp.float32)
    spread = lax.optimization_barrier(jnp.mean(middle_wide * middle_wide, axis=1, keepdims=True))
    normed = (middle_wide * lax.rsqrt(spread + epsilon) * norm_gain).astype(jnp.bfloat16)
    routed = experts_apply(normed, routing, route_weight, gate_weight, up_weight, down_weight)
    return (middle_wide + routed).astype(jnp.bfloat16)
```

```python
import functools
import math

import jax
import jax.numpy as jnp
from jax import lax
from jax.experimental import pallas as pl
from jax.experimental.pallas import tpu as pltpu
from jax.sharding import PartitionSpec as P

HW = 128
HN = 64
GROUPS = 4


epsilon = 1e-06


def globalize(pieces, shard_rows):
    shards = pieces.shape[0] // shard_rows
    grid = pieces.reshape(shards, shard_rows, pieces.shape[1])
    endings = grid[:, -1, :]
    offsets = jnp.cumsum(endings, axis=0) - endings
    return (grid + offsets[:, None, :]).reshape(pieces.shape)


def head_block(
    state, queries, query_decay, keys, values, key_decay, first_key, first_query, head_width
):
    highest_old, weight_sum, weighted = state
    query_rows = queries.shape[0]
    head_count = query_decay.shape[1]
    key_rows = keys.shape[0]
    grid_query = queries.reshape(query_rows, head_count, head_width)
    grid_key = keys.reshape(key_rows, head_count, head_width)
    grid_value = values.reshape(key_rows, head_count, head_width)
    scores = jnp.einsum("thd,phd->htp", grid_query, grid_key, preferred_element_type=jnp.float32)
    scores = scores * head_width ** (-0.5) + query_decay.T[:, :, None] - key_decay.T[:, None, :]
    query_place = first_query + jnp.arange(query_rows, dtype=jnp.int32)
    key_place = first_key + jnp.arange(key_rows, dtype=jnp.int32)
    scores = jnp.where(key_place[None, None, :] <= query_place[None, :, None], scores, -jnp.inf)
    highest = jnp.maximum(highest_old, jnp.max(scores, axis=2))
    weights = jnp.exp(scores - highest[:, :, None])
    shrink = jnp.exp(highest_old - highest)
    weight_sum = weight_sum * shrink + jnp.sum(weights, axis=2)
    product = jnp.einsum(
        "htp,phd->htd", weights.astype(jnp.bfloat16), grid_value, preferred_element_type=jnp.float32
    )
    weighted = weighted * shrink[:, :, None] + product
    return (highest, weight_sum, weighted)


def fresh_state(head_count, shard_rows, head_width):
    return (
        jnp.full((head_count, shard_rows), -1e30, jnp.float32),
        jnp.zeros((head_count, shard_rows), jnp.float32),
        jnp.zeros((head_count, shard_rows, head_width), jnp.float32),
    )


def finish(state, shard_rows):
    highest, weight_sum, weighted = state
    mixed_heads = weighted / weight_sum[:, :, None]
    joined = jnp.transpose(mixed_heads, (1, 0, 2))
    return joined.reshape(shard_rows, weighted.shape[0] * weighted.shape[2]).astype(jnp.bfloat16)


def body(
    residual,
    query_wide,
    key_wide,
    value_wide,
    query_narrow,
    key_narrow,
    value_narrow,
    gate_wide,
    gate_narrow,
    out_wide,
    out_narrow,
    norm_gain,
    routing,
    route_weight,
    gate_weight,
    up_weight,
    down_weight,
):
    shard_rows = query_wide.shape[0]
    half_rows = shard_rows // 2
    sp_place = lax.axis_index("sp")
    first_query = sp_place * shard_rows
    running_wide = jnp.cumsum(jax.nn.log_sigmoid(gate_wide), axis=0)
    running_narrow = jnp.cumsum(jax.nn.log_sigmoid(gate_narrow), axis=0)
    pieces_wide, pieces_narrow = (
        lax.all_gather(running_wide, "sp", axis=0, tiled=True),
        lax.all_gather(running_narrow, "sp", axis=0, tiled=True),
    )
    every_wide = globalize(pieces_wide, shard_rows)
    every_narrow = globalize(pieces_narrow, shard_rows)
    late_first = first_query + half_rows
    halves = []
    for place, part_wide, part_narrow in (
        (first_query, query_wide[:half_rows], query_narrow[:half_rows]),
        (late_first, query_wide[half_rows:], query_narrow[half_rows:]),
    ):
        halves.append(
            (
                place,
                part_wide,
                part_narrow,
                lax.dynamic_slice_in_dim(every_wide, place, half_rows, 0),
                lax.dynamic_slice_in_dim(every_narrow, place, half_rows, 0),
            )
        )

    def half_state():
        return (
            fresh_state(gate_wide.shape[1], half_rows, HW),
            fresh_state(gate_narrow.shape[1], half_rows, HN),
        )

    state = (half_state(), half_state())
    keys_wide = lax.all_gather(key_wide, "sp", axis=0, tiled=True)
    values_wide = lax.all_gather(value_wide, "sp", axis=0, tiled=True)
    keys_narrow = lax.all_gather(key_narrow, "sp", axis=0, tiled=True)
    values_narrow = lax.all_gather(value_narrow, "sp", axis=0, tiled=True)
    span_rows = keys_wide.shape[0]
    block_size = math.gcd(span_rows, 2048)

    def visit(carried, position):
        inside = position * block_size

        def take_block(source):
            return lax.dynamic_slice_in_dim(source, inside, block_size, 0)

        def take_decay(source):
            return lax.dynamic_slice_in_dim(source, inside, block_size, 0)

        block_kw = take_block(keys_wide)
        block_vw = take_block(values_wide)
        block_kn = take_block(keys_narrow)
        block_vn = take_block(values_narrow)
        block_dw = take_decay(every_wide)
        block_dn = take_decay(every_narrow)

        def one_half(current, half):
            place, part_wide, part_narrow, query_decay_wide, query_decay_narrow = half

            def work(inner):
                first = head_block(
                    inner[0],
                    part_wide,
                    query_decay_wide,
                    block_kw,
                    block_vw,
                    block_dw,
                    inside,
                    place,
                    HW,
                )
                second = head_block(
                    inner[1],
                    part_narrow,
                    query_decay_narrow,
                    block_kn,
                    block_vn,
                    block_dn,
                    inside,
                    place,
                    HN,
                )
                return (first, second)

            def skip(inner):
                return inner

            return lax.cond(inside <= place + half_rows - 1, work, skip, current)

        updated = (one_half(carried[0], halves[0]), one_half(carried[1], halves[1]))
        return (updated, None)

    state, _ = lax.scan(visit, state, jnp.arange(span_rows // block_size, dtype=jnp.int32))
    att_wide = jnp.concatenate(
        [finish(state[0][0], half_rows), finish(state[1][0], half_rows)], axis=0
    )
    att_narrow = jnp.concatenate(
        [finish(state[0][1], half_rows), finish(state[1][1], half_rows)], axis=0
    )
    own_rows = residual.shape[0]
    tp_place = lax.axis_index("tp")
    rows_wide = lax.dynamic_slice_in_dim(
        out_wide, tp_place * att_wide.shape[1], att_wide.shape[1], 0
    )
    rows_narrow = lax.dynamic_slice_in_dim(
        out_narrow, tp_place * att_narrow.shape[1], att_narrow.shape[1], 0
    )
    first = jnp.dot(att_wide, rows_wide, preferred_element_type=jnp.float32)
    second = jnp.dot(att_narrow, rows_narrow, preferred_element_type=jnp.float32)
    mixed = lax.psum_scatter(
        (first + second).astype(jnp.bfloat16), "tp", scatter_dimension=0, tiled=True
    ).astype(jnp.float32)
    middle = (residual.astype(jnp.float32) + mixed).astype(jnp.bfloat16)
    middle_wide = middle.astype(jnp.float32)
    spread = jnp.mean(middle_wide * middle_wide, axis=1, keepdims=True)
    normed = (middle_wide * lax.rsqrt(spread + epsilon) * norm_gain).astype(jnp.bfloat16)
    features = normed.shape[1]
    chosen_count = routing.shape[1]
    expert_count = gate_weight.shape[0] * lax.axis_size("sp")
    capacity = own_rows * GROUPS // expert_count
    flat_routes = routing.reshape(-1)
    matches = (flat_routes[:, None] == jnp.arange(expert_count, dtype=jnp.int32)[None, :]).astype(
        jnp.int32
    )
    ranking = jnp.sum((jnp.cumsum(matches, axis=0) - matches) * matches, axis=1)
    placing = flat_routes * capacity + ranking
    picker = (
        placing[None, :] == jnp.arange(expert_count * capacity, dtype=jnp.int32)[:, None]
    ).astype(jnp.bfloat16)
    picker = jnp.sum(picker.reshape(expert_count * capacity, own_rows, chosen_count), axis=2)
    outgoing = jnp.dot(picker, normed, preferred_element_type=jnp.float32).astype(jnp.bfloat16)
    outgoing = outgoing.reshape(expert_count, capacity, features)
    arrived = lax.all_to_all(outgoing, "sp", split_axis=0, concat_axis=0, tiled=True)
    pooled = lax.all_gather(arrived.reshape(-1, features), "tp", axis=0, tiled=True)
    gate_value = jnp.dot(pooled, gate_weight[0], preferred_element_type=jnp.float32)
    up_value = jnp.dot(pooled, up_weight[0], preferred_element_type=jnp.float32)
    hidden = (jax.nn.silu(gate_value) * up_value).astype(jnp.bfloat16)
    answers = lax.psum_scatter(
        jnp.dot(hidden, down_weight[0], preferred_element_type=jnp.float32).astype(jnp.bfloat16),
        "tp",
        scatter_dimension=0,
        tiled=True,
    )
    returned = lax.all_to_all(
        answers.reshape(expert_count, capacity, features),
        "sp",
        split_axis=0,
        concat_axis=0,
        tiled=True,
    )
    picked = jnp.take(returned.reshape(expert_count * capacity, features), placing, axis=0)
    picked = picked.reshape(own_rows, chosen_count, features).astype(jnp.float32)
    combined = jnp.sum(route_weight[:, :, None] * picked, axis=1)
    return (middle_wide + combined).astype(jnp.bfloat16)


CORES = 2
MESH = pl.DeviceIdType.MESH
VMEM = pl.BlockSpec(memory_space=pltpu.VMEM)


def greet(peers):
    barrier = pltpu.get_barrier_semaphore()
    for peer in peers:
        pl.semaphore_signal(barrier, inc=1, device_id=peer, device_id_type=MESH)
    pl.semaphore_wait(barrier, len(peers))


def remote(source, target, send, receive, peer):
    return pltpu.make_async_remote_copy(
        src_ref=source,
        dst_ref=target,
        send_sem=send,
        recv_sem=receive,
        device_id=peer,
        device_id_type=MESH,
    )


def call(kernel, number, outs, scratch, args):
    return pl.pallas_call(
        kernel,
        out_shape=outs,
        in_specs=[VMEM] * len(args),
        out_specs=[VMEM] * len(outs),
        scratch_shapes=scratch,
        compiler_params=pltpu.CompilerParams(collective_id=number, has_side_effects=True),
    )(*args)


DMA = pltpu.SemaphoreType.DMA


def keys_kernel(outer, inner, count, *refs):
    ins, outs = refs[:count], refs[count : 2 * count]
    local, send_up, take_up, send_in, take_in = refs[2 * count :]
    place = lax.axis_index("sp")
    o, i = place // inner, place % inner
    tp = lax.axis_index("tp")

    def at(o_, i_):
        return (o_ * inner + i_, tp)

    greet(
        [at((o + d) % outer, i) for d in range(1, outer)]
        + [at(o, (i + d) % inner) for d in range(1, inner)]
    )
    other = at((o + 1) % outer, i)

    def up(t, a):
        slot = (o - t) * inner + i
        source = ins[a] if t == 0 else outs[a].at[slot]
        return remote(source, outs[a].at[slot], send_up.at[t, a], take_up.at[t, a], at(o + 1, i))

    def across(t, d, a):
        slot = (o - t) * inner + i
        source = ins[a] if t == 0 else outs[a].at[slot]
        return remote(
            source,
            outs[a].at[slot],
            send_in.at[t, d - 1, a],
            take_in.at[t, d - 1, a],
            at(o, (i + d) % inner),
        )

    def landed(slot, a, semaphore):
        remote(outs[a].at[slot], outs[a].at[slot], semaphore, semaphore, other).wait_recv()

    for a in range(count):
        pltpu.make_async_copy(ins[a], outs[a].at[place], local.at[a]).start()
    for t in range(outer):

        @pl.when(o >= t)
        def _(t=t):
            for a in range(count):
                if t > 0:
                    landed((o - t) * inner + i, a, take_up.at[t - 1, a])
                if t < outer - 1:

                    @pl.when(o + 1 < outer)
                    def _(a=a):
                        up(t, a).start()

                for d in range(1, inner):
                    if t > 0:
                        across(t, d, a).start()
                    else:

                        @pl.when((i + d) % inner > i)
                        def _(a=a, d=d):
                            across(t, d, a).start()

    for t in range(outer):

        @pl.when(o >= t)
        def _(t=t):
            for a in range(count):
                for d in range(1, inner):
                    giver = (i - d + inner) % inner
                    slot = (o - t) * inner + giver
                    if t > 0:
                        landed(slot, a, take_in.at[t, d - 1, a])
                        across(t, d, a).wait_send()
                    else:

                        @pl.when(giver < i)
                        def _(a=a, d=d, slot=slot):
                            landed(slot, a, take_in.at[0, d - 1, a])

                        @pl.when((i + d) % inner > i)
                        def _(a=a, d=d):
                            across(0, d, a).wait_send()

                if t < outer - 1:

                    @pl.when(o + 1 < outer)
                    def _(a=a):
                        up(t, a).wait_send()

    for a in range(count):
        pltpu.make_async_copy(ins[a], outs[a].at[place], local.at[a]).wait()


def gather_keys(arrays, outer, inner):
    count = len(arrays)
    outs = [jax.ShapeDtypeStruct((outer * inner,) + x.shape, x.dtype) for x in arrays]
    scratch = [
        DMA((count,)),
        DMA((outer, count)),
        DMA((outer, count)),
        DMA((outer, inner, count)),
        DMA((outer, inner, count)),
    ]
    return call(functools.partial(keys_kernel, outer, inner, count), 1, outs, scratch, arrays)


def attend_kernel(qw, qn, near, kw, vw, kn, vn, far, out, top, total, mixed):
    place = lax.axis_index("sp")
    rows = qw.shape[0]
    width = qn.shape[1]
    heads = 1 + width // HN
    lanes = lax.broadcasted_iota(jnp.int32, (rows, width), 1) // HN

    def query(h):
        if h == 0:
            return qw[...]
        return jnp.where(lanes == h - 1, qn[...], jnp.zeros_like(qn[...]))

    def block(j, shift, diagonal):
        for h in range(heads):
            keys, values = (kw, vw) if h == 0 else (kn, vn)
            size = HW if h == 0 else HN
            scores = lax.dot_general(
                query(h), keys[j], (((1,), (1,)), ((), ())), preferred_element_type=jnp.float32
            )
            drop = (near[:, h : h + 1] + shift[h]) - far[j, h : h + 1, :]
            scores = scores * size ** (-0.5) + drop
            if diagonal:
                t = lax.broadcasted_iota(jnp.int32, scores.shape, 0)
                s = lax.broadcasted_iota(jnp.int32, scores.shape, 1)
                scores = jnp.where(s <= t, scores, -jnp.inf)
            peak = jnp.max(scores, axis=1, keepdims=True)
            if diagonal:
                weights = jnp.exp(scores - peak)
                total[h] = jnp.sum(weights, axis=1, keepdims=True)
                mixed[h] = jnp.dot(
                    weights.astype(jnp.bfloat16), values[j], preferred_element_type=jnp.float32
                )
                top[h] = peak
            else:
                before = top[h]
                peak = jnp.maximum(before, peak)
                weights = jnp.exp(scores - peak)
                shrink = jnp.exp(before - peak)
                total[h] = total[h] * shrink + jnp.sum(weights, axis=1, keepdims=True)
                mixed[h] = mixed[h] * shrink + jnp.dot(
                    weights.astype(jnp.bfloat16), values[j], preferred_element_type=jnp.float32
                )
                top[h] = peak

    block(place, [jnp.zeros((1, 1), jnp.float32)] * heads, True)

    def step(t, shift):
        j = place - 1 - t
        shift = tuple(shift[h] + far[j, h : h + 1, rows - 1 : rows] for h in range(heads))
        block(j, shift, False)
        return shift

    lax.fori_loop(0, place, step, tuple(jnp.zeros((1, 1), jnp.float32) for _ in range(heads)))
    out[:, : qw.shape[1]] = (mixed[0] / total[0]).astype(jnp.bfloat16)
    narrow = mixed[1] / total[1]
    for h in range(2, heads):
        narrow = jnp.where(lanes == h - 1, mixed[h] / total[h], narrow)
    out[:, qw.shape[1] :] = narrow.astype(jnp.bfloat16)


def swap_kernel(axis, n, stride, source, target, local, send, take):
    sp, tp = lax.axis_index("sp"), lax.axis_index("tp")
    me = (sp if axis == "sp" else tp) // stride
    rest = (sp if axis == "sp" else tp) % stride

    def at(k):
        return (k * stride + rest, tp) if axis == "sp" else (sp, k * stride + rest)

    greet([at((me + d) % n) for d in range(1, n)])

    def copy(d):
        k = (me + d) % n
        return remote(source.at[k], target.at[me], send.at[d], take.at[d], at(k))

    for d in range(1, n):
        copy(d).start()
    own = pltpu.make_async_copy(source.at[me], target.at[me], local.at[0])
    own.start()
    own.wait()
    for d in range(1, n):
        slot = target.at[(me - d + n) % n]
        remote(slot, slot, send.at[d], take.at[d], at((me + d) % n)).wait_recv()
        copy(d).wait_send()


def swap(array, axis, n, stride, number):
    return call(
        functools.partial(swap_kernel, axis, n, stride),
        number,
        [jax.ShapeDtypeStruct(array.shape, array.dtype)],
        [DMA((1,)), DMA((n,)), DMA((n,))],
        [array],
    )[0]


def expert_kernel(outer, inner, ys, outgoing, gate, up, down, returned, *refs):
    pooled, answers, half, chip_a, chip_b, from_x, from_y, next_a, next_b = refs[:9]
    last_a, last_b, final, send, take = refs[9:]
    place, tp = lax.axis_index("sp"), lax.axis_index("tp")
    o, i, y, c = place // inner, place % inner, tp // CORES, tp % CORES
    far_i, far_y, far_c = (i + 1) % inner, (y + 1) % ys, (c + 1) % CORES
    features = down.shape[1]
    cap = outgoing.shape[1]
    h = cap // 2
    low, high = pl.ds(0, h), pl.ds(h, h)

    def at(o_, i_, y_, c_):
        return (o_ * inner + i_, y_ * CORES + c_)

    across, along, mate = at(o, far_i, y, c), at(o, i, far_y, c), at(o, i, y, far_c)
    greet([at((o + d) % outer, i, y, c) for d in range(1, outer)] + [across, along, mate])
    started = []

    def push(kind, t, source, target, peer):
        copy = remote(source, target, send.at[kind, t], take.at[kind, t], peer)
        copy.start()
        started.append(copy)

    def landed(kind, t, where):
        remote(where, where, send.at[kind, t], take.at[kind, t], mate).wait_recv()

    def begin(t):
        slot = pooled.at[t, c, i, y]
        source = outgoing.at[o]
        if t > 0:
            landed(0, t, slot)
            source = slot
        push(1, t, source, slot, across)
        push(2, t, source, slot, along)
        push(5, t, source, slot, mate)

    def relay(t):
        slot = pooled.at[t, c, far_i, y]
        landed(1, t, slot)
        part = pooled.at[t, c, far_i, y, low]
        push(3, t, part, part, along)
        push(6, t, slot, slot, mate)
        slot = pooled.at[t, c, i, far_y]
        landed(2, t, slot)
        part = pooled.at[t, c, i, far_y, high]
        push(4, t, part, part, across)
        push(7, t, slot, slot, mate)

    def corner(t):
        landed(3, t, pooled.at[t, c, far_i, far_y, low])
        landed(4, t, pooled.at[t, c, far_i, far_y, high])
        slot = pooled.at[t, c, far_i, far_y]
        push(8, t, slot, slot, mate)

    def feed(t):
        landed(5, t, pooled.at[t, far_c, i, y])
        landed(6, t, pooled.at[t, far_c, far_i, y])
        landed(7, t, pooled.at[t, far_c, i, far_y])
        landed(8, t, pooled.at[t, far_c, far_i, far_y])
        rows = CORES * inner * ys * cap
        x = pooled[t, :, :, :, :, :features].reshape(rows, features)
        extra = pooled[t, :, :, :, :, features:].reshape(rows, -1).astype(jnp.float32)
        lane = lax.broadcasted_iota(jnp.int32, extra.shape, 1)
        scale = jnp.sum(jnp.where(lane // 2 == i, extra, 0.0), axis=1, keepdims=True)
        g = jnp.dot(x, gate[...], preferred_element_type=jnp.float32)
        u = jnp.dot(x, up[...], preferred_element_type=jnp.float32)
        hidden = (jax.nn.silu(g) * u).astype(jnp.bfloat16)
        wide = math.gcd(features, 512)
        for n in range(features // wide):
            columns = pl.ds(n * wide, wide)
            part = jnp.dot(hidden, down[:, columns], preferred_element_type=jnp.float32)
            answers[t, :, :, :, :, columns] = (
                (part * scale).astype(jnp.bfloat16).reshape(CORES, inner, ys, cap, wide)
            )
        push(9, t, answers.at[t, far_c], half.at[t], mate)

    def gather(t):
        landed(9, t, half.at[t])
        for i_ in range(inner):
            for y_ in range(ys):
                total = answers[t, c, i_, y_].astype(jnp.float32)
                total = (total + half[t, i_, y_].astype(jnp.float32)).astype(jnp.bfloat16)
                chip_a[t, i_, y_] = total[:h]
                chip_b[t, y_, i_] = total[h:]
        push(10, t, chip_a.at[t, far_i], from_x.at[t], across)
        push(11, t, chip_b.at[t, far_y], from_y.at[t], along)

    def add(*parts):
        total = parts[0].astype(jnp.float32)
        for part in parts[1:]:
            total = total + part.astype(jnp.float32)
        return total.astype(jnp.bfloat16)

    def turn(t):
        landed(10, t, from_x.at[t])
        next_a[t] = add(chip_a[t, i, far_y], from_x[t, far_y])
        push(12, t, next_a.at[t], last_a.at[t], along)
        landed(11, t, from_y.at[t])
        next_b[t] = add(chip_b[t, y, far_i], from_y[t, far_i])
        push(13, t, next_b.at[t], last_b.at[t], across)

    def home(t):
        landed(12, t, last_a.at[t])
        landed(13, t, last_b.at[t])
        target = returned.at[o] if t == 0 else final.at[t]
        target[:h] = add(chip_a[t, i, y], from_x[t, y], last_a[t])
        target[h:] = add(chip_b[t, y, i], from_y[t, i], last_b[t])
        if t > 0:
            push(14, t, final.at[t], returned.at[o], at((o - t + outer) % outer, i, y, c))

    for d in range(1, outer):
        there = (o + d) % outer
        push(0, d, outgoing.at[there], pooled.at[d, c, i, y], at(there, i, y, c))
    pooled[0, c, i, y] = outgoing[o]
    begin(0)
    begin(1)
    for k in range(outer + 3):
        if k < outer:
            relay(k)
            if k + 2 < outer:
                begin(k + 2)
            corner(k)
        if 0 <= k - 1 < outer:
            gather(k - 1)
        if k < outer:
            feed(k)
        if 0 <= k - 3 < outer:
            home(k - 3)
        if 0 <= k - 2 < outer:
            turn(k - 2)
    for t in range(1, outer):
        landed(14, t, returned.at[(o + t) % outer])
    for copy in started:
        copy.wait_send()


def experts(outgoing, gate, up, down, outer, inner, ys):
    cap, width = outgoing.shape[1:]
    features = down.shape[1]
    h = cap // 2
    kind = jnp.bfloat16
    scratch = [
        pltpu.VMEM((outer, CORES, inner, ys, cap, width), kind),
        pltpu.VMEM((outer, CORES, inner, ys, cap, features), kind),
        pltpu.VMEM((outer, inner, ys, cap, features), kind),
        pltpu.VMEM((outer, inner, ys, h, features), kind),
        pltpu.VMEM((outer, ys, inner, h, features), kind),
        pltpu.VMEM((outer, ys, h, features), kind),
        pltpu.VMEM((outer, inner, h, features), kind),
        pltpu.VMEM((outer, h, features), kind),
        pltpu.VMEM((outer, h, features), kind),
        pltpu.VMEM((outer, h, features), kind),
        pltpu.VMEM((outer, h, features), kind),
        pltpu.VMEM((outer, cap, features), kind),
        DMA((15, outer)),
        DMA((15, outer)),
    ]
    return call(
        functools.partial(expert_kernel, outer, inner, ys),
        3,
        [jax.ShapeDtypeStruct((outer, cap, features), kind)],
        scratch,
        [outgoing, gate, up, down],
    )[0]


def fast_body(
    residual,
    query_wide,
    key_wide,
    value_wide,
    query_narrow,
    key_narrow,
    value_narrow,
    gate_wide,
    gate_narrow,
    out_wide,
    out_narrow,
    norm_gain,
    routing,
    route_weight,
    gate_weight,
    up_weight,
    down_weight,
):
    inner = routing.shape[1]
    places = lax.axis_size("sp")
    outer = places // inner
    parts = lax.axis_size("tp")
    ys = parts // CORES
    own_rows, features = residual.shape

    gates = jnp.concatenate([gate_wide, gate_narrow], axis=1).T
    running = jnp.cumsum(jax.nn.log_sigmoid(gates), axis=1)
    heads = gates.shape[0]
    far = jnp.pad(running, ((0, -heads % 8), (0, 0)))
    keys_wide, values_wide, keys_narrow, values_narrow, far = gather_keys(
        [key_wide, value_wide, key_narrow, value_narrow, far], outer, inner
    )
    shard_rows, wide = query_wide.shape
    narrow = query_narrow.shape[1]
    att = pl.pallas_call(
        attend_kernel,
        out_shape=jax.ShapeDtypeStruct((shard_rows, wide + narrow), jnp.bfloat16),
        in_specs=[VMEM] * 8,
        out_specs=VMEM,
        scratch_shapes=[
            pltpu.VMEM((heads, shard_rows, 1), jnp.float32),
            pltpu.VMEM((heads, shard_rows, 1), jnp.float32),
            pltpu.VMEM((heads, shard_rows, wide), jnp.float32),
        ],
    )(
        query_wide,
        query_narrow,
        running.T,
        keys_wide,
        values_wide,
        keys_narrow,
        values_narrow,
        far,
    )
    att = swap(att.reshape(parts, own_rows, wide + narrow), "tp", parts, 1, 2)
    att_wide = jnp.transpose(att[:, :, :wide], (1, 0, 2)).reshape(own_rows, parts * wide)
    att_narrow = jnp.transpose(att[:, :, wide:], (1, 0, 2)).reshape(own_rows, parts * narrow)
    mixed = jnp.dot(att_wide, out_wide, preferred_element_type=jnp.float32)
    mixed = mixed + jnp.dot(att_narrow, out_narrow, preferred_element_type=jnp.float32)
    middle = (residual.astype(jnp.float32) + mixed).astype(jnp.bfloat16)
    middle_wide = middle.astype(jnp.float32)
    spread = jnp.mean(middle_wide * middle_wide, axis=1, keepdims=True)
    normed = (middle_wide * lax.rsqrt(spread + epsilon) * norm_gain).astype(jnp.bfloat16)

    capacity = own_rows * GROUPS // places
    group = routing[:, 0] // inner
    matches = (group[:, None] == jnp.arange(GROUPS, dtype=jnp.int32)[None, :]).astype(jnp.int32)
    ranking = jnp.sum((jnp.cumsum(matches, axis=0) - matches) * matches, axis=1)
    placing = group * capacity + ranking
    picker = placing[None, :] == jnp.arange(GROUPS * capacity, dtype=jnp.int32)[:, None]
    of_expert = jnp.sum(
        jnp.where(
            (routing % inner)[:, :, None] == jnp.arange(inner, dtype=jnp.int32)[None, None, :],
            route_weight[:, :, None],
            0.0,
        ),
        axis=1,
    )
    high = of_expert.astype(jnp.bfloat16)
    rest = (of_expert - high.astype(jnp.float32)).astype(jnp.bfloat16)
    extra = jnp.stack([high, rest], axis=2).reshape(own_rows, 2 * inner)
    extra = jnp.pad(extra, ((0, 0), (0, -2 * inner % 128)))
    picker = picker.astype(jnp.bfloat16)
    outgoing = jnp.dot(
        picker, jnp.concatenate([normed, extra], axis=1), preferred_element_type=jnp.float32
    ).astype(jnp.bfloat16)
    returned = experts(
        outgoing.reshape(GROUPS, capacity, outgoing.shape[1]),
        gate_weight[0],
        up_weight[0],
        down_weight[0],
        outer,
        inner,
        ys,
    )
    combined = jnp.dot(
        picker.T, returned.reshape(-1, features), preferred_element_type=jnp.float32
    )
    return (middle_wide + combined).astype(jnp.bfloat16)


def choose(*args):
    routing, gate_weight = args[12], args[14]
    experts = gate_weight.shape[0] * lax.axis_size("sp")
    paired = lax.axis_size("tp") == 2 * CORES and gate_weight.shape[0] == 1
    paired = paired and routing.shape[1] == 2
    if paired and experts == GROUPS * routing.shape[1]:
        return fast_body(*args)
    return body(*args)


def solution(mesh):
    placed = (
        P(("sp", "tp"), None),
        P("sp", "tp"),
        P("sp", "tp"),
        P("sp", "tp"),
        P("sp", "tp"),
        P("sp", "tp"),
        P("sp", "tp"),
        P("sp", "tp"),
        P("sp", "tp"),
        P(),
        P(),
        P(),
        P(("sp", "tp"), None),
        P(("sp", "tp"), None),
        P("sp", None, "tp"),
        P("sp", None, "tp"),
        P("sp", "tp", None),
    )
    return jax.shard_map(
        choose, mesh=mesh, in_specs=placed, out_specs=P(("sp", "tp"), None), check_vma=False
    )
```

```python
import functools
import math

import jax
import jax.numpy as jnp
from jax import lax
from jax.experimental import pallas as pl
from jax.experimental.pallas import tpu as pltpu
from jax.sharding import PartitionSpec as P

HW = 128
HN = 64
GROUPS = 4


epsilon = 1e-06


def globalize(pieces, shard_rows):
    shards = pieces.shape[0] // shard_rows
    grid = pieces.reshape(shards, shard_rows, pieces.shape[1])
    endings = grid[:, -1, :]
    offsets = jnp.cumsum(endings, axis=0) - endings
    return (grid + offsets[:, None, :]).reshape(pieces.shape)


def head_block(
    state, queries, query_decay, keys, values, key_decay, first_key, first_query, head_width
):
    highest_old, weight_sum, weighted = state
    query_rows = queries.shape[0]
    head_count = query_decay.shape[1]
    key_rows = keys.shape[0]
    grid_query = queries.reshape(query_rows, head_count, head_width)
    grid_key = keys.reshape(key_rows, head_count, head_width)
    grid_value = values.reshape(key_rows, head_count, head_width)
    scores = jnp.einsum("thd,phd->htp", grid_query, grid_key, preferred_element_type=jnp.float32)
    scores = scores * head_width ** (-0.5) + query_decay.T[:, :, None] - key_decay.T[:, None, :]
    query_place = first_query + jnp.arange(query_rows, dtype=jnp.int32)
    key_place = first_key + jnp.arange(key_rows, dtype=jnp.int32)
    scores = jnp.where(key_place[None, None, :] <= query_place[None, :, None], scores, -jnp.inf)
    highest = jnp.maximum(highest_old, jnp.max(scores, axis=2))
    weights = jnp.exp(scores - highest[:, :, None])
    shrink = jnp.exp(highest_old - highest)
    weight_sum = weight_sum * shrink + jnp.sum(weights, axis=2)
    product = jnp.einsum(
        "htp,phd->htd", weights.astype(jnp.bfloat16), grid_value, preferred_element_type=jnp.float32
    )
    weighted = weighted * shrink[:, :, None] + product
    return (highest, weight_sum, weighted)


def fresh_state(head_count, shard_rows, head_width):
    return (
        jnp.full((head_count, shard_rows), -1e30, jnp.float32),
        jnp.zeros((head_count, shard_rows), jnp.float32),
        jnp.zeros((head_count, shard_rows, head_width), jnp.float32),
    )


def finish(state, shard_rows):
    highest, weight_sum, weighted = state
    mixed_heads = weighted / weight_sum[:, :, None]
    joined = jnp.transpose(mixed_heads, (1, 0, 2))
    return joined.reshape(shard_rows, weighted.shape[0] * weighted.shape[2]).astype(jnp.bfloat16)


def body(
    residual,
    query_wide,
    key_wide,
    value_wide,
    query_narrow,
    key_narrow,
    value_narrow,
    gate_wide,
    gate_narrow,
    out_wide,
    out_narrow,
    norm_gain,
    routing,
    route_weight,
    gate_weight,
    up_weight,
    down_weight,
):
    shard_rows = query_wide.shape[0]
    half_rows = shard_rows // 2
    sp_place = lax.axis_index("sp")
    first_query = sp_place * shard_rows
    running_wide = jnp.cumsum(jax.nn.log_sigmoid(gate_wide), axis=0)
    running_narrow = jnp.cumsum(jax.nn.log_sigmoid(gate_narrow), axis=0)
    pieces_wide, pieces_narrow = (
        lax.all_gather(running_wide, "sp", axis=0, tiled=True),
        lax.all_gather(running_narrow, "sp", axis=0, tiled=True),
    )
    every_wide = globalize(pieces_wide, shard_rows)
    every_narrow = globalize(pieces_narrow, shard_rows)
    late_first = first_query + half_rows
    halves = []
    for place, part_wide, part_narrow in (
        (first_query, query_wide[:half_rows], query_narrow[:half_rows]),
        (late_first, query_wide[half_rows:], query_narrow[half_rows:]),
    ):
        halves.append(
            (
                place,
                part_wide,
                part_narrow,
                lax.dynamic_slice_in_dim(every_wide, place, half_rows, 0),
                lax.dynamic_slice_in_dim(every_narrow, place, half_rows, 0),
            )
        )

    def half_state():
        return (
            fresh_state(gate_wide.shape[1], half_rows, HW),
            fresh_state(gate_narrow.shape[1], half_rows, HN),
        )

    state = (half_state(), half_state())
    keys_wide = lax.all_gather(key_wide, "sp", axis=0, tiled=True)
    values_wide = lax.all_gather(value_wide, "sp", axis=0, tiled=True)
    keys_narrow = lax.all_gather(key_narrow, "sp", axis=0, tiled=True)
    values_narrow = lax.all_gather(value_narrow, "sp", axis=0, tiled=True)
    span_rows = keys_wide.shape[0]
    block_size = math.gcd(span_rows, 2048)

    def visit(carried, position):
        inside = position * block_size

        def take_block(source):
            return lax.dynamic_slice_in_dim(source, inside, block_size, 0)

        def take_decay(source):
            return lax.dynamic_slice_in_dim(source, inside, block_size, 0)

        block_kw = take_block(keys_wide)
        block_vw = take_block(values_wide)
        block_kn = take_block(keys_narrow)
        block_vn = take_block(values_narrow)
        block_dw = take_decay(every_wide)
        block_dn = take_decay(every_narrow)

        def one_half(current, half):
            place, part_wide, part_narrow, query_decay_wide, query_decay_narrow = half

            def work(inner):
                first = head_block(
                    inner[0],
                    part_wide,
                    query_decay_wide,
                    block_kw,
                    block_vw,
                    block_dw,
                    inside,
                    place,
                    HW,
                )
                second = head_block(
                    inner[1],
                    part_narrow,
                    query_decay_narrow,
                    block_kn,
                    block_vn,
                    block_dn,
                    inside,
                    place,
                    HN,
                )
                return (first, second)

            def skip(inner):
                return inner

            return lax.cond(inside <= place + half_rows - 1, work, skip, current)

        updated = (one_half(carried[0], halves[0]), one_half(carried[1], halves[1]))
        return (updated, None)

    state, _ = lax.scan(visit, state, jnp.arange(span_rows // block_size, dtype=jnp.int32))
    att_wide = jnp.concatenate(
        [finish(state[0][0], half_rows), finish(state[1][0], half_rows)], axis=0
    )
    att_narrow = jnp.concatenate(
        [finish(state[0][1], half_rows), finish(state[1][1], half_rows)], axis=0
    )
    own_rows = residual.shape[0]
    tp_place = lax.axis_index("tp")
    rows_wide = lax.dynamic_slice_in_dim(
        out_wide, tp_place * att_wide.shape[1], att_wide.shape[1], 0
    )
    rows_narrow = lax.dynamic_slice_in_dim(
        out_narrow, tp_place * att_narrow.shape[1], att_narrow.shape[1], 0
    )
    first = jnp.dot(att_wide, rows_wide, preferred_element_type=jnp.float32)
    second = jnp.dot(att_narrow, rows_narrow, preferred_element_type=jnp.float32)
    mixed = lax.psum_scatter(
        (first + second).astype(jnp.bfloat16), "tp", scatter_dimension=0, tiled=True
    ).astype(jnp.float32)
    middle = (residual.astype(jnp.float32) + mixed).astype(jnp.bfloat16)
    middle_wide = middle.astype(jnp.float32)
    spread = jnp.mean(middle_wide * middle_wide, axis=1, keepdims=True)
    normed = (middle_wide * lax.rsqrt(spread + epsilon) * norm_gain).astype(jnp.bfloat16)
    features = normed.shape[1]
    chosen_count = routing.shape[1]
    expert_count = gate_weight.shape[0] * lax.axis_size("sp")
    capacity = own_rows * GROUPS // expert_count
    flat_routes = routing.reshape(-1)
    matches = (flat_routes[:, None] == jnp.arange(expert_count, dtype=jnp.int32)[None, :]).astype(
        jnp.int32
    )
    ranking = jnp.sum((jnp.cumsum(matches, axis=0) - matches) * matches, axis=1)
    placing = flat_routes * capacity + ranking
    picker = (
        placing[None, :] == jnp.arange(expert_count * capacity, dtype=jnp.int32)[:, None]
    ).astype(jnp.bfloat16)
    picker = jnp.sum(picker.reshape(expert_count * capacity, own_rows, chosen_count), axis=2)
    outgoing = jnp.dot(picker, normed, preferred_element_type=jnp.float32).astype(jnp.bfloat16)
    outgoing = outgoing.reshape(expert_count, capacity, features)
    arrived = lax.all_to_all(outgoing, "sp", split_axis=0, concat_axis=0, tiled=True)
    pooled = lax.all_gather(arrived.reshape(-1, features), "tp", axis=0, tiled=True)
    gate_value = jnp.dot(pooled, gate_weight[0], preferred_element_type=jnp.float32)
    up_value = jnp.dot(pooled, up_weight[0], preferred_element_type=jnp.float32)
    hidden = (jax.nn.silu(gate_value) * up_value).astype(jnp.bfloat16)
    answers = lax.psum_scatter(
        jnp.dot(hidden, down_weight[0], preferred_element_type=jnp.float32).astype(jnp.bfloat16),
        "tp",
        scatter_dimension=0,
        tiled=True,
    )
    returned = lax.all_to_all(
        answers.reshape(expert_count, capacity, features),
        "sp",
        split_axis=0,
        concat_axis=0,
        tiled=True,
    )
    picked = jnp.take(returned.reshape(expert_count * capacity, features), placing, axis=0)
    picked = picked.reshape(own_rows, chosen_count, features).astype(jnp.float32)
    combined = jnp.sum(route_weight[:, :, None] * picked, axis=1)
    return (middle_wide + combined).astype(jnp.bfloat16)


CORES = 2
MESH = pl.DeviceIdType.MESH
VMEM = pl.BlockSpec(memory_space=pltpu.VMEM)


def greet(peers):
    barrier = pltpu.get_barrier_semaphore()
    for peer in peers:
        pl.semaphore_signal(barrier, inc=1, device_id=peer, device_id_type=MESH)
    pl.semaphore_wait(barrier, len(peers))


def remote(source, target, send, receive, peer):
    return pltpu.make_async_remote_copy(
        src_ref=source,
        dst_ref=target,
        send_sem=send,
        recv_sem=receive,
        device_id=peer,
        device_id_type=MESH,
    )


DMA = pltpu.SemaphoreType.DMA


LOG2E = math.log2(math.e)


def layer_kernel(outer, inner, ys, *refs):
    gates, qw, kw, vw, qn, kn, vn, residual, gain, picker, extra = refs[:11]
    out_wide, out_narrow, gate_hbm, up_hbm, down_hbm, result = refs[11:17]
    kws, vws, kns, vns, far, run, peak, total, acc_w, acc_n, att, swapped = refs[17:29]
    wide_w, narrow_w, gate, up, down, middle, outgoing, returned = refs[29:37]
    pooled, answers, half, chip_a, chip_b, from_x, from_y, next_a, next_b = refs[37:46]
    last_a, last_b, final = refs[46:49]
    load, lift_s, lift_r, cross_s, cross_r, far_s, far_r, swap_s, swap_r, send, take = refs[49:]
    place, tp = lax.axis_index("sp"), lax.axis_index("tp")
    o, i, y, c = place // inner, place % inner, tp // CORES, tp % CORES
    far_i, far_y, far_c = (i + 1) % inner, (y + 1) % ys, (c + 1) % CORES
    places, parts = outer * inner, ys * CORES
    rows, wide = qw.shape
    narrow = qn.shape[1]
    heads = 1 + narrow // HN
    own_rows, features = residual.shape
    cap = outgoing.shape[1]
    h = cap // 2
    low, high = pl.ds(0, h), pl.ds(h, h)

    def at(o_, i_, y_, c_):
        return (o_ * inner + i_, y_ * CORES + c_)

    across, along, mate = at(o, far_i, y, c), at(o, i, far_y, c), at(o, i, y, far_c)

    loads = [
        pltpu.make_async_copy(source, target, load.at[n])
        for n, (source, target) in enumerate(
            [
                (out_wide, wide_w),
                (out_narrow, narrow_w),
                (gate_hbm.at[0], gate),
                (up_hbm.at[0], up),
                (down_hbm.at[0], down),
            ]
        )
    ]
    for copy in loads:
        copy.start()
    far[...] = jnp.zeros_like(far)
    greet(
        [((place + d) % places, tp) for d in range(1, places)]
        + [(place, (tp + d) % parts) for d in range(1, parts)]
    )

    ins, blocks = (kw, vw, kn, vn), (kws, vws, kns, vns)
    count = len(ins)

    def source_of(t, a):
        slot = (o - t) * inner + i
        return (ins[a] if t == 0 else blocks[a].at[slot]), blocks[a].at[slot]

    def lift(t, a):
        source, target = source_of(t, a)
        return remote(
            source, target, lift_s.at[t, a], lift_r.at[t, a], at(o + 1, i, y, c)
        )

    def cross(t, a):
        source, target = source_of(t, a)
        return remote(source, target, cross_s.at[t, a], cross_r.at[t, a], across)

    def arrived(where, semaphore):
        remote(where, where, semaphore, semaphore, mate).wait_recv()

    for a in range(count):

        @pl.when(o + 1 < outer)
        def _(a=a):
            lift(0, a).start()

        @pl.when(i < far_i)
        def _(a=a):
            cross(0, a).start()

    x = gates[...]
    step = jnp.minimum(x, 0.0) - jnp.log1p(jnp.exp(-jnp.abs(x)))
    lane = lax.broadcasted_iota(jnp.int32, step.shape, 1)
    shift = 1
    while shift < rows:
        step = step + jnp.where(lane >= shift, pltpu.roll(step, shift, 1), 0.0)
        shift *= 2
    run[...] = step
    near = step * LOG2E

    head_lane = lax.broadcasted_iota(jnp.int32, (rows, narrow), 1) // HN

    def attend(block_of, decay, diagonal):
        columns = jnp.transpose(decay * LOG2E)
        for n in range(heads):
            k, v = (block_of(0), block_of(1)) if n == 0 else (block_of(2), block_of(3))
            if n == 0:
                q, size = qw[...], HW
            else:
                q, size = jnp.where(head_lane == n - 1, qn[...], jnp.zeros_like(qn[...])), HN
            s = lax.dot_general(k, q, (((1,), (1,)), ((), ())), preferred_element_type=jnp.float32)
            s = s * (LOG2E * size ** (-0.5)) - columns[:, n : n + 1]
            if diagonal:
                key = lax.broadcasted_iota(jnp.int32, s.shape, 0)
                query = lax.broadcasted_iota(jnp.int32, s.shape, 1)
                s = jnp.where(key <= query, s, -jnp.inf)
            row = near[n : n + 1]
            new = jnp.max(s, axis=0, keepdims=True) + row
            if not diagonal:
                before = peak[n : n + 1]
                new = jnp.maximum(new, before)
            weights = jnp.exp2(s - (new - row))
            mass = jnp.sum(weights, axis=0, keepdims=True)
            part = lax.dot_general(
                v if n == 0 else v[:, (n - 1) * HN : n * HN],
                weights.astype(jnp.bfloat16),
                (((0,), (0,)), ((), ())),
                preferred_element_type=jnp.float32,
            )
            acc = acc_w if n == 0 else acc_n.at[(n - 1) * HN : n * HN]
            if diagonal:
                total[n : n + 1] = mass
                acc[...] = part
            else:
                shrink = jnp.exp2(before - new)
                total[n : n + 1] = total[n : n + 1] * shrink + mass
                acc[...] = acc[...] * shrink + part
            peak[n : n + 1] = new

    attend(lambda a: ins[a][...], step, True)
    for d in range(1, places):

        @pl.when(place + d < places)
        def _(d=d):
            remote(run, far.at[place], far_s.at[d], far_r.at[d], (place + d, tp)).start()

    for d in range(1, places):

        @pl.when(place >= d)
        def _(d=d):
            arrived(far.at[place - d], far_r.at[d])

    def visit(slot):
        offset = jnp.zeros((far.shape[1], 1), jnp.float32)
        for b in range(places):
            inside = jnp.logical_and(b >= slot, b < place)
            offset = offset + jnp.where(inside, far[b, :, rows - 1 : rows], 0.0)
        attend(lambda a: blocks[a][slot], far[slot] - offset, False)

    def relay(t):
        @pl.when(o >= t)
        def _():
            for a in range(count):
                arrived(blocks[a].at[(o - t) * inner + i], lift_r.at[t - 1, a])
                if t < outer - 1:

                    @pl.when(o + 1 < outer)
                    def _(a=a):
                        lift(t, a).start()

                cross(t, a).start()

    def own(t):
        @pl.when(o >= t)
        def _():
            visit((o - t) * inner + i)

    def other(t):
        @pl.when((o >= t) if t > 0 else (far_i < i))
        def _():
            slot = (o - t) * inner + far_i
            for a in range(count):
                arrived(blocks[a].at[slot], cross_r.at[t, a])
            visit(slot)

    for t in range(outer):
        if t > 0:
            own(t)
        if t + 1 < outer:
            relay(t + 1)
        other(t)

    mixed = jnp.transpose(acc_w[...] / total[0:1]).astype(jnp.bfloat16)
    att[:, :, :wide] = mixed.reshape(parts, own_rows, wide)
    for n in range(1, heads):
        piece = slice((n - 1) * HN, n * HN)
        acc_n[piece] = acc_n[piece] / total[n : n + 1]
    mixed = jnp.transpose(acc_n[...]).astype(jnp.bfloat16)
    att[:, :, wide:] = mixed.reshape(parts, own_rows, narrow)

    def swap(d):
        k = (tp + d) % parts
        return remote(att.at[k], swapped.at[tp], swap_s.at[d], swap_r.at[d], (place, k))

    for d in range(1, parts):
        swap(d).start()
    swapped[tp] = att[tp]
    for t in range(outer):
        for a in range(count):
            if t < outer - 1:

                @pl.when(jnp.logical_and(o >= t, o + 1 < outer))
                def _(t=t, a=a):
                    lift(t, a).wait_send()

            @pl.when((o >= t) if t > 0 else (i < far_i))
            def _(t=t, a=a):
                cross(t, a).wait_send()

    for d in range(1, places):

        @pl.when(place + d < places)
        def _(d=d):
            remote(run, far.at[place], far_s.at[d], far_r.at[d], (place + d, tp)).wait_send()

    loads[0].wait()
    loads[1].wait()
    for d in range(1, parts):
        arrived(swapped.at[(tp - d + parts) % parts], swap_r.at[d])
        swap(d).wait_send()
    rows_w = jnp.concatenate([swapped[p, :, :wide] for p in range(parts)], axis=1)
    rows_n = jnp.concatenate([swapped[p, :, wide:] for p in range(parts)], axis=1)
    tile = math.gcd(features, 512)
    squares = jnp.zeros((own_rows, 1), jnp.float32)
    for n in range(features // tile):
        at_n = pl.ds(n * tile, tile)
        part = jnp.dot(rows_w, wide_w[:, at_n], preferred_element_type=jnp.float32)
        part = part + jnp.dot(rows_n, narrow_w[:, at_n], preferred_element_type=jnp.float32)
        part = (residual[:, at_n].astype(jnp.float32) + part).astype(jnp.bfloat16)
        middle[:, at_n] = part
        part = part.astype(jnp.float32)
        squares = squares + jnp.sum(part * part, axis=1, keepdims=True)
    factor = lax.rsqrt(squares / features + epsilon)
    pick = picker[...]
    for n in range(features // tile):
        at_n = pl.ds(n * tile, tile)
        part = middle[:, at_n].astype(jnp.float32) * factor * gain[:, at_n]
        part = jnp.dot(pick, part.astype(jnp.bfloat16), preferred_element_type=jnp.float32)
        outgoing[:, :, at_n] = part.astype(jnp.bfloat16).reshape(GROUPS, cap, tile)
    part = jnp.dot(pick, extra[...], preferred_element_type=jnp.float32)
    outgoing[:, :, features:] = part.astype(jnp.bfloat16).reshape(GROUPS, cap, extra.shape[1])

    started = []

    def push(kind, t, source, target, peer):
        copy = remote(source, target, send.at[kind, t], take.at[kind, t], peer)
        copy.start()
        started.append(copy)

    def landed(kind, t, where):
        arrived(where, take.at[kind, t])

    def begin(t):
        slot = pooled.at[t, c, i, y]
        source = outgoing.at[o]
        if t > 0:
            landed(0, t, slot)
            source = slot
        push(1, t, source, slot, across)
        push(2, t, source, slot, along)
        push(5, t, source, slot, mate)

    def relay(t):
        slot = pooled.at[t, c, far_i, y]
        landed(1, t, slot)
        part = pooled.at[t, c, far_i, y, low]
        push(3, t, part, part, along)
        push(6, t, slot, slot, mate)
        slot = pooled.at[t, c, i, far_y]
        landed(2, t, slot)
        part = pooled.at[t, c, i, far_y, high]
        push(4, t, part, part, across)
        push(7, t, slot, slot, mate)

    def corner(t):
        landed(3, t, pooled.at[t, c, far_i, far_y, low])
        landed(4, t, pooled.at[t, c, far_i, far_y, high])
        slot = pooled.at[t, c, far_i, far_y]
        push(8, t, slot, slot, mate)

    def feed(t):
        landed(5, t, pooled.at[t, far_c, i, y])
        landed(6, t, pooled.at[t, far_c, far_i, y])
        landed(7, t, pooled.at[t, far_c, i, far_y])
        landed(8, t, pooled.at[t, far_c, far_i, far_y])
        rows = CORES * inner * ys * cap
        x = pooled[t, :, :, :, :, :features].reshape(rows, features)
        extra = pooled[t, :, :, :, :, features:].reshape(rows, -1).astype(jnp.float32)
        lane = lax.broadcasted_iota(jnp.int32, extra.shape, 1)
        scale = jnp.sum(jnp.where(lane // 2 == i, extra, 0.0), axis=1, keepdims=True)
        if t == 0:
            for copy in loads[2:]:
                copy.wait()
        g = jnp.dot(x, gate[...], preferred_element_type=jnp.float32)
        u = jnp.dot(x, up[...], preferred_element_type=jnp.float32)
        hidden = (jax.nn.silu(g) * u).astype(jnp.bfloat16)
        wide = math.gcd(features, 512)
        for n in range(features // wide):
            columns = pl.ds(n * wide, wide)
            part = jnp.dot(hidden, down[:, columns], preferred_element_type=jnp.float32)
            answers[t, :, :, :, :, columns] = (
                (part * scale).astype(jnp.bfloat16).reshape(CORES, inner, ys, cap, wide)
            )
        push(9, t, answers.at[t, far_c], half.at[t], mate)

    def gather(t):
        landed(9, t, half.at[t])
        for i_ in range(inner):
            for y_ in range(ys):
                total = answers[t, c, i_, y_].astype(jnp.float32)
                total = (total + half[t, i_, y_].astype(jnp.float32)).astype(jnp.bfloat16)
                chip_a[t, i_, y_] = total[:h]
                chip_b[t, y_, i_] = total[h:]
        push(10, t, chip_a.at[t, far_i], from_x.at[t], across)
        push(11, t, chip_b.at[t, far_y], from_y.at[t], along)

    def add(*parts):
        total = parts[0].astype(jnp.float32)
        for part in parts[1:]:
            total = total + part.astype(jnp.float32)
        return total.astype(jnp.bfloat16)

    def turn(t):
        landed(10, t, from_x.at[t])
        next_a[t] = add(chip_a[t, i, far_y], from_x[t, far_y])
        push(12, t, next_a.at[t], last_a.at[t], along)
        landed(11, t, from_y.at[t])
        next_b[t] = add(chip_b[t, y, far_i], from_y[t, far_i])
        push(13, t, next_b.at[t], last_b.at[t], across)

    def home(t):
        landed(12, t, last_a.at[t])
        landed(13, t, last_b.at[t])
        target = returned.at[o] if t == 0 else final.at[t]
        target[:h] = add(chip_a[t, i, y], from_x[t, y], last_a[t])
        target[h:] = add(chip_b[t, y, i], from_y[t, i], last_b[t])
        if t > 0:
            push(14, t, final.at[t], returned.at[o], at((o - t + outer) % outer, i, y, c))

    for d in range(1, outer):
        there = (o + d) % outer
        push(0, d, outgoing.at[there], pooled.at[d, c, i, y], at(there, i, y, c))
    pooled[0, c, i, y] = outgoing[o]
    begin(0)
    begin(1)
    for k in range(outer + 3):
        if k < outer:
            relay(k)
            if k + 2 < outer:
                begin(k + 2)
            corner(k)
        if 0 <= k - 1 < outer:
            gather(k - 1)
        if k < outer:
            feed(k)
        if 0 <= k - 3 < outer:
            home(k - 3)
        if 0 <= k - 2 < outer:
            turn(k - 2)
    for t in range(1, outer):
        landed(14, t, returned.at[(o + t) % outer])
    for copy in started:
        copy.wait_send()
    slots = returned[...].reshape(GROUPS * cap, features)
    combined = lax.dot_general(
        pick, slots, (((0,), (0,)), ((), ())), preferred_element_type=jnp.float32
    )
    result[...] = (middle[...].astype(jnp.float32) + combined).astype(jnp.bfloat16)


def fast_body(
    residual,
    query_wide,
    key_wide,
    value_wide,
    query_narrow,
    key_narrow,
    value_narrow,
    gate_wide,
    gate_narrow,
    out_wide,
    out_narrow,
    norm_gain,
    routing,
    route_weight,
    gate_weight,
    up_weight,
    down_weight,
):
    inner = routing.shape[1]
    places = lax.axis_size("sp")
    outer = places // inner
    parts = lax.axis_size("tp")
    ys = parts // CORES
    own_rows, features = residual.shape
    gates = jnp.concatenate([gate_wide, gate_narrow], axis=1).T
    gates = jnp.pad(gates, ((0, -gates.shape[0] % 8), (0, 0)))
    rows, wide = query_wide.shape
    narrow = query_narrow.shape[1]

    cap = own_rows * GROUPS // places
    group = routing[:, 0] // inner
    matches = (group[:, None] == jnp.arange(GROUPS, dtype=jnp.int32)[None, :]).astype(jnp.int32)
    ranking = jnp.sum((jnp.cumsum(matches, axis=0) - matches) * matches, axis=1)
    placing = group * cap + ranking
    picker = placing[None, :] == jnp.arange(GROUPS * cap, dtype=jnp.int32)[:, None]
    picker = picker.astype(jnp.bfloat16)
    of_expert = jnp.sum(
        jnp.where(
            (routing % inner)[:, :, None] == jnp.arange(inner, dtype=jnp.int32)[None, None, :],
            route_weight[:, :, None],
            0.0,
        ),
        axis=1,
    )
    high = of_expert.astype(jnp.bfloat16)
    rest = (of_expert - high.astype(jnp.float32)).astype(jnp.bfloat16)
    extra = jnp.stack([high, rest], axis=2).reshape(own_rows, 2 * inner)
    extra = jnp.pad(extra, ((0, 0), (0, -2 * inner % 128)))

    h = cap // 2
    width = features + extra.shape[1]
    kind, full = jnp.bfloat16, jnp.float32

    def vmem(*shape, dtype=kind):
        return pltpu.VMEM(shape, dtype)

    scratch = [
        vmem(places, rows, wide),
        vmem(places, rows, wide),
        vmem(places, rows, narrow),
        vmem(places, rows, narrow),
        vmem(places, gates.shape[0], rows, dtype=full),
        vmem(gates.shape[0], rows, dtype=full),
        vmem(gates.shape[0], rows, dtype=full),
        vmem(gates.shape[0], rows, dtype=full),
        vmem(wide, rows, dtype=full),
        vmem(narrow, rows, dtype=full),
        vmem(parts, own_rows, wide + narrow),
        vmem(parts, own_rows, wide + narrow),
        vmem(*out_wide.shape),
        vmem(*out_narrow.shape),
        vmem(*gate_weight.shape[1:]),
        vmem(*up_weight.shape[1:]),
        vmem(*down_weight.shape[1:]),
        vmem(own_rows, features),
        vmem(GROUPS, cap, width),
        vmem(outer, cap, features),
        vmem(outer, CORES, inner, ys, cap, width),
        vmem(outer, CORES, inner, ys, cap, features),
        vmem(outer, inner, ys, cap, features),
        vmem(outer, inner, ys, h, features),
        vmem(outer, ys, inner, h, features),
        vmem(outer, ys, h, features),
        vmem(outer, inner, h, features),
        vmem(outer, h, features),
        vmem(outer, h, features),
        vmem(outer, h, features),
        vmem(outer, h, features),
        vmem(outer, cap, features),
        DMA((5,)),
        DMA((outer, 4)),
        DMA((outer, 4)),
        DMA((outer, 4)),
        DMA((outer, 4)),
        DMA((places,)),
        DMA((places,)),
        DMA((parts,)),
        DMA((parts,)),
        DMA((15, outer)),
        DMA((15, outer)),
    ]
    anywhere = pl.BlockSpec(memory_space=pl.ANY)
    return pl.pallas_call(
        functools.partial(layer_kernel, outer, inner, ys),
        out_shape=jax.ShapeDtypeStruct(residual.shape, residual.dtype),
        in_specs=[VMEM] * 11 + [anywhere] * 5,
        out_specs=VMEM,
        scratch_shapes=scratch,
        compiler_params=pltpu.CompilerParams(
            collective_id=1, has_side_effects=True, vmem_limit_bytes=56 * 1024 * 1024
        ),
    )(
        gates,
        query_wide,
        key_wide,
        value_wide,
        query_narrow,
        key_narrow,
        value_narrow,
        residual,
        norm_gain[None, :],
        picker,
        extra,
        out_wide,
        out_narrow,
        gate_weight,
        up_weight,
        down_weight,
    )


def choose(*args):
    routing, gate_weight = args[12], args[14]
    experts = gate_weight.shape[0] * lax.axis_size("sp")
    paired = lax.axis_size("tp") == 2 * CORES and gate_weight.shape[0] == 1
    paired = paired and routing.shape[1] == 2
    if paired and experts == GROUPS * routing.shape[1]:
        return fast_body(*args)
    return body(*args)


def solution(mesh):
    placed = (
        P(("sp", "tp"), None),
        P("sp", "tp"),
        P("sp", "tp"),
        P("sp", "tp"),
        P("sp", "tp"),
        P("sp", "tp"),
        P("sp", "tp"),
        P("sp", "tp"),
        P("sp", "tp"),
        P(),
        P(),
        P(),
        P(("sp", "tp"), None),
        P(("sp", "tp"), None),
        P("sp", None, "tp"),
        P("sp", None, "tp"),
        P("sp", "tp", None),
    )
    return jax.shard_map(
        choose, mesh=mesh, in_specs=placed, out_specs=P(("sp", "tp"), None), check_vma=False
    )
```

```python
import functools
import math

import jax
import jax.numpy as jnp
from jax import lax
from jax.experimental import pallas as pl
from jax.experimental.pallas import tpu as pltpu
from jax.sharding import PartitionSpec as P

HW = 128
HN = 64
GROUPS = 4


epsilon = 1e-06


def globalize(pieces, shard_rows):
    shards = pieces.shape[0] // shard_rows
    grid = pieces.reshape(shards, shard_rows, pieces.shape[1])
    endings = grid[:, -1, :]
    offsets = jnp.cumsum(endings, axis=0) - endings
    return (grid + offsets[:, None, :]).reshape(pieces.shape)


def head_block(
    state, queries, query_decay, keys, values, key_decay, first_key, first_query, head_width
):
    highest_old, weight_sum, weighted = state
    query_rows = queries.shape[0]
    head_count = query_decay.shape[1]
    key_rows = keys.shape[0]
    grid_query = queries.reshape(query_rows, head_count, head_width)
    grid_key = keys.reshape(key_rows, head_count, head_width)
    grid_value = values.reshape(key_rows, head_count, head_width)
    scores = jnp.einsum("thd,phd->htp", grid_query, grid_key, preferred_element_type=jnp.float32)
    scores = scores * head_width ** (-0.5) + query_decay.T[:, :, None] - key_decay.T[:, None, :]
    query_place = first_query + jnp.arange(query_rows, dtype=jnp.int32)
    key_place = first_key + jnp.arange(key_rows, dtype=jnp.int32)
    scores = jnp.where(key_place[None, None, :] <= query_place[None, :, None], scores, -jnp.inf)
    highest = jnp.maximum(highest_old, jnp.max(scores, axis=2))
    weights = jnp.exp(scores - highest[:, :, None])
    shrink = jnp.exp(highest_old - highest)
    weight_sum = weight_sum * shrink + jnp.sum(weights, axis=2)
    product = jnp.einsum(
        "htp,phd->htd", weights.astype(jnp.bfloat16), grid_value, preferred_element_type=jnp.float32
    )
    weighted = weighted * shrink[:, :, None] + product
    return (highest, weight_sum, weighted)


def fresh_state(head_count, shard_rows, head_width):
    return (
        jnp.full((head_count, shard_rows), -1e30, jnp.float32),
        jnp.zeros((head_count, shard_rows), jnp.float32),
        jnp.zeros((head_count, shard_rows, head_width), jnp.float32),
    )


def finish(state, shard_rows):
    highest, weight_sum, weighted = state
    mixed_heads = weighted / weight_sum[:, :, None]
    joined = jnp.transpose(mixed_heads, (1, 0, 2))
    return joined.reshape(shard_rows, weighted.shape[0] * weighted.shape[2]).astype(jnp.bfloat16)


def body(
    residual,
    query_wide,
    key_wide,
    value_wide,
    query_narrow,
    key_narrow,
    value_narrow,
    gate_wide,
    gate_narrow,
    out_wide,
    out_narrow,
    norm_gain,
    routing,
    route_weight,
    gate_weight,
    up_weight,
    down_weight,
):
    shard_rows = query_wide.shape[0]
    half_rows = shard_rows // 2
    sp_place = lax.axis_index("sp")
    first_query = sp_place * shard_rows
    running_wide = jnp.cumsum(jax.nn.log_sigmoid(gate_wide), axis=0)
    running_narrow = jnp.cumsum(jax.nn.log_sigmoid(gate_narrow), axis=0)
    pieces_wide, pieces_narrow = (
        lax.all_gather(running_wide, "sp", axis=0, tiled=True),
        lax.all_gather(running_narrow, "sp", axis=0, tiled=True),
    )
    every_wide = globalize(pieces_wide, shard_rows)
    every_narrow = globalize(pieces_narrow, shard_rows)
    late_first = first_query + half_rows
    halves = []
    for place, part_wide, part_narrow in (
        (first_query, query_wide[:half_rows], query_narrow[:half_rows]),
        (late_first, query_wide[half_rows:], query_narrow[half_rows:]),
    ):
        halves.append(
            (
                place,
                part_wide,
                part_narrow,
                lax.dynamic_slice_in_dim(every_wide, place, half_rows, 0),
                lax.dynamic_slice_in_dim(every_narrow, place, half_rows, 0),
            )
        )

    def half_state():
        return (
            fresh_state(gate_wide.shape[1], half_rows, HW),
            fresh_state(gate_narrow.shape[1], half_rows, HN),
        )

    state = (half_state(), half_state())
    keys_wide = lax.all_gather(key_wide, "sp", axis=0, tiled=True)
    values_wide = lax.all_gather(value_wide, "sp", axis=0, tiled=True)
    keys_narrow = lax.all_gather(key_narrow, "sp", axis=0, tiled=True)
    values_narrow = lax.all_gather(value_narrow, "sp", axis=0, tiled=True)
    span_rows = keys_wide.shape[0]
    block_size = math.gcd(span_rows, 2048)

    def visit(carried, position):
        inside = position * block_size

        def take_block(source):
            return lax.dynamic_slice_in_dim(source, inside, block_size, 0)

        def take_decay(source):
            return lax.dynamic_slice_in_dim(source, inside, block_size, 0)

        block_kw = take_block(keys_wide)
        block_vw = take_block(values_wide)
        block_kn = take_block(keys_narrow)
        block_vn = take_block(values_narrow)
        block_dw = take_decay(every_wide)
        block_dn = take_decay(every_narrow)

        def one_half(current, half):
            place, part_wide, part_narrow, query_decay_wide, query_decay_narrow = half

            def work(inner):
                first = head_block(
                    inner[0],
                    part_wide,
                    query_decay_wide,
                    block_kw,
                    block_vw,
                    block_dw,
                    inside,
                    place,
                    HW,
                )
                second = head_block(
                    inner[1],
                    part_narrow,
                    query_decay_narrow,
                    block_kn,
                    block_vn,
                    block_dn,
                    inside,
                    place,
                    HN,
                )
                return (first, second)

            def skip(inner):
                return inner

            return lax.cond(inside <= place + half_rows - 1, work, skip, current)

        updated = (one_half(carried[0], halves[0]), one_half(carried[1], halves[1]))
        return (updated, None)

    state, _ = lax.scan(visit, state, jnp.arange(span_rows // block_size, dtype=jnp.int32))
    att_wide = jnp.concatenate(
        [finish(state[0][0], half_rows), finish(state[1][0], half_rows)], axis=0
    )
    att_narrow = jnp.concatenate(
        [finish(state[0][1], half_rows), finish(state[1][1], half_rows)], axis=0
    )
    own_rows = residual.shape[0]
    tp_place = lax.axis_index("tp")
    rows_wide = lax.dynamic_slice_in_dim(
        out_wide, tp_place * att_wide.shape[1], att_wide.shape[1], 0
    )
    rows_narrow = lax.dynamic_slice_in_dim(
        out_narrow, tp_place * att_narrow.shape[1], att_narrow.shape[1], 0
    )
    first = jnp.dot(att_wide, rows_wide, preferred_element_type=jnp.float32)
    second = jnp.dot(att_narrow, rows_narrow, preferred_element_type=jnp.float32)
    mixed = lax.psum_scatter(
        (first + second).astype(jnp.bfloat16), "tp", scatter_dimension=0, tiled=True
    ).astype(jnp.float32)
    middle = (residual.astype(jnp.float32) + mixed).astype(jnp.bfloat16)
    middle_wide = middle.astype(jnp.float32)
    spread = jnp.mean(middle_wide * middle_wide, axis=1, keepdims=True)
    normed = (middle_wide * lax.rsqrt(spread + epsilon) * norm_gain).astype(jnp.bfloat16)
    features = normed.shape[1]
    chosen_count = routing.shape[1]
    expert_count = gate_weight.shape[0] * lax.axis_size("sp")
    capacity = own_rows * GROUPS // expert_count
    flat_routes = routing.reshape(-1)
    matches = (flat_routes[:, None] == jnp.arange(expert_count, dtype=jnp.int32)[None, :]).astype(
        jnp.int32
    )
    ranking = jnp.sum((jnp.cumsum(matches, axis=0) - matches) * matches, axis=1)
    placing = flat_routes * capacity + ranking
    picker = (
        placing[None, :] == jnp.arange(expert_count * capacity, dtype=jnp.int32)[:, None]
    ).astype(jnp.bfloat16)
    picker = jnp.sum(picker.reshape(expert_count * capacity, own_rows, chosen_count), axis=2)
    outgoing = jnp.dot(picker, normed, preferred_element_type=jnp.float32).astype(jnp.bfloat16)
    outgoing = outgoing.reshape(expert_count, capacity, features)
    arrived = lax.all_to_all(outgoing, "sp", split_axis=0, concat_axis=0, tiled=True)
    pooled = lax.all_gather(arrived.reshape(-1, features), "tp", axis=0, tiled=True)
    gate_value = jnp.dot(pooled, gate_weight[0], preferred_element_type=jnp.float32)
    up_value = jnp.dot(pooled, up_weight[0], preferred_element_type=jnp.float32)
    hidden = (jax.nn.silu(gate_value) * up_value).astype(jnp.bfloat16)
    answers = lax.psum_scatter(
        jnp.dot(hidden, down_weight[0], preferred_element_type=jnp.float32).astype(jnp.bfloat16),
        "tp",
        scatter_dimension=0,
        tiled=True,
    )
    returned = lax.all_to_all(
        answers.reshape(expert_count, capacity, features),
        "sp",
        split_axis=0,
        concat_axis=0,
        tiled=True,
    )
    picked = jnp.take(returned.reshape(expert_count * capacity, features), placing, axis=0)
    picked = picked.reshape(own_rows, chosen_count, features).astype(jnp.float32)
    combined = jnp.sum(route_weight[:, :, None] * picked, axis=1)
    return (middle_wide + combined).astype(jnp.bfloat16)


CORES = 2
MESH = pl.DeviceIdType.MESH
VMEM = pl.BlockSpec(memory_space=pltpu.VMEM)


def greet(peers):
    barrier = pltpu.get_barrier_semaphore()
    for peer in peers:
        pl.semaphore_signal(barrier, inc=1, device_id=peer, device_id_type=MESH)
    pl.semaphore_wait(barrier, len(peers))


def remote(source, target, send, receive, peer):
    return pltpu.make_async_remote_copy(
        src_ref=source,
        dst_ref=target,
        send_sem=send,
        recv_sem=receive,
        device_id=peer,
        device_id_type=MESH,
    )


DMA = pltpu.SemaphoreType.DMA


LOG2E = math.log2(math.e)


def layer_kernel(outer, inner, ys, *refs):
    gate_w, gate_n, chosen, shares, qw, kw, vw, qn, kn, vn, residual, gain = refs[:12]
    out_wide, out_narrow, gate_hbm, up_hbm, down_hbm, result = refs[12:18]
    refs = refs[3:]
    kws, vws, kns, vns, far, run, peak, total, acc_w, acc_n, att, swapped = refs[15:27]
    wide_w, narrow_w, gate, up, down, middle, outgoing, returned = refs[27:35]
    pooled, answers, half, chip_a, chip_b, from_x, from_y, next_a, next_b = refs[35:44]
    last_a, last_b, final, picker, board, factor = refs[44:50]
    load, lift_s, lift_r, cross_s, cross_r, turn_s, turn_r = refs[50:57]
    far_s, far_r, swap_s, swap_r, send, take = refs[57:]
    place, tp = lax.axis_index("sp"), lax.axis_index("tp")
    o, i, y, c = place // inner, place % inner, tp // CORES, tp % CORES
    far_i, far_y, far_c = (i + 1) % inner, (y + 1) % ys, (c + 1) % CORES
    places, parts = outer * inner, ys * CORES
    rows, wide = qw.shape
    narrow = qn.shape[1]
    heads = 1 + narrow // HN
    own_rows, features = residual.shape
    cap = outgoing.shape[1]
    h = cap // 2
    low, high = pl.ds(0, h), pl.ds(h, h)

    def at(o_, i_, y_, c_):
        return (o_ * inner + i_, y_ * CORES + c_)

    across, along, mate = at(o, far_i, y, c), at(o, i, far_y, c), at(o, i, y, far_c)

    loads = [
        pltpu.make_async_copy(source, target, load.at[n])
        for n, (source, target) in enumerate(
            [
                (out_wide, wide_w),
                (out_narrow, narrow_w),
                (gate_hbm.at[0], gate),
                (up_hbm.at[0], up),
                (down_hbm.at[0], down),
            ]
        )
    ]
    for copy in loads:
        copy.start()
    far[...] = jnp.zeros_like(far)
    peers = [((place + d) % places, tp) for d in range(1, places)]
    peers = peers + [(place, (tp + d) % parts) for d in range(1, parts)]
    barrier = pltpu.get_barrier_semaphore()
    for peer in peers:
        pl.semaphore_signal(barrier, inc=1, device_id=peer, device_id_type=MESH)
    picks = chosen.shape[0]
    board[...] = jnp.zeros_like(board)
    board[:1] = gate_w[...]
    board[1:heads] = gate_n[...]
    board[heads : heads + picks, :own_rows] = chosen[...].astype(jnp.float32)
    board[heads + picks : heads + 2 * picks, :own_rows] = shares[...]
    facts = board[...]
    step = jnp.minimum(facts, 0.0) - jnp.log1p(jnp.exp(-jnp.abs(facts)))
    lane = lax.broadcasted_iota(jnp.int32, step.shape, 1)
    shift = 1
    while shift < rows:
        step = step + jnp.where(lane >= shift, pltpu.roll(step, shift, 1), 0.0)
        shift *= 2
    run[...] = step
    near = step * LOG2E
    pl.semaphore_wait(barrier, len(peers))
    for d in range(1, places):

        @pl.when(place + d < places)
        def _(d=d):
            remote(run, far.at[place], far_s.at[d], far_r.at[d], (place + d, tp)).start()

    ins, blocks = (kw, vw, kn, vn), (kws, vws, kns, vns)
    count = len(ins)

    def source_of(t, a):
        slot = (o - t) * inner + i
        return (ins[a] if t == 0 else blocks[a].at[slot]), blocks[a].at[slot]

    def lift(t, a):
        source, target = source_of(t, a)
        return remote(
            source, target, lift_s.at[t, a], lift_r.at[t, a], at(o + 1, i, y, c)
        )

    def cross(t, a):
        source, target = source_of(t, a)
        return remote(source, target, cross_s.at[t, a], cross_r.at[t, a], across)

    def arrived(where, semaphore):
        remote(where, where, semaphore, semaphore, mate).wait_recv()

    def detour(a):
        slot = blocks[a].at[far_i]
        return remote(slot, slot, turn_s.at[a], turn_r.at[a], at(o + 1, i, y, c))

    def detours(a):
        return a >= count // 2

    def crosses(t, a):
        if t == 0:
            return jnp.logical_or(i < far_i, o == 0) if detours(a) else i < far_i
        return o > t if detours(a) else o >= t

    for a in range(count):

        @pl.when(o + 1 < outer)
        def _(a=a):
            lift(0, a).start()

        @pl.when(crosses(0, a))
        def _(a=a):
            cross(0, a).start()

    head_lane = lax.broadcasted_iota(jnp.int32, (rows, narrow), 1) // HN

    def attend(block_of, decay, diagonal):
        columns = jnp.transpose(decay * LOG2E)
        for n in range(heads):
            k, v = (block_of(0), block_of(1)) if n == 0 else (block_of(2), block_of(3))
            if n == 0:
                q, size = qw[...], HW
            else:
                q, size = jnp.where(head_lane == n - 1, qn[...], jnp.zeros_like(qn[...])), HN
            s = lax.dot_general(k, q, (((1,), (1,)), ((), ())), preferred_element_type=jnp.float32)
            s = s * (LOG2E * size ** (-0.5)) - columns[:, n : n + 1]
            if diagonal:
                key = lax.broadcasted_iota(jnp.int32, s.shape, 0)
                query = lax.broadcasted_iota(jnp.int32, s.shape, 1)
                s = jnp.where(key <= query, s, -jnp.inf)
            row = near[n : n + 1]
            new = jnp.max(s, axis=0, keepdims=True) + row
            if not diagonal:
                before = peak[n : n + 1]
                new = jnp.maximum(new, before)
            weights = jnp.exp2(s - (new - row))
            mass = jnp.sum(weights, axis=0, keepdims=True)
            part = lax.dot_general(
                v if n == 0 else v[:, (n - 1) * HN : n * HN],
                weights.astype(jnp.bfloat16),
                (((0,), (0,)), ((), ())),
                preferred_element_type=jnp.float32,
            )
            acc = acc_w if n == 0 else acc_n.at[(n - 1) * HN : n * HN]
            if diagonal:
                total[n : n + 1] = mass
                acc[...] = part
            else:
                shrink = jnp.exp2(before - new)
                total[n : n + 1] = total[n : n + 1] * shrink + mass
                acc[...] = acc[...] * shrink + part
            peak[n : n + 1] = new

    attend(lambda a: ins[a][...], step, True)
    columns = jnp.transpose(facts)[:own_rows]

    def group_of(names):
        return jnp.floor((names + 0.5) / inner)

    group = group_of(facts[heads : heads + 1, :own_rows])
    ahead = lax.broadcasted_iota(jnp.int32, (own_rows, own_rows), 0)
    ahead = ahead < lax.broadcasted_iota(jnp.int32, (own_rows, own_rows), 1)
    same = jnp.logical_and(group_of(columns[:, heads : heads + 1]) == group, ahead)
    placing = group * cap + jnp.sum(jnp.where(same, 1.0, 0.0), axis=0, keepdims=True)
    slots = lax.broadcasted_iota(jnp.int32, (GROUPS * cap, own_rows), 0).astype(jnp.float32)
    picker[...] = jnp.where(slots == placing, 1.0, 0.0).astype(jnp.bfloat16)
    lane = lax.broadcasted_iota(jnp.int32, (own_rows, outgoing.shape[2] - features), 1)
    extra = jnp.zeros(lane.shape, jnp.float32)
    for e in range(inner):
        weight = jnp.zeros((own_rows, 1), jnp.float32)
        for k in range(picks):
            name = columns[:, heads + k : heads + k + 1]
            value = columns[:, heads + picks + k : heads + picks + k + 1]
            weight = weight + jnp.where(name - inner * group_of(name) == e, value, 0.0)
        top = weight.astype(jnp.bfloat16).astype(jnp.float32)
        extra = jnp.where(lane == 2 * e, top, extra)
        extra = jnp.where(lane == 2 * e + 1, weight - top, extra)
    part = jnp.dot(picker[...], extra.astype(jnp.bfloat16), preferred_element_type=jnp.float32)
    outgoing[:, :, features:] = part.astype(jnp.bfloat16).reshape(GROUPS, cap, lane.shape[1])

    for d in range(1, places):

        @pl.when(place >= d)
        def _(d=d):
            arrived(far.at[place - d], far_r.at[d])

    def visit(slot):
        offset = jnp.zeros((far.shape[1], 1), jnp.float32)
        for b in range(places):
            inside = jnp.logical_and(b >= slot, b < place)
            offset = offset + jnp.where(inside, far[b, :, rows - 1 : rows], 0.0)
        attend(lambda a: blocks[a][slot], far[slot] - offset, False)

    def relay(t):
        @pl.when(o >= t)
        def _():
            for a in range(count):
                arrived(blocks[a].at[(o - t) * inner + i], lift_r.at[t - 1, a])
                if t < outer - 1:

                    @pl.when(o + 1 < outer)
                    def _(a=a):
                        lift(t, a).start()

                pl.when(crosses(t, a))(lambda: cross(t, a).start())

    def own(t):
        @pl.when(o >= t)
        def _():
            visit((o - t) * inner + i)

    def other(t):
        slot = (o - t) * inner + far_i
        for a in range(count):
            where = blocks[a].at[slot]
            if not detours(a):
                pl.when((o >= t) if t > 0 else (far_i < i))(
                    lambda: arrived(where, cross_r.at[t, a])
                )
                continue
            if t > 0:
                pl.when(o > t)(lambda: arrived(where, cross_r.at[t, a]))
                pl.when(o == t)(lambda: arrived(where, turn_r.at[a]))
            else:
                pl.when(jnp.logical_or(far_i < i, o == 0))(
                    lambda: arrived(where, cross_r.at[t, a])
                )
            if t < outer - 1:
                pl.when(o == t)(lambda: detour(a).start())

        @pl.when((o >= t) if t > 0 else (far_i < i))
        def _():
            visit(slot)

    def finish():
        mixed = jnp.transpose(acc_w[...] / total[0:1]).astype(jnp.bfloat16)
        att[:, :, :wide] = mixed.reshape(parts, own_rows, wide)
        for n in range(1, heads):
            piece = slice((n - 1) * HN, n * HN)
            acc_n[piece] = acc_n[piece] / total[n : n + 1]
        mixed = jnp.transpose(acc_n[...]).astype(jnp.bfloat16)
        att[:, :, wide:] = mixed.reshape(parts, own_rows, narrow)
        for d in range(1, parts):
            swap(d).start()
        swapped[tp] = att[tp]

    def swap(d):
        k = (tp + d) % parts
        return remote(att.at[k], swapped.at[tp], swap_s.at[d], swap_r.at[d], (place, k))

    def settle():
        for d in range(1, parts):
            arrived(swapped.at[(tp - d + parts) % parts], swap_r.at[d])

    tile = math.gcd(features, 512)

    def project():
        rows_w = jnp.concatenate([swapped[p, :, :wide] for p in range(parts)], axis=1)
        rows_n = jnp.concatenate([swapped[p, :, wide:] for p in range(parts)], axis=1)
        squares = jnp.zeros((own_rows, 1), jnp.float32)
        for n in range(features // tile):
            at_n = pl.ds(n * tile, tile)
            part = jnp.dot(rows_w, wide_w[:, at_n], preferred_element_type=jnp.float32)
            part = part + jnp.dot(rows_n, narrow_w[:, at_n], preferred_element_type=jnp.float32)
            part = (residual[:, at_n].astype(jnp.float32) + part).astype(jnp.bfloat16)
            middle[:, at_n] = part
            part = part.astype(jnp.float32)
            squares = squares + jnp.sum(part * part, axis=1, keepdims=True)
        factor[...] = lax.rsqrt(squares / features + epsilon)

    def ready():
        for n in range(features // tile):
            at_n = pl.ds(n * tile, tile)
            part = middle[:, at_n].astype(jnp.float32) * factor[...] * gain[:, at_n]
            part = jnp.dot(
                picker[...], part.astype(jnp.bfloat16), preferred_element_type=jnp.float32
            )
            outgoing[:, :, at_n] = part.astype(jnp.bfloat16).reshape(GROUPS, cap, tile)

    def route(kind, t):
        mine, beside = pooled.at[t, c, i, y], pooled.at[t, c, far_i, y]
        below, corners = pooled.at[t, c, i, far_y], pooled.at[t, c, far_i, far_y]
        if kind == 0:
            return outgoing.at[t, low], pooled.at[o, c, i, y, low], at(t, i, y, c)
        if kind == 1:
            return outgoing.at[t, high], pooled.at[o, c, i, y, high], at(t, i, y, c)
        if kind == 2:
            return mine.at[low], mine.at[low], across
        if kind == 3:
            return mine.at[high], mine.at[high], across
        if kind == 4:
            return mine.at[low], mine.at[low], along
        if kind == 5:
            return mine.at[high], mine.at[high], along
        if kind == 6:
            return beside.at[low], beside.at[low], along
        if kind == 7:
            return below.at[high], below.at[high], across
        if kind in (8, 9, 10, 11):
            slot = (mine, beside, below, corners)[kind - 8]
            return slot, slot, mate
        if kind == 12:
            return answers.at[t, far_c], half.at[t], mate
        if kind == 13:
            return chip_a.at[t, far_i, far_y], from_x.at[t, far_y], across
        if kind == 14:
            return chip_a.at[t, far_i, y], from_x.at[t, y], across
        if kind == 15:
            return chip_b.at[t, far_y, far_i], from_y.at[t, far_i], along
        if kind == 16:
            return chip_b.at[t, far_y, i], from_y.at[t, i], along
        if kind == 17:
            return next_a.at[t], last_a.at[t], along
        if kind == 18:
            return next_b.at[t], last_b.at[t], across
        return final.at[t], returned.at[o], at(t, i, y, c)

    def copy_of(kind, t):
        source, target, peer = route(kind, t)
        mark = o if kind in (0, 1, 19) else t
        return remote(source, target, send.at[kind, t], take.at[kind, mark], peer)

    def push(kind, t):
        if kind in (0, 1, 19):
            pl.when(o != t)(lambda: copy_of(kind, t).start())
        else:
            copy_of(kind, t).start()

    def landed(kind, t, where):
        arrived(where, take.at[kind, t])

    def late(t):
        return jnp.logical_and(o + 2 <= t, o < outer - 2)

    def send_rows(t):
        push(0, t)
        push(1, t)

    def dispatch():
        for t in range(outer):
            pl.when(jnp.logical_not(late(t)))(lambda: send_rows(t))

        pooled[o, c, i, y] = outgoing[o]

    def begin(t):
        slot = pooled.at[t, c, i, y]

        def hold(kind, part):
            pl.when(o != t)(lambda: landed(kind, t, slot.at[part]))

        hold(0, low)
        push(2, t)
        hold(1, high)
        push(5, t)
        push(3, t)
        push(4, t)
        push(8, t)

    def pass_on(t):
        beside, below = pooled.at[t, c, far_i, y], pooled.at[t, c, i, far_y]
        landed(2, t, beside.at[low])
        push(6, t)
        landed(5, t, below.at[high])
        push(7, t)
        landed(3, t, beside.at[high])
        push(9, t)
        landed(4, t, below.at[low])
        push(10, t)

    def corner(t):
        landed(6, t, pooled.at[t, c, far_i, far_y, low])
        landed(7, t, pooled.at[t, c, far_i, far_y, high])
        push(11, t)

    def feed(t):
        landed(8, t, pooled.at[t, far_c, i, y])
        landed(9, t, pooled.at[t, far_c, far_i, y])
        landed(10, t, pooled.at[t, far_c, i, far_y])
        landed(11, t, pooled.at[t, far_c, far_i, far_y])
        rows = CORES * inner * ys * cap
        x = pooled[t, :, :, :, :, :features].reshape(rows, features)
        extra = pooled[t, :, :, :, :, features:].reshape(rows, -1).astype(jnp.float32)
        lane = lax.broadcasted_iota(jnp.int32, extra.shape, 1)
        scale = jnp.sum(jnp.where(lane // 2 == i, extra, 0.0), axis=1, keepdims=True)
        g = jnp.dot(x, gate[...], preferred_element_type=jnp.float32)
        u = jnp.dot(x, up[...], preferred_element_type=jnp.float32)
        hidden = (jax.nn.silu(g) * u).astype(jnp.bfloat16)
        wide = math.gcd(features, 512)
        for n in range(features // wide):
            columns = pl.ds(n * wide, wide)
            part = jnp.dot(hidden, down[:, columns], preferred_element_type=jnp.float32)
            answers[t, :, :, :, :, columns] = (
                (part * scale).astype(jnp.bfloat16).reshape(CORES, inner, ys, cap, wide)
            )
        push(12, t)

    def gather(t):
        landed(12, t, half.at[t])
        for i_ in range(inner):
            for y_ in range(ys):
                total = answers[t, c, i_, y_].astype(jnp.float32)
                total = (total + half[t, i_, y_].astype(jnp.float32)).astype(jnp.bfloat16)
                chip_a[t, i_, y_] = total[:h]
                chip_b[t, y_, i_] = total[h:]
        push(13, t)
        push(15, t)
        push(14, t)
        push(16, t)

    def add(*parts):
        total = parts[0].astype(jnp.float32)
        for part in parts[1:]:
            total = total + part.astype(jnp.float32)
        return total.astype(jnp.bfloat16)

    def turn(t):
        landed(13, t, from_x.at[t, far_y])
        next_a[t] = add(chip_a[t, i, far_y], from_x[t, far_y])
        push(17, t)
        landed(15, t, from_y.at[t, far_i])
        next_b[t] = add(chip_b[t, y, far_i], from_y[t, far_i])
        push(18, t)

    def home(t):
        landed(14, t, from_x.at[t, y])
        landed(16, t, from_y.at[t, i])
        landed(17, t, last_a.at[t])
        landed(18, t, last_b.at[t])
        final[t, :h] = add(chip_a[t, i, y], from_x[t, y], last_a[t])
        final[t, h:] = add(chip_b[t, y, i], from_y[t, i], last_b[t])
        push(19, t)

    final_plane = o == outer - 1
    relay(1)
    other(0)
    own(1)
    relay(2)
    other(1)
    own(2)
    relay(3)
    other(2)
    own(3)

    other(3)
    finish()

    loads[0].wait()
    loads[1].wait()
    settle()

    project()
    ready()
    dispatch()
    for copy in loads[2:]:
        copy.wait()

    @pl.when(final_plane)
    def _():
        begin(0)
        begin(1)
        pass_on(0)
        begin(2)
        begin(3)
        corner(0)
        feed(0)
        pass_on(1)
        corner(1)
        feed(1)
        gather(0)
        pass_on(2)
        gather(1)
        pass_on(3)
        corner(2)
        feed(2)
        turn(0)
        gather(2)
        corner(3)
        feed(3)
        turn(1)
        gather(3)
        home(0)
        turn(2)
        home(1)
        turn(3)
        home(2)
        home(3)

    @pl.when(jnp.logical_not(final_plane))
    def _():
        begin(0)
        pass_on(0)
        for t in range(outer):
            pl.when(late(t))(lambda: send_rows(t))
        for k in range(outer):
            if k + 1 < outer:
                begin(k + 1)
            if k >= 2:
                home(k - 2)
            corner(k)
            feed(k)
            if k + 1 < outer:
                pass_on(k + 1)
            if k >= 1:
                turn(k - 1)
            gather(k)
        home(outer - 2)
        turn(outer - 1)
        home(outer - 1)

    for t in range(outer):
        for a in range(count):
            if t < outer - 1:

                @pl.when(jnp.logical_and(o >= t, o + 1 < outer))
                def _(t=t, a=a):
                    lift(t, a).wait_send()

            @pl.when(crosses(t, a))
            def _(t=t, a=a):
                cross(t, a).wait_send()

    for a in range(count):
        if detours(a):

            @pl.when(o + 1 < outer)
            def _(a=a):
                detour(a).wait_send()

    for d in range(1, places):

        @pl.when(place + d < places)
        def _(d=d):
            remote(run, far.at[place], far_s.at[d], far_r.at[d], (place + d, tp)).wait_send()

    for d in range(1, parts):
        swap(d).wait_send()

    returned[o] = final[o]
    for t in range(outer):

        @pl.when(o != t)
        def _(t=t):
            landed(19, t, returned.at[t])

    for t in range(outer):
        for kind in range(20):
            if kind in (0, 1, 19):
                pl.when(o != t)(lambda: copy_of(kind, t).wait_send())
            else:
                copy_of(kind, t).wait_send()

    slots = returned[...].reshape(GROUPS * cap, features)
    combined = lax.dot_general(
        picker[...], slots, (((0,), (0,)), ((), ())), preferred_element_type=jnp.float32
    )
    result[...] = (middle[...].astype(jnp.float32) + combined).astype(jnp.bfloat16)


def fast_body(
    residual,
    query_wide,
    key_wide,
    value_wide,
    query_narrow,
    key_narrow,
    value_narrow,
    gate_wide,
    gate_narrow,
    out_wide,
    out_narrow,
    norm_gain,
    routing,
    route_weight,
    gate_weight,
    up_weight,
    down_weight,
):
    inner = routing.shape[1]
    places = lax.axis_size("sp")
    outer = places // inner
    parts = lax.axis_size("tp")
    ys = parts // CORES
    own_rows, features = residual.shape
    rows, wide = query_wide.shape
    narrow = query_narrow.shape[1]
    heads = gate_wide.shape[1] + gate_narrow.shape[1]
    lines = pl.cdiv(heads + 2 * inner, 8) * 8
    cap = own_rows * GROUPS // places
    h = cap // 2
    width = features + 128 * pl.cdiv(2 * inner, 128)
    kind, full = jnp.bfloat16, jnp.float32

    def vmem(*shape, dtype=kind):
        return pltpu.VMEM(shape, dtype)

    scratch = [
        vmem(places, rows, wide),
        vmem(places, rows, wide),
        vmem(places, rows, narrow),
        vmem(places, rows, narrow),
        vmem(places, lines, rows, dtype=full),
        vmem(lines, rows, dtype=full),
        vmem(lines, rows, dtype=full),
        vmem(lines, rows, dtype=full),
        vmem(wide, rows, dtype=full),
        vmem(narrow, rows, dtype=full),
        vmem(parts, own_rows, wide + narrow),
        vmem(parts, own_rows, wide + narrow),
        vmem(*out_wide.shape),
        vmem(*out_narrow.shape),
        vmem(*gate_weight.shape[1:]),
        vmem(*up_weight.shape[1:]),
        vmem(*down_weight.shape[1:]),
        vmem(own_rows, features),
        vmem(GROUPS, cap, width),
        vmem(outer, cap, features),
        vmem(outer, CORES, inner, ys, cap, width),
        vmem(outer, CORES, inner, ys, cap, features),
        vmem(outer, inner, ys, cap, features),
        vmem(outer, inner, ys, h, features),
        vmem(outer, ys, inner, h, features),
        vmem(outer, ys, h, features),
        vmem(outer, inner, h, features),
        vmem(outer, h, features),
        vmem(outer, h, features),
        vmem(outer, h, features),
        vmem(outer, h, features),
        vmem(outer, cap, features),
        vmem(GROUPS * cap, own_rows),
        vmem(lines, rows, dtype=full),
        vmem(own_rows, 1, dtype=full),
        DMA((5,)),
        DMA((outer, 4)),
        DMA((outer, 4)),
        DMA((outer, 4)),
        DMA((outer, 4)),
        DMA((4,)),
        DMA((4,)),
        DMA((places,)),
        DMA((places,)),
        DMA((parts,)),
        DMA((parts,)),
        DMA((20, outer)),
        DMA((20, outer)),
    ]
    anywhere = pl.BlockSpec(memory_space=pl.ANY)
    return pl.pallas_call(
        functools.partial(layer_kernel, outer, inner, ys),
        out_shape=jax.ShapeDtypeStruct(residual.shape, residual.dtype),
        in_specs=[VMEM] * 12 + [anywhere] * 5,
        out_specs=VMEM,
        scratch_shapes=scratch,
        compiler_params=pltpu.CompilerParams(
            collective_id=1, has_side_effects=True, vmem_limit_bytes=56 * 1024 * 1024
        ),
    )(
        gate_wide.T,
        gate_narrow.T,
        routing.T,
        route_weight.T,
        query_wide,
        key_wide,
        value_wide,
        query_narrow,
        key_narrow,
        value_narrow,
        residual,
        norm_gain[None, :],
        out_wide,
        out_narrow,
        gate_weight,
        up_weight,
        down_weight,
    )


def choose(*args):
    routing, gate_weight = args[12], args[14]
    experts = gate_weight.shape[0] * lax.axis_size("sp")
    paired = lax.axis_size("tp") == 2 * CORES and gate_weight.shape[0] == 1
    paired = paired and routing.shape[1] == 2
    if paired and experts == GROUPS * routing.shape[1]:
        return fast_body(*args)
    return body(*args)


def solution(mesh):
    placed = (
        P(("sp", "tp"), None),
        P("sp", "tp"),
        P("sp", "tp"),
        P("sp", "tp"),
        P("sp", "tp"),
        P("sp", "tp"),
        P("sp", "tp"),
        P("sp", "tp"),
        P("sp", "tp"),
        P(),
        P(),
        P(),
        P(("sp", "tp"), None),
        P(("sp", "tp"), None),
        P("sp", None, "tp"),
        P("sp", None, "tp"),
        P("sp", "tp", None),
    )
    return jax.shard_map(
        choose, mesh=mesh, in_specs=placed, out_specs=P(("sp", "tp"), None), check_vma=False
    )
```

```python
import functools
import math

import jax
import jax.numpy as jnp
from jax import lax
from jax.experimental import pallas as pl
from jax.experimental.pallas import tpu as pltpu
from jax.sharding import PartitionSpec as P

HW = 128
HN = 64
GROUPS = 4


epsilon = 1e-06


def globalize(pieces, shard_rows):
    shards = pieces.shape[0] // shard_rows
    grid = pieces.reshape(shards, shard_rows, pieces.shape[1])
    endings = grid[:, -1, :]
    offsets = jnp.cumsum(endings, axis=0) - endings
    return (grid + offsets[:, None, :]).reshape(pieces.shape)


def head_block(
    state, queries, query_decay, keys, values, key_decay, first_key, first_query, head_width
):
    highest_old, weight_sum, weighted = state
    query_rows = queries.shape[0]
    head_count = query_decay.shape[1]
    key_rows = keys.shape[0]
    grid_query = queries.reshape(query_rows, head_count, head_width)
    grid_key = keys.reshape(key_rows, head_count, head_width)
    grid_value = values.reshape(key_rows, head_count, head_width)
    scores = jnp.einsum("thd,phd->htp", grid_query, grid_key, preferred_element_type=jnp.float32)
    scores = scores * head_width ** (-0.5) + query_decay.T[:, :, None] - key_decay.T[:, None, :]
    query_place = first_query + jnp.arange(query_rows, dtype=jnp.int32)
    key_place = first_key + jnp.arange(key_rows, dtype=jnp.int32)
    scores = jnp.where(key_place[None, None, :] <= query_place[None, :, None], scores, -jnp.inf)
    highest = jnp.maximum(highest_old, jnp.max(scores, axis=2))
    weights = jnp.exp(scores - highest[:, :, None])
    shrink = jnp.exp(highest_old - highest)
    weight_sum = weight_sum * shrink + jnp.sum(weights, axis=2)
    product = jnp.einsum(
        "htp,phd->htd", weights.astype(jnp.bfloat16), grid_value, preferred_element_type=jnp.float32
    )
    weighted = weighted * shrink[:, :, None] + product
    return (highest, weight_sum, weighted)


def fresh_state(head_count, shard_rows, head_width):
    return (
        jnp.full((head_count, shard_rows), -1e30, jnp.float32),
        jnp.zeros((head_count, shard_rows), jnp.float32),
        jnp.zeros((head_count, shard_rows, head_width), jnp.float32),
    )


def finish(state, shard_rows):
    highest, weight_sum, weighted = state
    mixed_heads = weighted / weight_sum[:, :, None]
    joined = jnp.transpose(mixed_heads, (1, 0, 2))
    return joined.reshape(shard_rows, weighted.shape[0] * weighted.shape[2]).astype(jnp.bfloat16)


def body(
    residual,
    query_wide,
    key_wide,
    value_wide,
    query_narrow,
    key_narrow,
    value_narrow,
    gate_wide,
    gate_narrow,
    out_wide,
    out_narrow,
    norm_gain,
    routing,
    route_weight,
    gate_weight,
    up_weight,
    down_weight,
):
    shard_rows = query_wide.shape[0]
    half_rows = shard_rows // 2
    sp_place = lax.axis_index("sp")
    first_query = sp_place * shard_rows
    running_wide = jnp.cumsum(jax.nn.log_sigmoid(gate_wide), axis=0)
    running_narrow = jnp.cumsum(jax.nn.log_sigmoid(gate_narrow), axis=0)
    pieces_wide, pieces_narrow = (
        lax.all_gather(running_wide, "sp", axis=0, tiled=True),
        lax.all_gather(running_narrow, "sp", axis=0, tiled=True),
    )
    every_wide = globalize(pieces_wide, shard_rows)
    every_narrow = globalize(pieces_narrow, shard_rows)
    late_first = first_query + half_rows
    halves = []
    for place, part_wide, part_narrow in (
        (first_query, query_wide[:half_rows], query_narrow[:half_rows]),
        (late_first, query_wide[half_rows:], query_narrow[half_rows:]),
    ):
        halves.append(
            (
                place,
                part_wide,
                part_narrow,
                lax.dynamic_slice_in_dim(every_wide, place, half_rows, 0),
                lax.dynamic_slice_in_dim(every_narrow, place, half_rows, 0),
            )
        )

    def half_state():
        return (
            fresh_state(gate_wide.shape[1], half_rows, HW),
            fresh_state(gate_narrow.shape[1], half_rows, HN),
        )

    state = (half_state(), half_state())
    keys_wide = lax.all_gather(key_wide, "sp", axis=0, tiled=True)
    values_wide = lax.all_gather(value_wide, "sp", axis=0, tiled=True)
    keys_narrow = lax.all_gather(key_narrow, "sp", axis=0, tiled=True)
    values_narrow = lax.all_gather(value_narrow, "sp", axis=0, tiled=True)
    span_rows = keys_wide.shape[0]
    block_size = math.gcd(span_rows, 2048)

    def visit(carried, position):
        inside = position * block_size

        def take_block(source):
            return lax.dynamic_slice_in_dim(source, inside, block_size, 0)

        def take_decay(source):
            return lax.dynamic_slice_in_dim(source, inside, block_size, 0)

        block_kw = take_block(keys_wide)
        block_vw = take_block(values_wide)
        block_kn = take_block(keys_narrow)
        block_vn = take_block(values_narrow)
        block_dw = take_decay(every_wide)
        block_dn = take_decay(every_narrow)

        def one_half(current, half):
            place, part_wide, part_narrow, query_decay_wide, query_decay_narrow = half

            def work(inner):
                first = head_block(
                    inner[0],
                    part_wide,
                    query_decay_wide,
                    block_kw,
                    block_vw,
                    block_dw,
                    inside,
                    place,
                    HW,
                )
                second = head_block(
                    inner[1],
                    part_narrow,
                    query_decay_narrow,
                    block_kn,
                    block_vn,
                    block_dn,
                    inside,
                    place,
                    HN,
                )
                return (first, second)

            def skip(inner):
                return inner

            return lax.cond(inside <= place + half_rows - 1, work, skip, current)

        updated = (one_half(carried[0], halves[0]), one_half(carried[1], halves[1]))
        return (updated, None)

    state, _ = lax.scan(visit, state, jnp.arange(span_rows // block_size, dtype=jnp.int32))
    att_wide = jnp.concatenate(
        [finish(state[0][0], half_rows), finish(state[1][0], half_rows)], axis=0
    )
    att_narrow = jnp.concatenate(
        [finish(state[0][1], half_rows), finish(state[1][1], half_rows)], axis=0
    )
    own_rows = residual.shape[0]
    tp_place = lax.axis_index("tp")
    rows_wide = lax.dynamic_slice_in_dim(
        out_wide, tp_place * att_wide.shape[1], att_wide.shape[1], 0
    )
    rows_narrow = lax.dynamic_slice_in_dim(
        out_narrow, tp_place * att_narrow.shape[1], att_narrow.shape[1], 0
    )
    first = jnp.dot(att_wide, rows_wide, preferred_element_type=jnp.float32)
    second = jnp.dot(att_narrow, rows_narrow, preferred_element_type=jnp.float32)
    mixed = lax.psum_scatter(
        (first + second).astype(jnp.bfloat16), "tp", scatter_dimension=0, tiled=True
    ).astype(jnp.float32)
    middle = (residual.astype(jnp.float32) + mixed).astype(jnp.bfloat16)
    middle_wide = middle.astype(jnp.float32)
    spread = jnp.mean(middle_wide * middle_wide, axis=1, keepdims=True)
    normed = (middle_wide * lax.rsqrt(spread + epsilon) * norm_gain).astype(jnp.bfloat16)
    features = normed.shape[1]
    chosen_count = routing.shape[1]
    expert_count = gate_weight.shape[0] * lax.axis_size("sp")
    capacity = own_rows * GROUPS // expert_count
    flat_routes = routing.reshape(-1)
    matches = (flat_routes[:, None] == jnp.arange(expert_count, dtype=jnp.int32)[None, :]).astype(
        jnp.int32
    )
    ranking = jnp.sum((jnp.cumsum(matches, axis=0) - matches) * matches, axis=1)
    placing = flat_routes * capacity + ranking
    picker = (
        placing[None, :] == jnp.arange(expert_count * capacity, dtype=jnp.int32)[:, None]
    ).astype(jnp.bfloat16)
    picker = jnp.sum(picker.reshape(expert_count * capacity, own_rows, chosen_count), axis=2)
    outgoing = jnp.dot(picker, normed, preferred_element_type=jnp.float32).astype(jnp.bfloat16)
    outgoing = outgoing.reshape(expert_count, capacity, features)
    arrived = lax.all_to_all(outgoing, "sp", split_axis=0, concat_axis=0, tiled=True)
    pooled = lax.all_gather(arrived.reshape(-1, features), "tp", axis=0, tiled=True)
    gate_value = jnp.dot(pooled, gate_weight[0], preferred_element_type=jnp.float32)
    up_value = jnp.dot(pooled, up_weight[0], preferred_element_type=jnp.float32)
    hidden = (jax.nn.silu(gate_value) * up_value).astype(jnp.bfloat16)
    answers = lax.psum_scatter(
        jnp.dot(hidden, down_weight[0], preferred_element_type=jnp.float32).astype(jnp.bfloat16),
        "tp",
        scatter_dimension=0,
        tiled=True,
    )
    returned = lax.all_to_all(
        answers.reshape(expert_count, capacity, features),
        "sp",
        split_axis=0,
        concat_axis=0,
        tiled=True,
    )
    picked = jnp.take(returned.reshape(expert_count * capacity, features), placing, axis=0)
    picked = picked.reshape(own_rows, chosen_count, features).astype(jnp.float32)
    combined = jnp.sum(route_weight[:, :, None] * picked, axis=1)
    return (middle_wide + combined).astype(jnp.bfloat16)


CORES = 2
MESH = pl.DeviceIdType.MESH
VMEM = pl.BlockSpec(memory_space=pltpu.VMEM)


def greet(peers):
    barrier = pltpu.get_barrier_semaphore()
    for peer in peers:
        pl.semaphore_signal(barrier, inc=1, device_id=peer, device_id_type=MESH)
    pl.semaphore_wait(barrier, len(peers))


def remote(source, target, send, receive, peer):
    return pltpu.make_async_remote_copy(
        src_ref=source,
        dst_ref=target,
        send_sem=send,
        recv_sem=receive,
        device_id=peer,
        device_id_type=MESH,
    )


DMA = pltpu.SemaphoreType.DMA


SENDS = [0, 1, 2, 3, 4, 5, 6, 7, 8, 8, 8, 8, 9, 10, 10, 10, 10, 10, 10, 11, 12, 9, 10]
TAKES = [0, 1, 2, 3, 4, 5, 6, 6, 7, 7, 7, 7, 8, 9, 11, 10, 11, 11, 11, 12, 8, 9, 10]


LOG2E = math.log2(math.e)


def layer_kernel(outer, inner, ys, *refs):
    gate_w, gate_n, chosen, shares, qw, kw, vw, qn, kn, vn, residual, gain = refs[:12]
    out_wide, out_narrow, gate_hbm, up_hbm, down_hbm, result = refs[12:18]
    refs = refs[3:]
    kws, vws, kns, vns, far, run, peak, total, acc_w, acc_n, att, swapped = refs[15:27]
    wide_w, narrow_w, gate, up, down, middle, outgoing, returned = refs[27:35]
    pooled, answers, half, chip_a, chip_b, from_x, from_y, next_a, next_b = refs[35:44]
    last_a, last_b, final, picker, board, factor = refs[44:50]
    hidden, hidden_in, parts_own, parts_in, both, from_both, ended = refs[50:57]
    load, lift_s, lift_r, cross_s, cross_r, turn_s, turn_r = refs[57:64]
    far_s, far_r, swap_s, swap_r, give_s, give_r, send, take = refs[64:]
    place, tp = lax.axis_index("sp"), lax.axis_index("tp")
    o, i, y, c = place // inner, place % inner, tp // CORES, tp % CORES
    far_i, far_y, far_c = (i + 1) % inner, (y + 1) % ys, (c + 1) % CORES
    places, parts = outer * inner, ys * CORES
    rows, wide = qw.shape
    narrow = qn.shape[1]
    heads = 1 + narrow // HN
    own_rows, features = residual.shape
    cap = outgoing.shape[1]
    h = cap // 2
    low, high = pl.ds(0, h), pl.ds(h, h)
    units = gate.shape[1]
    deep = o >= outer - 2
    final_plane = o == outer - 1
    def at(o_, i_, y_, c_):
        return (o_ * inner + i_, y_ * CORES + c_)

    across, along, mate = at(o, far_i, y, c), at(o, i, far_y, c), at(o, i, y, far_c)

    loads = [
        pltpu.make_async_copy(source, target, load.at[n])
        for n, (source, target) in enumerate(
            [
                (out_wide, wide_w),
                (out_narrow, narrow_w),
                (gate_hbm.at[0], gate),
                (up_hbm.at[0], up),
                (down_hbm.at[0], down.at[y]),
            ]
        )
    ]
    for copy in loads:
        copy.start()
    far[...] = jnp.zeros_like(far)
    peers = [((place + d) % places, tp) for d in range(1, places)]
    peers = peers + [(place, (tp + d) % parts) for d in range(1, parts)]
    barrier = pltpu.get_barrier_semaphore()
    for peer in peers:
        pl.semaphore_signal(barrier, inc=1, device_id=peer, device_id_type=MESH)
    picks = chosen.shape[0]
    board[...] = jnp.zeros_like(board)
    board[:1] = gate_w[...]
    board[1:heads] = gate_n[...]
    board[heads : heads + picks, :own_rows] = chosen[...].astype(jnp.float32)
    board[heads + picks : heads + 2 * picks, :own_rows] = shares[...]
    facts = board[...]
    step = jnp.minimum(facts, 0.0) - jnp.log1p(jnp.exp(-jnp.abs(facts)))
    lane = lax.broadcasted_iota(jnp.int32, step.shape, 1)
    shift = 1
    while shift < rows:
        step = step + jnp.where(lane >= shift, pltpu.roll(step, shift, 1), 0.0)
        shift *= 2
    run[...] = step
    near = step * LOG2E
    pl.semaphore_wait(barrier, len(peers))
    for d in range(1, places):

        @pl.when(place + d < places)
        def _(d=d):
            remote(run, far.at[place], far_s.at[d], far_r.at[d], (place + d, tp)).start()

    ins, blocks = (kw, vw, kn, vn), (kws, vws, kns, vns)
    count = len(ins)

    def source_of(t, a):
        slot = (o - t) * inner + i
        return (ins[a] if t == 0 else blocks[a].at[slot]), blocks[a].at[slot]

    def lift(t, a):
        source, target = source_of(t, a)
        return remote(
            source, target, lift_s.at[t, a // 2], lift_r.at[t, a // 2], at(o + 1, i, y, c)
        )

    def cross(t, a):
        source, target = source_of(t, a)
        return remote(source, target, cross_s.at[t, a // 2], cross_r.at[t, a // 2], across)

    def twin(p):
        return blocks[2 * p].at[pl.ds(0, 2)]

    def arrived(where, semaphore):
        remote(where, where, semaphore, semaphore, mate).wait_recv()

    def detour(a):
        slot = blocks[a].at[far_i]
        return remote(slot, slot, turn_s.at[0], turn_r.at[0], at(o + 1, i, y, c))

    def detours(a):
        return a >= count // 2

    def give(p):
        lines = pl.ds(p * units // outer, units // outer)
        target = down.at[y, lines]
        return remote(down_hbm.at[0, lines], target, give_s.at[0], give_r.at[0], along)

    def crosses(t, a):
        if t == 0:
            return jnp.logical_or(i < far_i, o == 0) if detours(a) else i < far_i
        return o > t if detours(a) else o >= t

    for a in range(count):

        @pl.when(o + 1 < outer)
        def _(a=a):
            lift(0, a).start()

        @pl.when(crosses(0, a))
        def _(a=a):
            cross(0, a).start()

    for p in range(outer):
        pl.when(deep if p < outer - 1 else final_plane)(lambda: give(p).start())

    head_lane = lax.broadcasted_iota(jnp.int32, (rows, narrow), 1) // HN

    def attend(block_of, decay, diagonal):
        columns = jnp.transpose(decay * LOG2E)
        for n in range(heads):
            k, v = (block_of(0), block_of(1)) if n == 0 else (block_of(2), block_of(3))
            if n == 0:
                q, size = qw[...], HW
            else:
                q, size = jnp.where(head_lane == n - 1, qn[...], jnp.zeros_like(qn[...])), HN
            s = lax.dot_general(k, q, (((1,), (1,)), ((), ())), preferred_element_type=jnp.float32)
            s = s * (LOG2E * size ** (-0.5)) - columns[:, n : n + 1]
            if diagonal:
                key = lax.broadcasted_iota(jnp.int32, s.shape, 0)
                query = lax.broadcasted_iota(jnp.int32, s.shape, 1)
                s = jnp.where(key <= query, s, -jnp.inf)
            row = near[n : n + 1]
            new = jnp.max(s, axis=0, keepdims=True) + row
            if not diagonal:
                before = peak[n : n + 1]
                new = jnp.maximum(new, before)
            weights = jnp.exp2(s - (new - row))
            mass = jnp.sum(weights, axis=0, keepdims=True)
            part = lax.dot_general(
                v if n == 0 else v[:, (n - 1) * HN : n * HN],
                weights.astype(jnp.bfloat16),
                (((0,), (0,)), ((), ())),
                preferred_element_type=jnp.float32,
            )
            acc = acc_w if n == 0 else acc_n.at[(n - 1) * HN : n * HN]
            if diagonal:
                total[n : n + 1] = mass
                acc[...] = part
            else:
                shrink = jnp.exp2(before - new)
                total[n : n + 1] = total[n : n + 1] * shrink + mass
                acc[...] = acc[...] * shrink + part
            peak[n : n + 1] = new

    attend(lambda a: ins[a][...], step, True)
    columns = jnp.transpose(facts)[:own_rows]

    def group_of(names):
        return jnp.floor((names + 0.5) / inner)

    group = group_of(facts[heads : heads + 1, :own_rows])
    ahead = lax.broadcasted_iota(jnp.int32, (own_rows, own_rows), 0)
    ahead = ahead < lax.broadcasted_iota(jnp.int32, (own_rows, own_rows), 1)
    same = jnp.logical_and(group_of(columns[:, heads : heads + 1]) == group, ahead)
    placing = group * cap + jnp.sum(jnp.where(same, 1.0, 0.0), axis=0, keepdims=True)
    slots = lax.broadcasted_iota(jnp.int32, (GROUPS * cap, own_rows), 0).astype(jnp.float32)
    picker[...] = jnp.where(slots == placing, 1.0, 0.0).astype(jnp.bfloat16)
    lane = lax.broadcasted_iota(jnp.int32, (own_rows, outgoing.shape[2] - features), 1)
    extra = jnp.zeros(lane.shape, jnp.float32)
    for e in range(inner):
        weight = jnp.zeros((own_rows, 1), jnp.float32)
        for k in range(picks):
            name = columns[:, heads + k : heads + k + 1]
            value = columns[:, heads + picks + k : heads + picks + k + 1]
            weight = weight + jnp.where(name - inner * group_of(name) == e, value, 0.0)
        top = weight.astype(jnp.bfloat16).astype(jnp.float32)
        extra = jnp.where(lane == 2 * e, top, extra)
        extra = jnp.where(lane == 2 * e + 1, weight - top, extra)
    part = jnp.dot(picker[...], extra.astype(jnp.bfloat16), preferred_element_type=jnp.float32)
    outgoing[:, :, features:] = part.astype(jnp.bfloat16).reshape(GROUPS, cap, lane.shape[1])

    for d in range(1, places):

        @pl.when(place >= d)
        def _(d=d):
            arrived(far.at[place - d], far_r.at[d])

    def visit(slot):
        offset = jnp.zeros((far.shape[1], 1), jnp.float32)
        for b in range(places):
            inside = jnp.logical_and(b >= slot, b < place)
            offset = offset + jnp.where(inside, far[b, :, rows - 1 : rows], 0.0)
        attend(lambda a: blocks[a][slot], far[slot] - offset, False)

    def relay(t):
        @pl.when(o >= t)
        def _():
            for p in range(count // 2):
                arrived(twin(p), lift_r.at[t - 1, p])
                for a in (2 * p, 2 * p + 1):
                    if t < outer - 1:
                        pl.when(o + 1 < outer)(lambda: lift(t, a).start())
                    pl.when(crosses(t, a))(lambda: cross(t, a).start())

    def own(t):
        @pl.when(o >= t)
        def _():
            visit((o - t) * inner + i)

    def other(t):
        slot = (o - t) * inner + far_i
        needed = (o >= t) if t > 0 else (far_i < i)
        pl.when(needed)(lambda: arrived(twin(0), cross_r.at[t, 0]))
        if t > 0:
            pl.when(o > t)(lambda: arrived(twin(1), cross_r.at[t, 1]))
            pl.when(o == t)(lambda: arrived(twin(1), turn_r.at[0]))
        else:
            pl.when(jnp.logical_or(needed, o == 0))(lambda: arrived(twin(1), cross_r.at[t, 1]))
        if t < outer - 1:
            for a in range(count // 2, count):
                pl.when(o == t)(lambda: detour(a).start())

        @pl.when((o >= t) if t > 0 else (far_i < i))
        def _():
            visit(slot)

    def finish():
        mixed = jnp.transpose(acc_w[...] / total[0:1]).astype(jnp.bfloat16)
        att[:, :, :wide] = mixed.reshape(parts, own_rows, wide)
        for n in range(1, heads):
            piece = slice((n - 1) * HN, n * HN)
            acc_n[piece] = acc_n[piece] / total[n : n + 1]
        mixed = jnp.transpose(acc_n[...]).astype(jnp.bfloat16)
        att[:, :, wide:] = mixed.reshape(parts, own_rows, narrow)
        for d in range(1, parts):
            swap(d).start()
        swapped[tp] = att[tp]

    def swap(d):
        k = (tp + d) % parts
        return remote(att.at[k], swapped.at[tp], swap_s.at[0], swap_r.at[0], (place, k))

    def settle():
        arrived(swapped.at[pl.ds(0, parts - 1)], swap_r.at[0])

    tile = math.gcd(features, 512)

    def project():
        rows_w = jnp.concatenate([swapped[p, :, :wide] for p in range(parts)], axis=1)
        rows_n = jnp.concatenate([swapped[p, :, wide:] for p in range(parts)], axis=1)
        squares = jnp.zeros((own_rows, 1), jnp.float32)
        for n in range(features // tile):
            at_n = pl.ds(n * tile, tile)
            part = jnp.dot(rows_w, wide_w[:, at_n], preferred_element_type=jnp.float32)
            part = part + jnp.dot(rows_n, narrow_w[:, at_n], preferred_element_type=jnp.float32)
            part = (residual[:, at_n].astype(jnp.float32) + part).astype(jnp.bfloat16)
            middle[:, at_n] = part
            part = part.astype(jnp.float32)
            squares = squares + jnp.sum(part * part, axis=1, keepdims=True)
        factor[...] = lax.rsqrt(squares / features + epsilon)

    def ready():
        for n in range(features // tile):
            at_n = pl.ds(n * tile, tile)
            part = middle[:, at_n].astype(jnp.float32) * factor[...] * gain[:, at_n]
            part = jnp.dot(
                picker[...], part.astype(jnp.bfloat16), preferred_element_type=jnp.float32
            )
            outgoing[:, :, at_n] = part.astype(jnp.bfloat16).reshape(GROUPS, cap, tile)

    def route(kind, t):
        mine, beside = pooled.at[t, c, i, y], pooled.at[t, c, far_i, y]
        below, corners = pooled.at[t, c, i, far_y], pooled.at[t, c, far_i, far_y]
        if kind == 0:
            return outgoing.at[t, low], pooled.at[o, c, i, y, low], at(t, i, y, c)
        if kind == 1:
            return outgoing.at[t, high], pooled.at[o, c, i, y, high], at(t, i, y, c)
        if kind == 2:
            return mine.at[low], mine.at[low], across
        if kind == 3:
            return mine.at[high], mine.at[high], across
        if kind == 4:
            return mine.at[low], mine.at[low], along
        if kind == 5:
            return mine.at[high], mine.at[high], along
        if kind == 6:
            return beside.at[low], beside.at[low], along
        if kind == 7:
            return below.at[high], below.at[high], across
        if kind in (8, 9, 10, 11):
            slot = (mine, beside, below, corners)[kind - 8]
            return slot, slot, mate
        if kind == 12:
            return answers.at[t, far_c], half.at[t], mate
        if kind == 13:
            return chip_a.at[t, far_i, far_y], from_x.at[t, far_y], across
        if kind == 14:
            return chip_a.at[t, far_i, y], from_x.at[t, y], across
        if kind == 15:
            return chip_b.at[t, far_y, far_i], from_y.at[t, far_i], along
        if kind == 16:
            return chip_b.at[t, far_y, i], from_y.at[t, i], along
        if kind == 17:
            return next_a.at[t], last_a.at[t], along
        if kind == 18:
            return next_b.at[t], last_b.at[t], across
        if kind == 20:
            return hidden.at[t, far_y], hidden_in.at[t], along
        if kind == 21:
            return parts_own.at[t, far_c], parts_in.at[t], mate
        if kind == 22:
            return both.at[t, far_i], from_both.at[t], across
        return final.at[t], returned.at[o], at(t, i, y, c)

    def copy_of(kind, t):
        source, target, peer = route(kind, t)
        mark = o if kind in (0, 1, 19) else t
        return remote(source, target, send.at[SENDS[kind]], take.at[TAKES[kind], mark], peer)

    def push(kind, t):
        if kind in (0, 1, 19):
            pl.when(o != t)(lambda: copy_of(kind, t).start())
        else:
            copy_of(kind, t).start()

    def landed(kind, t, where):
        arrived(where, take.at[TAKES[kind], t])

    def late(t):
        return jnp.logical_and(o + 2 <= t, o < outer - 2)

    def send_rows(t):
        push(0, t)
        push(1, t)

    def dispatch():
        for t in reversed(range(outer)):
            pl.when(jnp.logical_not(late(t)))(lambda: send_rows(t))

        pooled[o, c, i, y] = outgoing[o]

    def begin(t):
        slot = pooled.at[t, c, i, y]

        def hold(kind, part):
            pl.when(o != t)(lambda: landed(kind, t, slot.at[part]))

        hold(0, low)
        push(2, t)
        hold(1, high)
        push(5, t)
        push(3, t)
        push(4, t)
        push(8, t)

    def pass_on(t):
        beside, below = pooled.at[t, c, far_i, y], pooled.at[t, c, i, far_y]
        landed(2, t, beside.at[low])
        push(6, t)
        landed(5, t, below.at[high])
        push(7, t)
        landed(3, t, beside.at[high])
        push(9, t)
        landed(4, t, below.at[low])
        push(10, t)

    def corner(t):
        landed(6, t, pooled.at[t, c, far_i, far_y])
        push(11, t)

    def feed(t):
        landed(8, t, pooled.at[t, far_c])
        rows = CORES * inner * ys * cap
        x = pooled[t, :, :, :, :, :features].reshape(rows, features)
        extra = pooled[t, :, :, :, :, features:].reshape(rows, -1).astype(jnp.float32)
        lane = lax.broadcasted_iota(jnp.int32, extra.shape, 1)
        scale = jnp.sum(jnp.where(lane // 2 == i, extra, 0.0), axis=1, keepdims=True)
        g = jnp.dot(x, gate[...], preferred_element_type=jnp.float32)
        u = jnp.dot(x, up[...], preferred_element_type=jnp.float32)
        made = (jax.nn.silu(g) * u).astype(jnp.bfloat16)
        wide = math.gcd(features, 512)
        for n in range(features // wide):
            columns = pl.ds(n * wide, wide)
            part = jnp.dot(made, down[y, :, columns], preferred_element_type=jnp.float32)
            answers[t, :, :, :, :, columns] = (
                (part * scale).astype(jnp.bfloat16).reshape(CORES, inner, ys, cap, wide)
            )
        push(12, t)

    def gather(t):
        landed(12, t, half.at[t])
        for i_ in range(inner):
            for y_ in range(ys):
                total = answers[t, c, i_, y_].astype(jnp.float32)
                total = (total + half[t, i_, y_].astype(jnp.float32)).astype(jnp.bfloat16)
                chip_a[t, i_, y_] = total[:h]
                chip_b[t, y_, i_] = total[h:]
        push(13, t)
        push(15, t)
        push(14, t)
        push(16, t)

    def add(*parts):
        total = parts[0].astype(jnp.float32)
        for part in parts[1:]:
            total = total + part.astype(jnp.float32)
        return total.astype(jnp.bfloat16)

    def turn(t):
        landed(13, t, from_x.at[t, far_y])
        next_a[t] = add(chip_a[t, i, far_y], from_x[t, far_y])
        push(17, t)
        landed(15, t, from_y.at[t, far_i])
        next_b[t] = add(chip_b[t, y, far_i], from_y[t, far_i])
        push(18, t)

    def home(t):
        landed(14, t, chip_a.at[t])
        final[t, :h] = add(chip_a[t, i, y], from_x[t, y], last_a[t])
        final[t, h:] = add(chip_b[t, y, i], from_y[t, i], last_b[t])
        push(19, t)

    def enter(t):
        landed(8, t, pooled.at[t, far_c])
        x = pooled[t, :, :, :, :, :features].reshape(CORES * inner * ys * cap, features)
        g = jnp.dot(x, gate[...], preferred_element_type=jnp.float32)
        u = jnp.dot(x, up[...], preferred_element_type=jnp.float32)
        made = (jax.nn.silu(g) * u).astype(jnp.bfloat16)
        made = made.reshape(CORES, inner, ys, cap, units)
        for y_ in range(ys):
            hidden[t, y_] = made[:, :, y_]
        push(20, t)

    def complete():
        arrived(down.at[far_y], give_r.at[0])

    def mix(t):
        landed(20, t, hidden_in.at[t])
        lines = CORES * inner * cap
        extra = pooled[t, :, :, y, :, features:].reshape(lines, -1).astype(jnp.float32)
        lane = lax.broadcasted_iota(jnp.int32, extra.shape, 1)
        scale = jnp.sum(jnp.where(lane // 2 == i, extra, 0.0), axis=1, keepdims=True)
        mine = hidden[t, y].reshape(lines, units)
        theirs = hidden_in[t].reshape(lines, units)
        for n in range(features // tile):
            at_n = pl.ds(n * tile, tile)
            part = jnp.dot(mine, down[y, :, at_n], preferred_element_type=jnp.float32)
            part = part + jnp.dot(theirs, down[far_y, :, at_n], preferred_element_type=jnp.float32)
            parts_own[t, :, :, :, at_n] = (
                (part * scale).astype(jnp.bfloat16).reshape(CORES, inner, cap, tile)
            )
        push(21, t)

    def pair(t):
        landed(21, t, parts_in.at[t])
        both[t] = add(parts_own[t, c], parts_in[t])
        push(22, t)

    def leave(t):
        landed(22, t, from_both.at[t])
        final[t] = add(both[t, i], from_both[t])
        push(19, t)

    relay(1)
    other(0)
    own(1)
    relay(2)
    other(1)
    own(2)
    relay(3)
    other(2)
    own(3)

    other(3)
    finish()

    loads[0].wait()
    loads[1].wait()
    settle()
    pl.when(o == outer - 2)(lambda: give(outer - 1).start())
    project()
    ready()
    dispatch()
    for copy in loads[2:]:
        copy.wait()

    @pl.when(deep)
    def _():
        begin(0)
        begin(1)
        pass_on(0)
        begin(2)
        begin(3)
        pass_on(1)
        corner(0)
        enter(0)
        complete()
        pass_on(2)
        corner(1)
        mix(0)
        enter(1)
        pass_on(3)
        pair(0)
        corner(2)
        enter(2)
        mix(1)
        pair(1)
        corner(3)
        mix(2)
        enter(3)
        leave(0)
        pair(2)
        mix(3)
        leave(1)
        pair(3)
        leave(2)
        leave(3)

    @pl.when(jnp.logical_not(deep))
    def _():
        begin(0)
        pass_on(0)
        for t in range(outer):
            pl.when(late(t))(lambda: send_rows(t))
        begin(1)
        corner(0)
        feed(0)
        pass_on(1)
        gather(0)
        begin(2)
        corner(1)
        feed(1)
        pass_on(2)
        turn(0)
        gather(1)
        begin(3)
        home(0)
        corner(2)
        feed(2)
        pass_on(3)
        turn(1)
        gather(2)
        home(1)
        corner(3)
        feed(3)
        turn(2)
        gather(3)
        home(2)
        turn(3)
        home(3)

    @pl.when(deep)
    def _():
        remote(down.at[y], down.at[y], give_s.at[0], give_r.at[0], mate).wait_send()

    def sent(p, semaphore):
        remote(twin(p), twin(p), semaphore, semaphore, mate).wait_send()

    for t in range(outer):
        for p in range(count // 2):
            if t < outer - 1:
                pl.when(jnp.logical_and(o >= t, o + 1 < outer))(lambda: sent(p, lift_s.at[t, p]))
            pl.when(crosses(t, 2 * p))(lambda: sent(p, cross_s.at[t, p]))

    pl.when(o + 1 < outer)(lambda: sent(1, turn_s.at[0]))

    for d in range(1, places):

        @pl.when(place + d < places)
        def _(d=d):
            remote(run, far.at[place], far_s.at[d], far_r.at[d], (place + d, tp)).wait_send()

    others = att.at[pl.ds(0, parts - 1)]
    remote(others, others, swap_s.at[0], swap_r.at[0], mate).wait_send()

    def returns(t):
        pl.when(o != t)(lambda: landed(19, t, returned.at[t]))

    returned[o] = final[o]
    for t in range(outer):
        returns(t)

    def drain(kind, whole):
        remote(whole, whole, send.at[SENDS[kind]], send.at[SENDS[kind]], mate).wait_send()

    drain(0, outgoing.at[pl.ds(0, outer - 1), low])
    drain(1, outgoing.at[pl.ds(0, outer - 1), high])
    for kind in range(2, 8):
        drain(kind, pooled.at[:, 0, 0, 0, low if kind in (2, 4, 6) else high])
    drain(8, pooled.at[pl.ds(0, outer // 2)])
    drain(19, final.at[pl.ds(0, outer - 1)])

    @pl.when(deep)
    def _():
        drain(20, hidden_in)
        drain(21, parts_in)
        drain(22, from_both)

    @pl.when(jnp.logical_not(deep))
    def _():
        drain(12, half)
        drain(13, half.at[pl.ds(0, 3 * outer // 4)])

    def combine():
        copies = []
        for n in range(features // tile):
            at_n = pl.ds(n * tile, tile)
            slots = returned[:, :, at_n].reshape(GROUPS * cap, tile)
            combined = lax.dot_general(
                picker[...], slots, (((0,), (0,)), ((), ())), preferred_element_type=jnp.float32
            )
            ended[n] = (middle[:, at_n].astype(jnp.float32) + combined).astype(jnp.bfloat16)
            copies.append(pltpu.make_async_copy(ended.at[n], result.at[:, at_n], load.at[5 + n]))
            copies[-1].start()
        for copy in copies:
            copy.wait()

    combine()


def fast_body(
    residual,
    query_wide,
    key_wide,
    value_wide,
    query_narrow,
    key_narrow,
    value_narrow,
    gate_wide,
    gate_narrow,
    out_wide,
    out_narrow,
    norm_gain,
    routing,
    route_weight,
    gate_weight,
    up_weight,
    down_weight,
):
    inner = routing.shape[1]
    places = lax.axis_size("sp")
    outer = places // inner
    parts = lax.axis_size("tp")
    ys = parts // CORES
    own_rows, features = residual.shape
    rows, wide = query_wide.shape
    narrow = query_narrow.shape[1]
    heads = gate_wide.shape[1] + gate_narrow.shape[1]
    lines = pl.cdiv(heads + 2 * inner, 8) * 8
    cap = own_rows * GROUPS // places
    h = cap // 2
    units = down_weight.shape[1]
    tiles = features // math.gcd(features, 512)
    width = features + 128 * pl.cdiv(2 * inner, 128)
    kind, full = jnp.bfloat16, jnp.float32

    def vmem(*shape, dtype=kind):
        return pltpu.VMEM(shape, dtype)

    scratch = [
        vmem(places, rows, wide),
        vmem(places, rows, wide),
        vmem(places, rows, narrow),
        vmem(places, rows, narrow),
        vmem(places, lines, rows, dtype=full),
        vmem(lines, rows, dtype=full),
        vmem(lines, rows, dtype=full),
        vmem(lines, rows, dtype=full),
        vmem(wide, rows, dtype=full),
        vmem(narrow, rows, dtype=full),
        vmem(parts, own_rows, wide + narrow),
        vmem(parts, own_rows, wide + narrow),
        vmem(*out_wide.shape),
        vmem(*out_narrow.shape),
        vmem(*gate_weight.shape[1:]),
        vmem(*up_weight.shape[1:]),
        vmem(ys, units, features),
        vmem(own_rows, features),
        vmem(GROUPS, cap, width),
        vmem(outer, cap, features),
        vmem(outer, CORES, inner, ys, cap, width),
        vmem(outer, CORES, inner, ys, cap, features),
        vmem(outer, inner, ys, cap, features),
        vmem(outer, inner, ys, h, features),
        vmem(outer, ys, inner, h, features),
        vmem(outer, ys, h, features),
        vmem(outer, inner, h, features),
        vmem(outer, h, features),
        vmem(outer, h, features),
        vmem(outer, h, features),
        vmem(outer, h, features),
        vmem(outer, cap, features),
        vmem(GROUPS * cap, own_rows),
        vmem(lines, rows, dtype=full),
        vmem(own_rows, 1, dtype=full),
        vmem(outer, ys, CORES, inner, cap, units),
        vmem(outer, CORES, inner, cap, units),
        vmem(outer, CORES, inner, cap, features),
        vmem(outer, inner, cap, features),
        vmem(outer, inner, cap, features),
        vmem(outer, cap, features),
        vmem(tiles, own_rows, features // tiles),
        DMA((5 + tiles,)),
        DMA((outer - 1, 2)),
        DMA((outer - 1, 2)),
        DMA((outer, 2)),
        DMA((outer, 2)),
        DMA((1,)),
        DMA((1,)),
        DMA((places,)),
        DMA((places,)),
        DMA((1,)),
        DMA((1,)),
        DMA((1,)),
        DMA((1,)),
        DMA((1 + max(SENDS),)),
        DMA((1 + max(TAKES), outer)),
    ]
    anywhere = pl.BlockSpec(memory_space=pl.ANY)
    return pl.pallas_call(
        functools.partial(layer_kernel, outer, inner, ys),
        out_shape=jax.ShapeDtypeStruct(residual.shape, residual.dtype),
        in_specs=[VMEM] * 12 + [anywhere] * 5,
        out_specs=anywhere,
        scratch_shapes=scratch,
        compiler_params=pltpu.CompilerParams(
            collective_id=1, has_side_effects=True, vmem_limit_bytes=56 * 1024 * 1024
        ),
    )(
        gate_wide.T,
        gate_narrow.T,
        routing.T,
        route_weight.T,
        query_wide,
        key_wide,
        value_wide,
        query_narrow,
        key_narrow,
        value_narrow,
        residual,
        norm_gain[None, :],
        out_wide,
        out_narrow,
        gate_weight,
        up_weight,
        down_weight,
    )


def choose(*args):
    routing, gate_weight = args[12], args[14]
    experts = gate_weight.shape[0] * lax.axis_size("sp")
    paired = lax.axis_size("tp") == 2 * CORES and gate_weight.shape[0] == 1
    paired = paired and routing.shape[1] == 2
    if paired and experts == GROUPS * routing.shape[1]:
        return fast_body(*args)
    return body(*args)


def solution(mesh):
    placed = (
        P(("sp", "tp"), None),
        P("sp", "tp"),
        P("sp", "tp"),
        P("sp", "tp"),
        P("sp", "tp"),
        P("sp", "tp"),
        P("sp", "tp"),
        P("sp", "tp"),
        P("sp", "tp"),
        P(),
        P(),
        P(),
        P(("sp", "tp"), None),
        P(("sp", "tp"), None),
        P("sp", None, "tp"),
        P("sp", None, "tp"),
        P("sp", "tp", None),
    )
    return jax.shard_map(
        choose, mesh=mesh, in_specs=placed, out_specs=P(("sp", "tp"), None), check_vma=False
    )
```

```python
import functools
import math

import jax
import jax.numpy as jnp
from jax import lax
from jax.experimental import pallas as pl
from jax.experimental.pallas import tpu as pltpu
from jax.sharding import PartitionSpec as P

HW = 128
HN = 64
GROUPS = 4


epsilon = 1e-06


def globalize(pieces, shard_rows):
    shards = pieces.shape[0] // shard_rows
    grid = pieces.reshape(shards, shard_rows, pieces.shape[1])
    endings = grid[:, -1, :]
    offsets = jnp.cumsum(endings, axis=0) - endings
    return (grid + offsets[:, None, :]).reshape(pieces.shape)


def head_block(
    state, queries, query_decay, keys, values, key_decay, first_key, first_query, head_width
):
    highest_old, weight_sum, weighted = state
    query_rows = queries.shape[0]
    head_count = query_decay.shape[1]
    key_rows = keys.shape[0]
    grid_query = queries.reshape(query_rows, head_count, head_width)
    grid_key = keys.reshape(key_rows, head_count, head_width)
    grid_value = values.reshape(key_rows, head_count, head_width)
    scores = jnp.einsum("thd,phd->htp", grid_query, grid_key, preferred_element_type=jnp.float32)
    scores = scores * head_width ** (-0.5) + query_decay.T[:, :, None] - key_decay.T[:, None, :]
    query_place = first_query + jnp.arange(query_rows, dtype=jnp.int32)
    key_place = first_key + jnp.arange(key_rows, dtype=jnp.int32)
    scores = jnp.where(key_place[None, None, :] <= query_place[None, :, None], scores, -jnp.inf)
    highest = jnp.maximum(highest_old, jnp.max(scores, axis=2))
    weights = jnp.exp(scores - highest[:, :, None])
    shrink = jnp.exp(highest_old - highest)
    weight_sum = weight_sum * shrink + jnp.sum(weights, axis=2)
    product = jnp.einsum(
        "htp,phd->htd", weights.astype(jnp.bfloat16), grid_value, preferred_element_type=jnp.float32
    )
    weighted = weighted * shrink[:, :, None] + product
    return (highest, weight_sum, weighted)


def fresh_state(head_count, shard_rows, head_width):
    return (
        jnp.full((head_count, shard_rows), -1e30, jnp.float32),
        jnp.zeros((head_count, shard_rows), jnp.float32),
        jnp.zeros((head_count, shard_rows, head_width), jnp.float32),
    )


def finish(state, shard_rows):
    highest, weight_sum, weighted = state
    mixed_heads = weighted / weight_sum[:, :, None]
    joined = jnp.transpose(mixed_heads, (1, 0, 2))
    return joined.reshape(shard_rows, weighted.shape[0] * weighted.shape[2]).astype(jnp.bfloat16)


def body(
    residual,
    query_wide,
    key_wide,
    value_wide,
    query_narrow,
    key_narrow,
    value_narrow,
    gate_wide,
    gate_narrow,
    out_wide,
    out_narrow,
    norm_gain,
    routing,
    route_weight,
    gate_weight,
    up_weight,
    down_weight,
):
    shard_rows = query_wide.shape[0]
    half_rows = shard_rows // 2
    sp_place = lax.axis_index("sp")
    first_query = sp_place * shard_rows
    running_wide = jnp.cumsum(jax.nn.log_sigmoid(gate_wide), axis=0)
    running_narrow = jnp.cumsum(jax.nn.log_sigmoid(gate_narrow), axis=0)
    pieces_wide, pieces_narrow = (
        lax.all_gather(running_wide, "sp", axis=0, tiled=True),
        lax.all_gather(running_narrow, "sp", axis=0, tiled=True),
    )
    every_wide = globalize(pieces_wide, shard_rows)
    every_narrow = globalize(pieces_narrow, shard_rows)
    late_first = first_query + half_rows
    halves = []
    for place, part_wide, part_narrow in (
        (first_query, query_wide[:half_rows], query_narrow[:half_rows]),
        (late_first, query_wide[half_rows:], query_narrow[half_rows:]),
    ):
        halves.append(
            (
                place,
                part_wide,
                part_narrow,
                lax.dynamic_slice_in_dim(every_wide, place, half_rows, 0),
                lax.dynamic_slice_in_dim(every_narrow, place, half_rows, 0),
            )
        )

    def half_state():
        return (
            fresh_state(gate_wide.shape[1], half_rows, HW),
            fresh_state(gate_narrow.shape[1], half_rows, HN),
        )

    state = (half_state(), half_state())
    keys_wide = lax.all_gather(key_wide, "sp", axis=0, tiled=True)
    values_wide = lax.all_gather(value_wide, "sp", axis=0, tiled=True)
    keys_narrow = lax.all_gather(key_narrow, "sp", axis=0, tiled=True)
    values_narrow = lax.all_gather(value_narrow, "sp", axis=0, tiled=True)
    span_rows = keys_wide.shape[0]
    block_size = math.gcd(span_rows, 2048)

    def visit(carried, position):
        inside = position * block_size

        def take_block(source):
            return lax.dynamic_slice_in_dim(source, inside, block_size, 0)

        def take_decay(source):
            return lax.dynamic_slice_in_dim(source, inside, block_size, 0)

        block_kw = take_block(keys_wide)
        block_vw = take_block(values_wide)
        block_kn = take_block(keys_narrow)
        block_vn = take_block(values_narrow)
        block_dw = take_decay(every_wide)
        block_dn = take_decay(every_narrow)

        def one_half(current, half):
            place, part_wide, part_narrow, query_decay_wide, query_decay_narrow = half

            def work(inner):
                first = head_block(
                    inner[0],
                    part_wide,
                    query_decay_wide,
                    block_kw,
                    block_vw,
                    block_dw,
                    inside,
                    place,
                    HW,
                )
                second = head_block(
                    inner[1],
                    part_narrow,
                    query_decay_narrow,
                    block_kn,
                    block_vn,
                    block_dn,
                    inside,
                    place,
                    HN,
                )
                return (first, second)

            def skip(inner):
                return inner

            return lax.cond(inside <= place + half_rows - 1, work, skip, current)

        updated = (one_half(carried[0], halves[0]), one_half(carried[1], halves[1]))
        return (updated, None)

    state, _ = lax.scan(visit, state, jnp.arange(span_rows // block_size, dtype=jnp.int32))
    att_wide = jnp.concatenate(
        [finish(state[0][0], half_rows), finish(state[1][0], half_rows)], axis=0
    )
    att_narrow = jnp.concatenate(
        [finish(state[0][1], half_rows), finish(state[1][1], half_rows)], axis=0
    )
    own_rows = residual.shape[0]
    tp_place = lax.axis_index("tp")
    rows_wide = lax.dynamic_slice_in_dim(
        out_wide, tp_place * att_wide.shape[1], att_wide.shape[1], 0
    )
    rows_narrow = lax.dynamic_slice_in_dim(
        out_narrow, tp_place * att_narrow.shape[1], att_narrow.shape[1], 0
    )
    first = jnp.dot(att_wide, rows_wide, preferred_element_type=jnp.float32)
    second = jnp.dot(att_narrow, rows_narrow, preferred_element_type=jnp.float32)
    mixed = lax.psum_scatter(
        (first + second).astype(jnp.bfloat16), "tp", scatter_dimension=0, tiled=True
    ).astype(jnp.float32)
    middle = (residual.astype(jnp.float32) + mixed).astype(jnp.bfloat16)
    middle_wide = middle.astype(jnp.float32)
    spread = jnp.mean(middle_wide * middle_wide, axis=1, keepdims=True)
    normed = (middle_wide * lax.rsqrt(spread + epsilon) * norm_gain).astype(jnp.bfloat16)
    features = normed.shape[1]
    chosen_count = routing.shape[1]
    expert_count = gate_weight.shape[0] * lax.axis_size("sp")
    capacity = own_rows * GROUPS // expert_count
    flat_routes = routing.reshape(-1)
    matches = (flat_routes[:, None] == jnp.arange(expert_count, dtype=jnp.int32)[None, :]).astype(
        jnp.int32
    )
    ranking = jnp.sum((jnp.cumsum(matches, axis=0) - matches) * matches, axis=1)
    placing = flat_routes * capacity + ranking
    picker = (
        placing[None, :] == jnp.arange(expert_count * capacity, dtype=jnp.int32)[:, None]
    ).astype(jnp.bfloat16)
    picker = jnp.sum(picker.reshape(expert_count * capacity, own_rows, chosen_count), axis=2)
    outgoing = jnp.dot(picker, normed, preferred_element_type=jnp.float32).astype(jnp.bfloat16)
    outgoing = outgoing.reshape(expert_count, capacity, features)
    arrived = lax.all_to_all(outgoing, "sp", split_axis=0, concat_axis=0, tiled=True)
    pooled = lax.all_gather(arrived.reshape(-1, features), "tp", axis=0, tiled=True)
    gate_value = jnp.dot(pooled, gate_weight[0], preferred_element_type=jnp.float32)
    up_value = jnp.dot(pooled, up_weight[0], preferred_element_type=jnp.float32)
    hidden = (jax.nn.silu(gate_value) * up_value).astype(jnp.bfloat16)
    answers = lax.psum_scatter(
        jnp.dot(hidden, down_weight[0], preferred_element_type=jnp.float32).astype(jnp.bfloat16),
        "tp",
        scatter_dimension=0,
        tiled=True,
    )
    returned = lax.all_to_all(
        answers.reshape(expert_count, capacity, features),
        "sp",
        split_axis=0,
        concat_axis=0,
        tiled=True,
    )
    picked = jnp.take(returned.reshape(expert_count * capacity, features), placing, axis=0)
    picked = picked.reshape(own_rows, chosen_count, features).astype(jnp.float32)
    combined = jnp.sum(route_weight[:, :, None] * picked, axis=1)
    return (middle_wide + combined).astype(jnp.bfloat16)


CORES = 2
MESH = pl.DeviceIdType.MESH
VMEM = pl.BlockSpec(memory_space=pltpu.VMEM)


def greet(peers):
    barrier = pltpu.get_barrier_semaphore()
    for peer in peers:
        pl.semaphore_signal(barrier, inc=1, device_id=peer, device_id_type=MESH)
    pl.semaphore_wait(barrier, len(peers))


def remote(source, target, send, receive, peer):
    return pltpu.make_async_remote_copy(
        src_ref=source,
        dst_ref=target,
        send_sem=send,
        recv_sem=receive,
        device_id=peer,
        device_id_type=MESH,
    )


DMA = pltpu.SemaphoreType.DMA


SENDS = [0, 1, 2, 3, 4, 5, 6, 7, 8, 8, 8, 8, 9, 10, 10, 10, 10, 10, 10, 11, 12, 9, 10]
TAKES = [0, 1, 2, 3, 4, 5, 6, 6, 7, 7, 7, 7, 8, 9, 11, 10, 11, 11, 11, 12, 8, 9, 10]


LOG2E = math.log2(math.e)


def layer_kernel(outer, inner, ys, *refs):
    gate_w, gate_n, chosen, shares, qw, kw, vw, qn, kn, vn, residual, gain = refs[:12]
    out_wide, out_narrow, gate_hbm, up_hbm, down_hbm, result = refs[12:18]
    refs = refs[3:]
    kws, vws, kns, vns, far, run, peak, total, acc_w, acc_n, att, swapped = refs[15:27]
    wide_w, narrow_w, gate, up, down, middle, outgoing, returned = refs[27:35]
    pooled, answers, half, chip_a, chip_b, from_x, from_y, next_a, next_b = refs[35:44]
    last_a, last_b, final, picker, board, factor = refs[44:50]
    hidden, hidden_in, parts_own, parts_in, both, from_both, ended = refs[50:57]
    load, lift_s, lift_r, cross_s, cross_r, turn_s, turn_r = refs[57:64]
    far_s, far_r, swap_s, swap_r, give_s, give_r, send, take = refs[64:]
    place, tp = lax.axis_index("sp"), lax.axis_index("tp")
    o, i, y, c = place // inner, place % inner, tp // CORES, tp % CORES
    far_i, far_y, far_c = (i + 1) % inner, (y + 1) % ys, (c + 1) % CORES
    places, parts = outer * inner, ys * CORES
    rows, wide = qw.shape
    narrow = qn.shape[1]
    heads = 1 + narrow // HN
    own_rows, features = residual.shape
    cap = outgoing.shape[1]
    h = cap // 2
    low, high = pl.ds(0, h), pl.ds(h, h)
    units = gate.shape[1]
    deep = o >= outer - 2
    final_plane = o == outer - 1
    def at(o_, i_, y_, c_):
        return (o_ * inner + i_, y_ * CORES + c_)

    across, along, mate = at(o, far_i, y, c), at(o, i, far_y, c), at(o, i, y, far_c)

    loads = [
        pltpu.make_async_copy(source, target, load.at[n])
        for n, (source, target) in enumerate(
            [
                (out_wide, wide_w),
                (out_narrow, narrow_w),
                (gate_hbm.at[0], gate),
                (up_hbm.at[0], up),
                (down_hbm.at[0], down.at[y]),
            ]
        )
    ]
    for copy in loads:
        copy.start()
    far[...] = jnp.zeros_like(far)
    peers = [((place + d) % places, tp) for d in range(1, places)]
    peers = peers + [(place, (tp + d) % parts) for d in range(1, parts)]
    barrier = pltpu.get_barrier_semaphore()
    for peer in peers:
        pl.semaphore_signal(barrier, inc=1, device_id=peer, device_id_type=MESH)
    picks = chosen.shape[0]
    board[...] = jnp.zeros_like(board)
    board[:1] = gate_w[...]
    board[1:heads] = gate_n[...]
    board[heads : heads + picks, :own_rows] = chosen[...].astype(jnp.float32)
    board[heads + picks : heads + 2 * picks, :own_rows] = shares[...]
    facts = board[...]
    step = jnp.minimum(facts, 0.0) - jnp.log1p(jnp.exp(-jnp.abs(facts)))
    lane = lax.broadcasted_iota(jnp.int32, step.shape, 1)
    shift = 1
    while shift < rows:
        step = step + jnp.where(lane >= shift, pltpu.roll(step, shift, 1), 0.0)
        shift *= 2
    run[...] = step
    near = step * LOG2E
    pl.semaphore_wait(barrier, len(peers))
    for d in range(1, places):

        @pl.when(place + d < places)
        def _(d=d):
            remote(run, far.at[place], far_s.at[d], far_r.at[d], (place + d, tp)).start()

    ins, blocks = (kw, vw, kn, vn), (kws, vws, kns, vns)
    count = len(ins)

    def source_of(t, a):
        slot = (o - t) * inner + i
        return (ins[a] if t == 0 else blocks[a].at[slot]), blocks[a].at[slot]

    def lift(t, a):
        source, target = source_of(t, a)
        return remote(
            source, target, lift_s.at[t, a // 2], lift_r.at[t, a], at(o + 1, i, y, c)
        )

    def cross(t, a):
        source, target = source_of(t, a)
        return remote(source, target, cross_s.at[t, a // 2], cross_r.at[t, a // 2], across)

    def twin(p):
        return blocks[2 * p].at[pl.ds(0, 2)]

    def arrived(where, semaphore):
        remote(where, where, semaphore, semaphore, mate).wait_recv()

    def detour(a):
        slot = blocks[a].at[far_i]
        return remote(slot, slot, turn_s.at[0], turn_r.at[0], at(o + 1, i, y, c))

    def detours(a):
        return a >= count // 2

    def give(p):
        lines = pl.ds(p * units // (2 * outer), units // (2 * outer))
        target = down.at[y, lines]
        return remote(down_hbm.at[0, lines], target, give_s.at[0], give_r.at[0], along)

    def crosses(t, a):
        if t == 0:
            return jnp.logical_or(i < far_i, o == 0) if detours(a) else i < far_i
        return o > t if detours(a) else o >= t

    for a in range(count):

        @pl.when(o + 1 < outer)
        def _(a=a):
            lift(0, a).start()

        @pl.when(crosses(0, a))
        def _(a=a):
            cross(0, a).start()

    for p in range(2 * outer):
        pl.when(deep if p < 2 * outer - 1 else final_plane)(lambda: give(p).start())

    head_lane = lax.broadcasted_iota(jnp.int32, (rows, narrow), 1) // HN

    def attend(block_of, decay, diagonal):
        columns = jnp.transpose(decay * LOG2E)
        for n in range(heads):
            k, v = (block_of(0), block_of(1)) if n == 0 else (block_of(2), block_of(3))
            if n == 0:
                q, size = qw[...], HW
            else:
                q, size = jnp.where(head_lane == n - 1, qn[...], jnp.zeros_like(qn[...])), HN
            s = lax.dot_general(k, q, (((1,), (1,)), ((), ())), preferred_element_type=jnp.float32)
            s = s * (LOG2E * size ** (-0.5)) - columns[:, n : n + 1]
            if diagonal:
                key = lax.broadcasted_iota(jnp.int32, s.shape, 0)
                query = lax.broadcasted_iota(jnp.int32, s.shape, 1)
                s = jnp.where(key <= query, s, -jnp.inf)
            row = near[n : n + 1]
            new = jnp.max(s, axis=0, keepdims=True) + row
            if not diagonal:
                before = peak[n : n + 1]
                new = jnp.maximum(new, before)
            weights = jnp.exp2(s - (new - row))
            mass = jnp.sum(weights, axis=0, keepdims=True)
            part = lax.dot_general(
                v if n == 0 else v[:, (n - 1) * HN : n * HN],
                weights.astype(jnp.bfloat16),
                (((0,), (0,)), ((), ())),
                preferred_element_type=jnp.float32,
            )
            acc = acc_w if n == 0 else acc_n.at[(n - 1) * HN : n * HN]
            if diagonal:
                total[n : n + 1] = mass
                acc[...] = part
            else:
                shrink = jnp.exp2(before - new)
                total[n : n + 1] = total[n : n + 1] * shrink + mass
                acc[...] = acc[...] * shrink + part
            peak[n : n + 1] = new

    attend(lambda a: ins[a][...], step, True)
    columns = jnp.transpose(facts)[:own_rows]

    def group_of(names):
        return jnp.floor((names + 0.5) / inner)

    group = group_of(facts[heads : heads + 1, :own_rows])
    ahead = lax.broadcasted_iota(jnp.int32, (own_rows, own_rows), 0)
    ahead = ahead < lax.broadcasted_iota(jnp.int32, (own_rows, own_rows), 1)
    same = jnp.logical_and(group_of(columns[:, heads : heads + 1]) == group, ahead)
    placing = group * cap + jnp.sum(jnp.where(same, 1.0, 0.0), axis=0, keepdims=True)
    slots = lax.broadcasted_iota(jnp.int32, (GROUPS * cap, own_rows), 0).astype(jnp.float32)
    picker[...] = jnp.where(slots == placing, 1.0, 0.0).astype(jnp.bfloat16)
    lane = lax.broadcasted_iota(jnp.int32, (own_rows, outgoing.shape[2] - features), 1)
    extra = jnp.zeros(lane.shape, jnp.float32)
    for e in range(inner):
        weight = jnp.zeros((own_rows, 1), jnp.float32)
        for k in range(picks):
            name = columns[:, heads + k : heads + k + 1]
            value = columns[:, heads + picks + k : heads + picks + k + 1]
            weight = weight + jnp.where(name - inner * group_of(name) == e, value, 0.0)
        top = weight.astype(jnp.bfloat16).astype(jnp.float32)
        extra = jnp.where(lane == 2 * e, top, extra)
        extra = jnp.where(lane == 2 * e + 1, weight - top, extra)
    part = jnp.dot(picker[...], extra.astype(jnp.bfloat16), preferred_element_type=jnp.float32)
    outgoing[:, :, features:] = part.astype(jnp.bfloat16).reshape(GROUPS, cap, lane.shape[1])

    for d in range(1, places):

        @pl.when(place >= d)
        def _(d=d):
            arrived(far.at[place - d], far_r.at[d])

    def visit(slot):
        offset = jnp.zeros((far.shape[1], 1), jnp.float32)
        for b in range(places):
            inside = jnp.logical_and(b >= slot, b < place)
            offset = offset + jnp.where(inside, far[b, :, rows - 1 : rows], 0.0)
        attend(lambda a: blocks[a][slot], far[slot] - offset, False)

    def relay(t):
        @pl.when(o >= t)
        def _():
            for a in range(count):
                arrived(blocks[a].at[0], lift_r.at[t - 1, a])
                if t < outer - 1:
                    pl.when(o + 1 < outer)(lambda: lift(t, a).start())
                pl.when(crosses(t, a))(lambda: cross(t, a).start())

    def own(t):
        @pl.when(o >= t)
        def _():
            visit((o - t) * inner + i)

    def other(t):
        slot = (o - t) * inner + far_i
        needed = (o >= t) if t > 0 else (far_i < i)
        pl.when(needed)(lambda: arrived(twin(0), cross_r.at[t, 0]))
        if t > 0:
            pl.when(o > t)(lambda: arrived(twin(1), cross_r.at[t, 1]))
            pl.when(o == t)(lambda: arrived(twin(1), turn_r.at[0]))
        else:
            pl.when(jnp.logical_or(needed, o == 0))(lambda: arrived(twin(1), cross_r.at[t, 1]))
        if t < outer - 1:
            for a in range(count // 2, count):
                pl.when(o == t)(lambda: detour(a).start())

        @pl.when((o >= t) if t > 0 else (far_i < i))
        def _():
            visit(slot)

    def finish():
        mixed = jnp.transpose(acc_w[...] / total[0:1]).astype(jnp.bfloat16)
        att[:, :, :wide] = mixed.reshape(parts, own_rows, wide)
        for n in range(1, heads):
            piece = slice((n - 1) * HN, n * HN)
            acc_n[piece] = acc_n[piece] / total[n : n + 1]
        mixed = jnp.transpose(acc_n[...]).astype(jnp.bfloat16)
        att[:, :, wide:] = mixed.reshape(parts, own_rows, narrow)
        for d in range(1, parts):
            swap(d).start()
        swapped[tp] = att[tp]

    def swap(d):
        k = (tp + d) % parts
        return remote(att.at[k], swapped.at[tp], swap_s.at[0], swap_r.at[0], (place, k))

    def settle():
        arrived(swapped.at[pl.ds(0, parts - 1)], swap_r.at[0])

    tile = math.gcd(features, 512)

    def project():
        rows_w = jnp.concatenate([swapped[p, :, :wide] for p in range(parts)], axis=1)
        rows_n = jnp.concatenate([swapped[p, :, wide:] for p in range(parts)], axis=1)
        squares = jnp.zeros((own_rows, 1), jnp.float32)
        for n in range(features // tile):
            at_n = pl.ds(n * tile, tile)
            part = jnp.dot(rows_w, wide_w[:, at_n], preferred_element_type=jnp.float32)
            part = part + jnp.dot(rows_n, narrow_w[:, at_n], preferred_element_type=jnp.float32)
            part = (residual[:, at_n].astype(jnp.float32) + part).astype(jnp.bfloat16)
            middle[:, at_n] = part
            part = part.astype(jnp.float32)
            squares = squares + jnp.sum(part * part, axis=1, keepdims=True)
        factor[...] = lax.rsqrt(squares / features + epsilon)

    def ready():
        for n in range(features // tile):
            at_n = pl.ds(n * tile, tile)
            part = middle[:, at_n].astype(jnp.float32) * factor[...] * gain[:, at_n]
            part = jnp.dot(
                picker[...], part.astype(jnp.bfloat16), preferred_element_type=jnp.float32
            )
            outgoing[:, :, at_n] = part.astype(jnp.bfloat16).reshape(GROUPS, cap, tile)

    def route(kind, t):
        mine, beside = pooled.at[t, c, i, y], pooled.at[t, c, far_i, y]
        below, corners = pooled.at[t, c, i, far_y], pooled.at[t, c, far_i, far_y]
        if kind == 0:
            return outgoing.at[t, low], pooled.at[o, c, i, y, low], at(t, i, y, c)
        if kind == 1:
            return outgoing.at[t, high], pooled.at[o, c, i, y, high], at(t, i, y, c)
        if kind == 2:
            return mine.at[low], mine.at[low], across
        if kind == 3:
            return mine.at[high], mine.at[high], across
        if kind == 4:
            return mine.at[low], mine.at[low], along
        if kind == 5:
            return mine.at[high], mine.at[high], along
        if kind == 6:
            return beside.at[low], beside.at[low], along
        if kind == 7:
            return below.at[high], below.at[high], across
        if kind in (8, 9, 10, 11):
            slot = (mine, beside, below, corners)[kind - 8]
            return slot, slot, mate
        if kind == 12:
            return answers.at[t, far_c], half.at[t], mate
        if kind == 13:
            return chip_a.at[t, far_i, far_y], from_x.at[t, far_y], across
        if kind == 14:
            return chip_a.at[t, far_i, y], from_x.at[t, y], across
        if kind == 15:
            return chip_b.at[t, far_y, far_i], from_y.at[t, far_i], along
        if kind == 16:
            return chip_b.at[t, far_y, i], from_y.at[t, i], along
        if kind == 17:
            return next_a.at[t], last_a.at[t], along
        if kind == 18:
            return next_b.at[t], last_b.at[t], across
        if kind == 20:
            return hidden.at[t, far_y], hidden_in.at[t], along
        if kind == 21:
            return parts_own.at[t, far_c], parts_in.at[t], mate
        if kind == 22:
            return both.at[t, far_i], from_both.at[t], across
        return final.at[t], returned.at[o], at(t, i, y, c)

    def copy_of(kind, t):
        source, target, peer = route(kind, t)
        mark = o if kind in (0, 1, 19) else t
        return remote(source, target, send.at[SENDS[kind]], take.at[TAKES[kind], mark], peer)

    def push(kind, t):
        if kind in (0, 1, 19):
            pl.when(o != t)(lambda: copy_of(kind, t).start())
        else:
            copy_of(kind, t).start()

    def landed(kind, t, where):
        arrived(where, take.at[TAKES[kind], t])

    def late(t):
        return jnp.logical_and(o + 2 <= t, o < outer - 2)

    def send_rows(t):
        push(0, t)
        push(1, t)

    def dispatch():
        for t in reversed(range(outer)):
            pl.when(jnp.logical_not(late(t)))(lambda: send_rows(t))

        pooled[o, c, i, y] = outgoing[o]

    def begin(t):
        slot = pooled.at[t, c, i, y]

        def hold(kind, part):
            pl.when(o != t)(lambda: landed(kind, t, slot.at[part]))

        hold(0, low)
        push(2, t)
        hold(1, high)
        push(5, t)
        push(3, t)
        push(4, t)
        push(8, t)

    def pass_on(t):
        beside, below = pooled.at[t, c, far_i, y], pooled.at[t, c, i, far_y]
        landed(2, t, beside.at[low])
        push(6, t)
        landed(5, t, below.at[high])
        push(7, t)
        landed(3, t, beside.at[high])
        push(9, t)
        landed(4, t, below.at[low])
        push(10, t)

    def corner(t):
        landed(6, t, pooled.at[t, c, far_i, far_y])
        push(11, t)

    def feed(t):
        landed(8, t, pooled.at[t, far_c])
        rows = CORES * inner * ys * cap
        x = pooled[t, :, :, :, :, :features].reshape(rows, features)
        extra = pooled[t, :, :, :, :, features:].reshape(rows, -1).astype(jnp.float32)
        lane = lax.broadcasted_iota(jnp.int32, extra.shape, 1)
        scale = jnp.sum(jnp.where(lane // 2 == i, extra, 0.0), axis=1, keepdims=True)
        g = jnp.dot(x, gate[...], preferred_element_type=jnp.float32)
        u = jnp.dot(x, up[...], preferred_element_type=jnp.float32)
        made = (jax.nn.silu(g) * u).astype(jnp.bfloat16)
        wide = math.gcd(features, 512)
        for n in range(features // wide):
            columns = pl.ds(n * wide, wide)
            part = jnp.dot(made, down[y, :, columns], preferred_element_type=jnp.float32)
            answers[t, :, :, :, :, columns] = (
                (part * scale).astype(jnp.bfloat16).reshape(CORES, inner, ys, cap, wide)
            )
        push(12, t)

    def gather(t):
        landed(12, t, half.at[t])
        for i_ in range(inner):
            for y_ in range(ys):
                total = answers[t, c, i_, y_].astype(jnp.float32)
                total = (total + half[t, i_, y_].astype(jnp.float32)).astype(jnp.bfloat16)
                chip_a[t, i_, y_] = total[:h]
                chip_b[t, y_, i_] = total[h:]
        push(13, t)
        push(15, t)
        push(14, t)
        push(16, t)

    def add(*parts):
        total = parts[0].astype(jnp.float32)
        for part in parts[1:]:
            total = total + part.astype(jnp.float32)
        return total.astype(jnp.bfloat16)

    def turn(t):
        landed(13, t, from_x.at[t, far_y])
        next_a[t] = add(chip_a[t, i, far_y], from_x[t, far_y])
        push(17, t)
        landed(15, t, from_y.at[t, far_i])
        next_b[t] = add(chip_b[t, y, far_i], from_y[t, far_i])
        push(18, t)

    def home(t):
        landed(14, t, chip_a.at[t])
        final[t, :h] = add(chip_a[t, i, y], from_x[t, y], last_a[t])
        final[t, h:] = add(chip_b[t, y, i], from_y[t, i], last_b[t])
        push(19, t)

    def enter(t):
        landed(8, t, pooled.at[t, far_c])
        x = pooled[t, :, :, :, :, :features].reshape(CORES * inner * ys * cap, features)
        g = jnp.dot(x, gate[...], preferred_element_type=jnp.float32)
        u = jnp.dot(x, up[...], preferred_element_type=jnp.float32)
        made = (jax.nn.silu(g) * u).astype(jnp.bfloat16)
        made = made.reshape(CORES, inner, ys, cap, units)
        for y_ in range(ys):
            hidden[t, y_] = made[:, :, y_]
        push(20, t)

    def complete():
        arrived(down.at[far_y], give_r.at[0])

    def mix(t):
        landed(20, t, hidden_in.at[t])
        lines = CORES * inner * cap
        extra = pooled[t, :, :, y, :, features:].reshape(lines, -1).astype(jnp.float32)
        lane = lax.broadcasted_iota(jnp.int32, extra.shape, 1)
        scale = jnp.sum(jnp.where(lane // 2 == i, extra, 0.0), axis=1, keepdims=True)
        mine = hidden[t, y].reshape(lines, units)
        theirs = hidden_in[t].reshape(lines, units)
        for n in range(features // tile):
            at_n = pl.ds(n * tile, tile)
            part = jnp.dot(mine, down[y, :, at_n], preferred_element_type=jnp.float32)
            part = part + jnp.dot(theirs, down[far_y, :, at_n], preferred_element_type=jnp.float32)
            parts_own[t, :, :, :, at_n] = (
                (part * scale).astype(jnp.bfloat16).reshape(CORES, inner, cap, tile)
            )
        push(21, t)

    def pair(t):
        landed(21, t, parts_in.at[t])
        both[t] = add(parts_own[t, c], parts_in[t])
        push(22, t)

    def leave(t):
        landed(22, t, from_both.at[t])
        final[t] = add(both[t, i], from_both[t])
        push(19, t)

    relay(1)
    other(0)
    own(1)
    relay(2)
    other(1)
    own(2)
    relay(3)
    other(2)
    own(3)

    other(3)
    finish()

    loads[0].wait()
    loads[1].wait()
    settle()
    project()
    ready()
    dispatch()
    for copy in loads[2:]:
        copy.wait()

    @pl.when(final_plane)
    def _():
        begin(0)
        begin(3)
        pass_on(0)
        begin(1)
        begin(2)
        pass_on(3)
        corner(0)
        enter(0)
        complete()
        pass_on(1)
        corner(3)
        mix(0)
        enter(3)
        pass_on(2)
        pair(0)
        corner(1)
        enter(1)
        mix(3)
        pair(3)
        corner(2)
        mix(1)
        enter(2)
        leave(0)
        pair(1)
        mix(2)
        leave(3)
        pair(2)
        leave(1)
        leave(2)

    @pl.when(o == outer - 2)
    def _():
        begin(2)
        begin(0)
        pass_on(2)
        pass_on(0)
        give(2 * outer - 1).start()
        corner(2)
        enter(2)
        begin(3)
        begin(1)
        complete()
        pass_on(3)
        corner(0)
        mix(2)
        enter(0)
        pass_on(1)
        pair(2)
        corner(3)
        enter(3)
        mix(0)
        pair(0)
        corner(1)
        mix(3)
        enter(1)
        leave(2)
        pair(3)
        mix(1)
        leave(0)
        pair(1)
        leave(3)
        leave(1)

    @pl.when(jnp.logical_not(deep))
    def _():
        begin(0)
        pass_on(0)
        for t in range(outer):
            pl.when(late(t))(lambda: send_rows(t))
        begin(1)
        corner(0)
        feed(0)
        pass_on(1)
        gather(0)
        begin(2)
        corner(1)
        feed(1)
        pl.when(o == outer - 3)(lambda: begin(3))
        pass_on(2)
        turn(0)
        gather(1)
        corner(2)
        feed(2)
        pl.when(o == outer - 4)(lambda: begin(3))
        pass_on(3)
        home(0)
        turn(1)
        gather(2)
        corner(3)
        feed(3)
        home(1)
        turn(2)
        gather(3)
        home(2)
        turn(3)
        home(3)

    @pl.when(deep)
    def _():
        remote(down.at[y], down.at[y], give_s.at[0], give_r.at[0], mate).wait_send()

    def sent(p, semaphore):
        remote(twin(p), twin(p), semaphore, semaphore, mate).wait_send()

    for t in range(outer):
        for p in range(count // 2):
            if t < outer - 1:
                pl.when(jnp.logical_and(o >= t, o + 1 < outer))(lambda: sent(p, lift_s.at[t, p]))
            pl.when(crosses(t, 2 * p))(lambda: sent(p, cross_s.at[t, p]))

    pl.when(o + 1 < outer)(lambda: sent(1, turn_s.at[0]))

    for d in range(1, places):

        @pl.when(place + d < places)
        def _(d=d):
            remote(run, far.at[place], far_s.at[d], far_r.at[d], (place + d, tp)).wait_send()

    others = att.at[pl.ds(0, parts - 1)]
    remote(others, others, swap_s.at[0], swap_r.at[0], mate).wait_send()

    def returns(t):
        pl.when(o != t)(lambda: landed(19, t, returned.at[t]))

    returned[o] = final[o]
    for t in range(outer):
        returns(t)

    def drain(kind, whole):
        remote(whole, whole, send.at[SENDS[kind]], send.at[SENDS[kind]], mate).wait_send()

    drain(0, outgoing.at[pl.ds(0, outer - 1), low])
    drain(1, outgoing.at[pl.ds(0, outer - 1), high])
    for kind in range(2, 8):
        drain(kind, pooled.at[:, 0, 0, 0, low if kind in (2, 4, 6) else high])
    drain(8, pooled.at[pl.ds(0, outer // 2)])
    drain(19, final.at[pl.ds(0, outer - 1)])

    @pl.when(deep)
    def _():
        drain(20, hidden_in)
        drain(21, parts_in)
        drain(22, from_both)

    @pl.when(jnp.logical_not(deep))
    def _():
        drain(12, half)
        drain(13, half.at[pl.ds(0, 3 * outer // 4)])

    def combine():
        copies = []
        for n in range(features // tile):
            at_n = pl.ds(n * tile, tile)
            slots = returned[:, :, at_n].reshape(GROUPS * cap, tile)
            combined = lax.dot_general(
                picker[...], slots, (((0,), (0,)), ((), ())), preferred_element_type=jnp.float32
            )
            ended[n] = (middle[:, at_n].astype(jnp.float32) + combined).astype(jnp.bfloat16)
            copies.append(pltpu.make_async_copy(ended.at[n], result.at[:, at_n], load.at[5 + n]))
            copies[-1].start()
        for copy in copies:
            copy.wait()

    combine()


def fast_body(
    residual,
    query_wide,
    key_wide,
    value_wide,
    query_narrow,
    key_narrow,
    value_narrow,
    gate_wide,
    gate_narrow,
    out_wide,
    out_narrow,
    norm_gain,
    routing,
    route_weight,
    gate_weight,
    up_weight,
    down_weight,
):
    inner = routing.shape[1]
    places = lax.axis_size("sp")
    outer = places // inner
    parts = lax.axis_size("tp")
    ys = parts // CORES
    own_rows, features = residual.shape
    rows, wide = query_wide.shape
    narrow = query_narrow.shape[1]
    heads = gate_wide.shape[1] + gate_narrow.shape[1]
    lines = pl.cdiv(heads + 2 * inner, 8) * 8
    cap = own_rows * GROUPS // places
    h = cap // 2
    units = down_weight.shape[1]
    tiles = features // math.gcd(features, 512)
    width = features + 128 * pl.cdiv(2 * inner, 128)
    kind, full = jnp.bfloat16, jnp.float32

    def vmem(*shape, dtype=kind):
        return pltpu.VMEM(shape, dtype)

    scratch = [
        vmem(places, rows, wide),
        vmem(places, rows, wide),
        vmem(places, rows, narrow),
        vmem(places, rows, narrow),
        vmem(places, lines, rows, dtype=full),
        vmem(lines, rows, dtype=full),
        vmem(lines, rows, dtype=full),
        vmem(lines, rows, dtype=full),
        vmem(wide, rows, dtype=full),
        vmem(narrow, rows, dtype=full),
        vmem(parts, own_rows, wide + narrow),
        vmem(parts, own_rows, wide + narrow),
        vmem(*out_wide.shape),
        vmem(*out_narrow.shape),
        vmem(*gate_weight.shape[1:]),
        vmem(*up_weight.shape[1:]),
        vmem(ys, units, features),
        vmem(own_rows, features),
        vmem(GROUPS, cap, width),
        vmem(outer, cap, features),
        vmem(outer, CORES, inner, ys, cap, width),
        vmem(outer, CORES, inner, ys, cap, features),
        vmem(outer, inner, ys, cap, features),
        vmem(outer, inner, ys, h, features),
        vmem(outer, ys, inner, h, features),
        vmem(outer, ys, h, features),
        vmem(outer, inner, h, features),
        vmem(outer, h, features),
        vmem(outer, h, features),
        vmem(outer, h, features),
        vmem(outer, h, features),
        vmem(outer, cap, features),
        vmem(GROUPS * cap, own_rows),
        vmem(lines, rows, dtype=full),
        vmem(own_rows, 1, dtype=full),
        vmem(outer, ys, CORES, inner, cap, units),
        vmem(outer, CORES, inner, cap, units),
        vmem(outer, CORES, inner, cap, features),
        vmem(outer, inner, cap, features),
        vmem(outer, inner, cap, features),
        vmem(outer, cap, features),
        vmem(tiles, own_rows, features // tiles),
        DMA((5 + tiles,)),
        DMA((outer - 1, 2)),
        DMA((outer - 1, 4)),
        DMA((outer, 2)),
        DMA((outer, 2)),
        DMA((1,)),
        DMA((1,)),
        DMA((places,)),
        DMA((places,)),
        DMA((1,)),
        DMA((1,)),
        DMA((1,)),
        DMA((1,)),
        DMA((1 + max(SENDS),)),
        DMA((1 + max(TAKES), outer)),
    ]
    anywhere = pl.BlockSpec(memory_space=pl.ANY)
    return pl.pallas_call(
        functools.partial(layer_kernel, outer, inner, ys),
        out_shape=jax.ShapeDtypeStruct(residual.shape, residual.dtype),
        in_specs=[VMEM] * 12 + [anywhere] * 5,
        out_specs=anywhere,
        scratch_shapes=scratch,
        compiler_params=pltpu.CompilerParams(
            collective_id=1, has_side_effects=True, vmem_limit_bytes=56 * 1024 * 1024
        ),
    )(
        gate_wide.T,
        gate_narrow.T,
        routing.T,
        route_weight.T,
        query_wide,
        key_wide,
        value_wide,
        query_narrow,
        key_narrow,
        value_narrow,
        residual,
        norm_gain[None, :],
        out_wide,
        out_narrow,
        gate_weight,
        up_weight,
        down_weight,
    )


def choose(*args):
    routing, gate_weight = args[12], args[14]
    experts = gate_weight.shape[0] * lax.axis_size("sp")
    paired = lax.axis_size("tp") == 2 * CORES and gate_weight.shape[0] == 1
    paired = paired and routing.shape[1] == 2
    if paired and experts == GROUPS * routing.shape[1]:
        return fast_body(*args)
    return body(*args)


def solution(mesh):
    placed = (
        P(("sp", "tp"), None),
        P("sp", "tp"),
        P("sp", "tp"),
        P("sp", "tp"),
        P("sp", "tp"),
        P("sp", "tp"),
        P("sp", "tp"),
        P("sp", "tp"),
        P("sp", "tp"),
        P(),
        P(),
        P(),
        P(("sp", "tp"), None),
        P(("sp", "tp"), None),
        P("sp", None, "tp"),
        P("sp", None, "tp"),
        P("sp", "tp", None),
    )
    return jax.shard_map(
        choose, mesh=mesh, in_specs=placed, out_specs=P(("sp", "tp"), None), check_vma=False
    )
```

```python
import functools
import math

import jax
import jax.numpy as jnp
from jax import lax
from jax.experimental import pallas as pl
from jax.experimental.pallas import tpu as pltpu
from jax.sharding import PartitionSpec as P

HW = 128
HN = 64
GROUPS = 4


epsilon = 1e-06


def globalize(pieces, shard_rows):
    shards = pieces.shape[0] // shard_rows
    grid = pieces.reshape(shards, shard_rows, pieces.shape[1])
    endings = grid[:, -1, :]
    offsets = jnp.cumsum(endings, axis=0) - endings
    return (grid + offsets[:, None, :]).reshape(pieces.shape)


def head_block(
    state, queries, query_decay, keys, values, key_decay, first_key, first_query, head_width
):
    highest_old, weight_sum, weighted = state
    query_rows = queries.shape[0]
    head_count = query_decay.shape[1]
    key_rows = keys.shape[0]
    grid_query = queries.reshape(query_rows, head_count, head_width)
    grid_key = keys.reshape(key_rows, head_count, head_width)
    grid_value = values.reshape(key_rows, head_count, head_width)
    scores = jnp.einsum("thd,phd->htp", grid_query, grid_key, preferred_element_type=jnp.float32)
    scores = scores * head_width ** (-0.5) + query_decay.T[:, :, None] - key_decay.T[:, None, :]
    query_place = first_query + jnp.arange(query_rows, dtype=jnp.int32)
    key_place = first_key + jnp.arange(key_rows, dtype=jnp.int32)
    scores = jnp.where(key_place[None, None, :] <= query_place[None, :, None], scores, -jnp.inf)
    highest = jnp.maximum(highest_old, jnp.max(scores, axis=2))
    weights = jnp.exp(scores - highest[:, :, None])
    shrink = jnp.exp(highest_old - highest)
    weight_sum = weight_sum * shrink + jnp.sum(weights, axis=2)
    product = jnp.einsum(
        "htp,phd->htd", weights.astype(jnp.bfloat16), grid_value, preferred_element_type=jnp.float32
    )
    weighted = weighted * shrink[:, :, None] + product
    return (highest, weight_sum, weighted)


def fresh_state(head_count, shard_rows, head_width):
    return (
        jnp.full((head_count, shard_rows), -1e30, jnp.float32),
        jnp.zeros((head_count, shard_rows), jnp.float32),
        jnp.zeros((head_count, shard_rows, head_width), jnp.float32),
    )


def finish(state, shard_rows):
    highest, weight_sum, weighted = state
    mixed_heads = weighted / weight_sum[:, :, None]
    joined = jnp.transpose(mixed_heads, (1, 0, 2))
    return joined.reshape(shard_rows, weighted.shape[0] * weighted.shape[2]).astype(jnp.bfloat16)


def body(
    residual,
    query_wide,
    key_wide,
    value_wide,
    query_narrow,
    key_narrow,
    value_narrow,
    gate_wide,
    gate_narrow,
    out_wide,
    out_narrow,
    norm_gain,
    routing,
    route_weight,
    gate_weight,
    up_weight,
    down_weight,
):
    shard_rows = query_wide.shape[0]
    half_rows = shard_rows // 2
    sp_place = lax.axis_index("sp")
    first_query = sp_place * shard_rows
    running_wide = jnp.cumsum(jax.nn.log_sigmoid(gate_wide), axis=0)
    running_narrow = jnp.cumsum(jax.nn.log_sigmoid(gate_narrow), axis=0)
    pieces_wide, pieces_narrow = (
        lax.all_gather(running_wide, "sp", axis=0, tiled=True),
        lax.all_gather(running_narrow, "sp", axis=0, tiled=True),
    )
    every_wide = globalize(pieces_wide, shard_rows)
    every_narrow = globalize(pieces_narrow, shard_rows)
    late_first = first_query + half_rows
    halves = []
    for place, part_wide, part_narrow in (
        (first_query, query_wide[:half_rows], query_narrow[:half_rows]),
        (late_first, query_wide[half_rows:], query_narrow[half_rows:]),
    ):
        halves.append(
            (
                place,
                part_wide,
                part_narrow,
                lax.dynamic_slice_in_dim(every_wide, place, half_rows, 0),
                lax.dynamic_slice_in_dim(every_narrow, place, half_rows, 0),
            )
        )

    def half_state():
        return (
            fresh_state(gate_wide.shape[1], half_rows, HW),
            fresh_state(gate_narrow.shape[1], half_rows, HN),
        )

    state = (half_state(), half_state())
    keys_wide = lax.all_gather(key_wide, "sp", axis=0, tiled=True)
    values_wide = lax.all_gather(value_wide, "sp", axis=0, tiled=True)
    keys_narrow = lax.all_gather(key_narrow, "sp", axis=0, tiled=True)
    values_narrow = lax.all_gather(value_narrow, "sp", axis=0, tiled=True)
    span_rows = keys_wide.shape[0]
    block_size = math.gcd(span_rows, 2048)

    def visit(carried, position):
        inside = position * block_size

        def take_block(source):
            return lax.dynamic_slice_in_dim(source, inside, block_size, 0)

        def take_decay(source):
            return lax.dynamic_slice_in_dim(source, inside, block_size, 0)

        block_kw = take_block(keys_wide)
        block_vw = take_block(values_wide)
        block_kn = take_block(keys_narrow)
        block_vn = take_block(values_narrow)
        block_dw = take_decay(every_wide)
        block_dn = take_decay(every_narrow)

        def one_half(current, half):
            place, part_wide, part_narrow, query_decay_wide, query_decay_narrow = half

            def work(inner):
                first = head_block(
                    inner[0],
                    part_wide,
                    query_decay_wide,
                    block_kw,
                    block_vw,
                    block_dw,
                    inside,
                    place,
                    HW,
                )
                second = head_block(
                    inner[1],
                    part_narrow,
                    query_decay_narrow,
                    block_kn,
                    block_vn,
                    block_dn,
                    inside,
                    place,
                    HN,
                )
                return (first, second)

            def skip(inner):
                return inner

            return lax.cond(inside <= place + half_rows - 1, work, skip, current)

        updated = (one_half(carried[0], halves[0]), one_half(carried[1], halves[1]))
        return (updated, None)

    state, _ = lax.scan(visit, state, jnp.arange(span_rows // block_size, dtype=jnp.int32))
    att_wide = jnp.concatenate(
        [finish(state[0][0], half_rows), finish(state[1][0], half_rows)], axis=0
    )
    att_narrow = jnp.concatenate(
        [finish(state[0][1], half_rows), finish(state[1][1], half_rows)], axis=0
    )
    own_rows = residual.shape[0]
    tp_place = lax.axis_index("tp")
    rows_wide = lax.dynamic_slice_in_dim(
        out_wide, tp_place * att_wide.shape[1], att_wide.shape[1], 0
    )
    rows_narrow = lax.dynamic_slice_in_dim(
        out_narrow, tp_place * att_narrow.shape[1], att_narrow.shape[1], 0
    )
    first = jnp.dot(att_wide, rows_wide, preferred_element_type=jnp.float32)
    second = jnp.dot(att_narrow, rows_narrow, preferred_element_type=jnp.float32)
    mixed = lax.psum_scatter(
        (first + second).astype(jnp.bfloat16), "tp", scatter_dimension=0, tiled=True
    ).astype(jnp.float32)
    middle = (residual.astype(jnp.float32) + mixed).astype(jnp.bfloat16)
    middle_wide = middle.astype(jnp.float32)
    spread = jnp.mean(middle_wide * middle_wide, axis=1, keepdims=True)
    normed = (middle_wide * lax.rsqrt(spread + epsilon) * norm_gain).astype(jnp.bfloat16)
    features = normed.shape[1]
    chosen_count = routing.shape[1]
    expert_count = gate_weight.shape[0] * lax.axis_size("sp")
    capacity = own_rows * GROUPS // expert_count
    flat_routes = routing.reshape(-1)
    matches = (flat_routes[:, None] == jnp.arange(expert_count, dtype=jnp.int32)[None, :]).astype(
        jnp.int32
    )
    ranking = jnp.sum((jnp.cumsum(matches, axis=0) - matches) * matches, axis=1)
    placing = flat_routes * capacity + ranking
    picker = (
        placing[None, :] == jnp.arange(expert_count * capacity, dtype=jnp.int32)[:, None]
    ).astype(jnp.bfloat16)
    picker = jnp.sum(picker.reshape(expert_count * capacity, own_rows, chosen_count), axis=2)
    outgoing = jnp.dot(picker, normed, preferred_element_type=jnp.float32).astype(jnp.bfloat16)
    outgoing = outgoing.reshape(expert_count, capacity, features)
    arrived = lax.all_to_all(outgoing, "sp", split_axis=0, concat_axis=0, tiled=True)
    pooled = lax.all_gather(arrived.reshape(-1, features), "tp", axis=0, tiled=True)
    gate_value = jnp.dot(pooled, gate_weight[0], preferred_element_type=jnp.float32)
    up_value = jnp.dot(pooled, up_weight[0], preferred_element_type=jnp.float32)
    hidden = (jax.nn.silu(gate_value) * up_value).astype(jnp.bfloat16)
    answers = lax.psum_scatter(
        jnp.dot(hidden, down_weight[0], preferred_element_type=jnp.float32).astype(jnp.bfloat16),
        "tp",
        scatter_dimension=0,
        tiled=True,
    )
    returned = lax.all_to_all(
        answers.reshape(expert_count, capacity, features),
        "sp",
        split_axis=0,
        concat_axis=0,
        tiled=True,
    )
    picked = jnp.take(returned.reshape(expert_count * capacity, features), placing, axis=0)
    picked = picked.reshape(own_rows, chosen_count, features).astype(jnp.float32)
    combined = jnp.sum(route_weight[:, :, None] * picked, axis=1)
    return (middle_wide + combined).astype(jnp.bfloat16)


CORES = 2
MESH = pl.DeviceIdType.MESH
VMEM = pl.BlockSpec(memory_space=pltpu.VMEM)


def greet(peers):
    barrier = pltpu.get_barrier_semaphore()
    for peer in peers:
        pl.semaphore_signal(barrier, inc=1, device_id=peer, device_id_type=MESH)
    pl.semaphore_wait(barrier, len(peers))


def remote(source, target, send, receive, peer):
    return pltpu.make_async_remote_copy(
        src_ref=source,
        dst_ref=target,
        send_sem=send,
        recv_sem=receive,
        device_id=peer,
        device_id_type=MESH,
    )


DMA = pltpu.SemaphoreType.DMA


SENDS = [0, 1, 2, 3, 4, 5, 6, 7, 8, 8, 8, 8, 9, 10, 10, 10, 10, 10, 10, 11, 12, 9, 10]
TAKES = [0, 1, 2, 3, 4, 5, 6, 6, 7, 7, 7, 7, 8, 9, 11, 10, 11, 11, 11, 12, 8, 9, 10]


LOG2E = math.log2(math.e)


def layer_kernel(outer, inner, ys, *refs):
    gate_w, gate_n, chosen, shares, qw, kw, vw, qn, kn, vn, residual, gain = refs[:12]
    out_wide, out_narrow, gate_hbm, up_hbm, down_hbm, result = refs[12:18]
    refs = refs[3:]
    kws, vws, kns, vns, far, run, peak, total, acc_w, acc_n, att, swapped = refs[15:27]
    wide_w, narrow_w, gate, up, down, middle, outgoing, returned = refs[27:35]
    pooled, answers, half, chip_a, chip_b, from_x, from_y, next_a, next_b = refs[35:44]
    last_a, last_b, final, picker, board, factor = refs[44:50]
    hidden, hidden_in, parts_own, parts_in, both, from_both, ended = refs[50:57]
    load, lift_s, lift_r, cross_s, cross_r, turn_s, turn_r = refs[57:64]
    far_s, far_r, swap_s, swap_r, give_s, give_r, send, take = refs[64:]
    place, tp = lax.axis_index("sp"), lax.axis_index("tp")
    o, i, y, c = place // inner, place % inner, tp // CORES, tp % CORES
    far_i, far_y, far_c = (i + 1) % inner, (y + 1) % ys, (c + 1) % CORES
    places, parts = outer * inner, ys * CORES
    rows, wide = qw.shape
    narrow = qn.shape[1]
    heads = 1 + narrow // HN
    own_rows, features = residual.shape
    cap = outgoing.shape[1]
    h = cap // 2
    low, high = pl.ds(0, h), pl.ds(h, h)
    units = gate.shape[1]
    deep = o >= outer - 2
    final_plane = o == outer - 1
    def at(o_, i_, y_, c_):
        return (o_ * inner + i_, y_ * CORES + c_)

    across, along, mate = at(o, far_i, y, c), at(o, i, far_y, c), at(o, i, y, far_c)

    loads = [
        pltpu.make_async_copy(source, target, load.at[n])
        for n, (source, target) in enumerate(
            [
                (out_wide, wide_w),
                (out_narrow, narrow_w),
                (gate_hbm.at[0], gate),
                (up_hbm.at[0], up),
                (down_hbm.at[0], down.at[y]),
            ]
        )
    ]
    for copy in loads:
        copy.start()
    far[...] = jnp.zeros_like(far)
    peers = [((place + d) % places, tp) for d in range(1, places)]
    peers = peers + [(place, (tp + d) % parts) for d in range(1, parts)]
    barrier = pltpu.get_barrier_semaphore()
    for peer in peers:
        pl.semaphore_signal(barrier, inc=1, device_id=peer, device_id_type=MESH)
    picks = chosen.shape[0]
    board[...] = jnp.zeros_like(board)
    board[:1] = gate_w[...]
    board[1:heads] = gate_n[...]
    board[heads : heads + picks, :own_rows] = chosen[...].astype(jnp.float32)
    board[heads + picks : heads + 2 * picks, :own_rows] = shares[...]
    facts = board[...]
    step = jnp.minimum(facts, 0.0) - jnp.log1p(jnp.exp(-jnp.abs(facts)))
    lane = lax.broadcasted_iota(jnp.int32, step.shape, 1)
    shift = 1
    while shift < rows:
        step = step + jnp.where(lane >= shift, pltpu.roll(step, shift, 1), 0.0)
        shift *= 2
    run[...] = step
    near = step * LOG2E
    pl.semaphore_wait(barrier, len(peers))
    for d in range(1, places):

        @pl.when(place + d < places)
        def _(d=d):
            remote(run, far.at[place], far_s.at[0], far_r.at[0], (place + d, tp)).start()

    ins, blocks = (kw, vw, kn, vn), (kws, vws, kns, vns)
    count = len(ins)

    def source_of(t, a):
        slot = (o - t) * inner + i
        return (ins[a] if t == 0 else blocks[a].at[slot]), blocks[a].at[slot]

    def lift(t, a):
        source, target = source_of(t, a)
        return remote(
            source, target, lift_s.at[t, a // 2], lift_r.at[t, a], at(o + 1, i, y, c)
        )

    def cross(t, a):
        source, target = source_of(t, a)
        return remote(source, target, cross_s.at[t, a // 2], cross_r.at[t, a // 2], across)

    def twin(p):
        return blocks[2 * p].at[pl.ds(0, 2)]

    def arrived(where, semaphore):
        remote(where, where, semaphore, semaphore, mate).wait_recv()

    def detour(a):
        slot = blocks[a].at[far_i]
        return remote(slot, slot, turn_s.at[0], turn_r.at[0], at(o + 1, i, y, c))

    def detours(a):
        return a >= count // 2

    def give(p):
        lines = pl.ds(p * units // (2 * outer), units // (2 * outer))
        target = down.at[y, lines]
        return remote(down_hbm.at[0, lines], target, give_s.at[0], give_r.at[0], along)

    def crosses(t, a):
        if t == 0:
            return jnp.logical_or(i < far_i, o == 0) if detours(a) else i < far_i
        return o > t if detours(a) else o >= t

    for a in range(count):

        @pl.when(o + 1 < outer)
        def _(a=a):
            lift(0, a).start()

        @pl.when(crosses(0, a))
        def _(a=a):
            cross(0, a).start()

    for p in range(2 * outer):
        pl.when(deep if p < 2 * outer - 1 else final_plane)(lambda: give(p).start())

    head_lane = lax.broadcasted_iota(jnp.int32, (rows, narrow), 1) // HN

    def attend(block_of, decay, diagonal):
        columns = jnp.transpose(decay * LOG2E)
        for n in range(heads):
            k, v = (block_of(0), block_of(1)) if n == 0 else (block_of(2), block_of(3))
            if n == 0:
                q, size = qw[...], HW
            else:
                q, size = jnp.where(head_lane == n - 1, qn[...], jnp.zeros_like(qn[...])), HN
            s = lax.dot_general(k, q, (((1,), (1,)), ((), ())), preferred_element_type=jnp.float32)
            s = s * (LOG2E * size ** (-0.5)) - columns[:, n : n + 1]
            if diagonal:
                key = lax.broadcasted_iota(jnp.int32, s.shape, 0)
                query = lax.broadcasted_iota(jnp.int32, s.shape, 1)
                s = jnp.where(key <= query, s, -jnp.inf)
            row = near[n : n + 1]
            new = jnp.max(s, axis=0, keepdims=True) + row
            if not diagonal:
                before = peak[n : n + 1]
                new = jnp.maximum(new, before)
            weights = jnp.exp2(s - (new - row))
            mass = jnp.sum(weights, axis=0, keepdims=True)
            part = lax.dot_general(
                v if n == 0 else v[:, (n - 1) * HN : n * HN],
                weights.astype(jnp.bfloat16),
                (((0,), (0,)), ((), ())),
                preferred_element_type=jnp.float32,
            )
            acc = acc_w if n == 0 else acc_n.at[(n - 1) * HN : n * HN]
            if diagonal:
                total[n : n + 1] = mass
                acc[...] = part
            else:
                shrink = jnp.exp2(before - new)
                total[n : n + 1] = total[n : n + 1] * shrink + mass
                acc[...] = acc[...] * shrink + part
            peak[n : n + 1] = new

    attend(lambda a: ins[a][...], step, True)
    columns = jnp.transpose(facts)[:own_rows]

    def group_of(names):
        return jnp.floor((names + 0.5) / inner)

    group = group_of(facts[heads : heads + 1, :own_rows])
    ahead = lax.broadcasted_iota(jnp.int32, (own_rows, own_rows), 0)
    ahead = ahead < lax.broadcasted_iota(jnp.int32, (own_rows, own_rows), 1)
    same = jnp.logical_and(group_of(columns[:, heads : heads + 1]) == group, ahead)
    placing = group * cap + jnp.sum(jnp.where(same, 1.0, 0.0), axis=0, keepdims=True)
    slots = lax.broadcasted_iota(jnp.int32, (GROUPS * cap, own_rows), 0).astype(jnp.float32)
    picker[...] = jnp.where(slots == placing, 1.0, 0.0).astype(jnp.bfloat16)
    lane = lax.broadcasted_iota(jnp.int32, (own_rows, outgoing.shape[2] - features), 1)
    extra = jnp.zeros(lane.shape, jnp.float32)
    for e in range(inner):
        weight = jnp.zeros((own_rows, 1), jnp.float32)
        for k in range(picks):
            name = columns[:, heads + k : heads + k + 1]
            value = columns[:, heads + picks + k : heads + picks + k + 1]
            weight = weight + jnp.where(name - inner * group_of(name) == e, value, 0.0)
        top = weight.astype(jnp.bfloat16).astype(jnp.float32)
        extra = jnp.where(lane == 2 * e, top, extra)
        extra = jnp.where(lane == 2 * e + 1, weight - top, extra)
    part = jnp.dot(picker[...], extra.astype(jnp.bfloat16), preferred_element_type=jnp.float32)
    outgoing[:, :, features:] = part.astype(jnp.bfloat16).reshape(GROUPS, cap, lane.shape[1])

    for d in range(1, places):

        @pl.when(place == d)
        def _(d=d):
            arrived(far.at[pl.ds(0, d)], far_r.at[0])

    def visit(slot):
        offset = jnp.zeros((far.shape[1], 1), jnp.float32)
        for b in range(places):
            inside = jnp.logical_and(b >= slot, b < place)
            offset = offset + jnp.where(inside, far[b, :, rows - 1 : rows], 0.0)
        attend(lambda a: blocks[a][slot], far[slot] - offset, False)

    def relay(t):
        @pl.when(o >= t)
        def _():
            for a in range(count):
                arrived(blocks[a].at[0], lift_r.at[t - 1, a])
                if t < outer - 1:
                    pl.when(o + 1 < outer)(lambda: lift(t, a).start())
                pl.when(crosses(t, a))(lambda: cross(t, a).start())

    def own(t):
        @pl.when(o >= t)
        def _():
            visit((o - t) * inner + i)

    def other(t):
        slot = (o - t) * inner + far_i
        needed = (o >= t) if t > 0 else (far_i < i)
        pl.when(needed)(lambda: arrived(twin(0), cross_r.at[t, 0]))
        if t > 0:
            pl.when(o > t)(lambda: arrived(twin(1), cross_r.at[t, 1]))
            pl.when(o == t)(lambda: arrived(twin(1), turn_r.at[0]))
        else:
            pl.when(jnp.logical_or(needed, o == 0))(lambda: arrived(twin(1), cross_r.at[t, 1]))
        if t < outer - 1:
            for a in range(count // 2, count):
                pl.when(o == t)(lambda: detour(a).start())

        @pl.when((o >= t) if t > 0 else (far_i < i))
        def _():
            visit(slot)

    def finish():
        mixed = jnp.transpose(acc_w[...] / total[0:1]).astype(jnp.bfloat16)
        att[:, :, :wide] = mixed.reshape(parts, own_rows, wide)
        for n in range(1, heads):
            piece = slice((n - 1) * HN, n * HN)
            acc_n[piece] = acc_n[piece] / total[n : n + 1]
        mixed = jnp.transpose(acc_n[...]).astype(jnp.bfloat16)
        att[:, :, wide:] = mixed.reshape(parts, own_rows, narrow)
        for d in range(1, parts):
            swap(d).start()
        swapped[tp] = att[tp]

    def swap(d):
        k = (tp + d) % parts
        return remote(att.at[k], swapped.at[tp], swap_s.at[0], swap_r.at[0], (place, k))

    def settle():
        arrived(swapped.at[pl.ds(0, parts - 1)], swap_r.at[0])

    tile = math.gcd(features, 512)

    def project():
        rows_w = jnp.concatenate([swapped[p, :, :wide] for p in range(parts)], axis=1)
        rows_n = jnp.concatenate([swapped[p, :, wide:] for p in range(parts)], axis=1)
        squares = jnp.zeros((own_rows, 1), jnp.float32)
        for n in range(features // tile):
            at_n = pl.ds(n * tile, tile)
            part = jnp.dot(rows_w, wide_w[:, at_n], preferred_element_type=jnp.float32)
            part = part + jnp.dot(rows_n, narrow_w[:, at_n], preferred_element_type=jnp.float32)
            part = (residual[:, at_n].astype(jnp.float32) + part).astype(jnp.bfloat16)
            middle[:, at_n] = part
            part = part.astype(jnp.float32)
            squares = squares + jnp.sum(part * part, axis=1, keepdims=True)
        factor[...] = lax.rsqrt(squares / features + epsilon)

    def ready():
        for n in range(features // tile):
            at_n = pl.ds(n * tile, tile)
            part = middle[:, at_n].astype(jnp.float32) * factor[...] * gain[:, at_n]
            part = jnp.dot(
                picker[...], part.astype(jnp.bfloat16), preferred_element_type=jnp.float32
            )
            outgoing[:, :, at_n] = part.astype(jnp.bfloat16).reshape(GROUPS, cap, tile)

    def route(kind, t):
        mine, beside = pooled.at[t, c, i, y], pooled.at[t, c, far_i, y]
        below, corners = pooled.at[t, c, i, far_y], pooled.at[t, c, far_i, far_y]
        if kind == 0:
            return outgoing.at[t, low], pooled.at[o, c, i, y, low], at(t, i, y, c)
        if kind == 1:
            return outgoing.at[t, high], pooled.at[o, c, i, y, high], at(t, i, y, c)
        if kind == 2:
            return mine.at[low], mine.at[low], across
        if kind == 3:
            return mine.at[high], mine.at[high], across
        if kind == 4:
            return mine.at[low], mine.at[low], along
        if kind == 5:
            return mine.at[high], mine.at[high], along
        if kind == 6:
            return beside.at[low], beside.at[low], along
        if kind == 7:
            return below.at[high], below.at[high], across
        if kind in (8, 9, 10, 11):
            slot = (mine, beside, below, corners)[kind - 8]
            return slot, slot, mate
        if kind == 12:
            return answers.at[t, far_c], half.at[t], mate
        if kind == 13:
            return chip_a.at[t, far_i, far_y], from_x.at[t, far_y], across
        if kind == 14:
            return chip_a.at[t, far_i, y], from_x.at[t, y], across
        if kind == 15:
            return chip_b.at[t, far_y, far_i], from_y.at[t, far_i], along
        if kind == 16:
            return chip_b.at[t, far_y, i], from_y.at[t, i], along
        if kind == 17:
            return next_a.at[t], last_a.at[t], along
        if kind == 18:
            return next_b.at[t], last_b.at[t], across
        if kind == 20:
            return hidden.at[t, far_y], hidden_in.at[t], along
        if kind == 21:
            return parts_own.at[t, far_c], parts_in.at[t], mate
        if kind == 22:
            return both.at[t, far_i], from_both.at[t], across
        return final.at[t], returned.at[o], at(t, i, y, c)

    def copy_of(kind, t):
        source, target, peer = route(kind, t)
        mark = o if kind in (0, 1, 19) else t
        return remote(source, target, send.at[SENDS[kind]], take.at[TAKES[kind], mark], peer)

    def push(kind, t):
        if kind in (0, 1, 19):
            pl.when(o != t)(lambda: copy_of(kind, t).start())
        else:
            copy_of(kind, t).start()

    def landed(kind, t, where):
        arrived(where, take.at[TAKES[kind], t])

    def late(t):
        return jnp.logical_and(o + 2 <= t, o < outer - 2)

    def send_rows(t):
        push(0, t)
        push(1, t)

    def dispatch():
        for t in reversed(range(outer)):
            pl.when(jnp.logical_not(late(t)))(lambda: send_rows(t))

        pooled[o, c, i, y] = outgoing[o]

    def begin(t):
        slot = pooled.at[t, c, i, y]

        def hold(kind, part):
            pl.when(o != t)(lambda: landed(kind, t, slot.at[part]))

        hold(0, low)
        push(2, t)
        hold(1, high)
        push(5, t)
        push(3, t)
        push(4, t)
        push(8, t)

    def pass_on(t):
        beside, below = pooled.at[t, c, far_i, y], pooled.at[t, c, i, far_y]
        landed(2, t, beside.at[low])
        push(6, t)
        landed(5, t, below.at[high])
        push(7, t)
        landed(3, t, beside.at[high])
        push(9, t)
        landed(4, t, below.at[low])
        push(10, t)

    def corner(t):
        landed(6, t, pooled.at[t, c, far_i, far_y])
        push(11, t)

    def feed(t):
        landed(8, t, pooled.at[t, far_c])
        rows = CORES * inner * ys * cap
        x = pooled[t, :, :, :, :, :features].reshape(rows, features)
        extra = pooled[t, :, :, :, :, features:].reshape(rows, -1).astype(jnp.float32)
        lane = lax.broadcasted_iota(jnp.int32, extra.shape, 1)
        scale = jnp.sum(jnp.where(lane // 2 == i, extra, 0.0), axis=1, keepdims=True)
        g = jnp.dot(x, gate[...], preferred_element_type=jnp.float32)
        u = jnp.dot(x, up[...], preferred_element_type=jnp.float32)
        made = (jax.nn.silu(g) * u).astype(jnp.bfloat16)
        wide = math.gcd(features, 512)
        for n in range(features // wide):
            columns = pl.ds(n * wide, wide)
            part = jnp.dot(made, down[y, :, columns], preferred_element_type=jnp.float32)
            answers[t, :, :, :, :, columns] = (
                (part * scale).astype(jnp.bfloat16).reshape(CORES, inner, ys, cap, wide)
            )
        push(12, t)

    def gather(t):
        landed(12, t, half.at[t])
        for i_ in range(inner):
            for y_ in range(ys):
                total = answers[t, c, i_, y_].astype(jnp.float32)
                total = (total + half[t, i_, y_].astype(jnp.float32)).astype(jnp.bfloat16)
                chip_a[t, i_, y_] = total[:h]
                chip_b[t, y_, i_] = total[h:]
        push(13, t)
        push(15, t)
        push(14, t)
        push(16, t)

    def add(*parts):
        total = parts[0].astype(jnp.float32)
        for part in parts[1:]:
            total = total + part.astype(jnp.float32)
        return total.astype(jnp.bfloat16)

    def turn(t):
        landed(13, t, from_x.at[t, far_y])
        next_a[t] = add(chip_a[t, i, far_y], from_x[t, far_y])
        push(17, t)
        landed(15, t, from_y.at[t, far_i])
        next_b[t] = add(chip_b[t, y, far_i], from_y[t, far_i])
        push(18, t)

    def home(t):
        landed(14, t, chip_a.at[t])
        final[t, :h] = add(chip_a[t, i, y], from_x[t, y], last_a[t])
        final[t, h:] = add(chip_b[t, y, i], from_y[t, i], last_b[t])
        push(19, t)

    def enter(t):
        landed(8, t, pooled.at[t, far_c])
        x = pooled[t, :, :, :, :, :features].reshape(CORES * inner * ys * cap, features)
        g = jnp.dot(x, gate[...], preferred_element_type=jnp.float32)
        u = jnp.dot(x, up[...], preferred_element_type=jnp.float32)
        made = (jax.nn.silu(g) * u).astype(jnp.bfloat16)
        made = made.reshape(CORES, inner, ys, cap, units)
        for y_ in range(ys):
            hidden[t, y_] = made[:, :, y_]
        push(20, t)

    def complete():
        arrived(down.at[far_y], give_r.at[0])

    def mix(t):
        landed(20, t, hidden_in.at[t])
        lines = CORES * inner * cap
        extra = pooled[t, :, :, y, :, features:].reshape(lines, -1).astype(jnp.float32)
        lane = lax.broadcasted_iota(jnp.int32, extra.shape, 1)
        scale = jnp.sum(jnp.where(lane // 2 == i, extra, 0.0), axis=1, keepdims=True)
        mine = hidden[t, y].reshape(lines, units)
        theirs = hidden_in[t].reshape(lines, units)
        for n in range(features // tile):
            at_n = pl.ds(n * tile, tile)
            part = jnp.dot(mine, down[y, :, at_n], preferred_element_type=jnp.float32)
            part = part + jnp.dot(theirs, down[far_y, :, at_n], preferred_element_type=jnp.float32)
            parts_own[t, :, :, :, at_n] = (
                (part * scale).astype(jnp.bfloat16).reshape(CORES, inner, cap, tile)
            )
        push(21, t)

    def pair(t):
        landed(21, t, parts_in.at[t])
        both[t] = add(parts_own[t, c], parts_in[t])
        push(22, t)

    def leave(t):
        landed(22, t, from_both.at[t])
        final[t] = add(both[t, i], from_both[t])
        push(19, t)

    relay(1)
    other(0)
    own(1)
    relay(2)
    other(1)
    own(2)
    relay(3)
    other(2)
    own(3)

    other(3)
    finish()

    loads[0].wait()
    loads[1].wait()
    settle()
    project()
    ready()
    dispatch()
    for copy in loads[2:]:
        copy.wait()

    @pl.when(final_plane)
    def _():
        begin(0)
        begin(3)
        pass_on(0)
        begin(1)
        begin(2)
        pass_on(3)
        corner(0)
        enter(0)
        complete()
        pass_on(1)
        corner(3)
        mix(0)
        enter(3)
        pass_on(2)
        pair(0)
        corner(1)
        enter(1)
        mix(3)
        pair(3)
        corner(2)
        mix(1)
        enter(2)
        leave(0)
        pair(1)
        mix(2)
        leave(3)
        pair(2)
        leave(1)
        leave(2)

    @pl.when(o == outer - 2)
    def _():
        begin(2)
        begin(0)
        pass_on(2)
        pass_on(0)
        give(2 * outer - 1).start()
        corner(2)
        enter(2)
        begin(3)
        begin(1)
        complete()
        pass_on(3)
        corner(0)
        mix(2)
        enter(0)
        pass_on(1)
        pair(2)
        corner(3)
        enter(3)
        mix(0)
        pair(0)
        corner(1)
        mix(3)
        enter(1)
        pair(3)
        leave(0)
        mix(1)
        pair(1)
        leave(3)
        leave(1)
        leave(2)

    @pl.when(jnp.logical_not(deep))
    def _():
        begin(0)
        pass_on(0)
        for t in range(outer):
            pl.when(late(t))(lambda: send_rows(t))
        begin(1)
        corner(0)
        feed(0)
        pass_on(1)
        gather(0)
        begin(2)
        corner(1)
        feed(1)
        pl.when(o == outer - 3)(lambda: begin(3))
        pass_on(2)
        turn(0)
        gather(1)
        corner(2)
        feed(2)
        pl.when(o == outer - 4)(lambda: begin(3))
        pass_on(3)
        home(0)
        turn(1)
        gather(2)
        corner(3)
        feed(3)
        home(1)
        turn(2)
        gather(3)
        home(2)
        turn(3)
        home(3)

    @pl.when(deep)
    def _():
        remote(down.at[y], down.at[y], give_s.at[0], give_r.at[0], mate).wait_send()

    def sent(p, semaphore):
        remote(twin(p), twin(p), semaphore, semaphore, mate).wait_send()

    for t in range(outer):
        for p in range(count // 2):
            if t < outer - 1:
                pl.when(jnp.logical_and(o >= t, o + 1 < outer))(lambda: sent(p, lift_s.at[t, p]))
            pl.when(crosses(t, 2 * p))(lambda: sent(p, cross_s.at[t, p]))

    pl.when(o + 1 < outer)(lambda: sent(1, turn_s.at[0]))

    for d in range(1, places):

        @pl.when(place + d == places - 1)
        def _(d=d):
            sums = far.at[pl.ds(0, d)]
            remote(sums, sums, far_s.at[0], far_r.at[0], mate).wait_send()

    others = att.at[pl.ds(0, parts - 1)]
    remote(others, others, swap_s.at[0], swap_r.at[0], mate).wait_send()

    def returns(t):
        pl.when(o != t)(lambda: landed(19, t, returned.at[t]))

    returned[o] = final[o]
    for t in range(outer):
        returns(t)

    def drain(kind, whole):
        remote(whole, whole, send.at[SENDS[kind]], send.at[SENDS[kind]], mate).wait_send()

    drain(0, outgoing.at[pl.ds(0, outer - 1), low])
    drain(1, outgoing.at[pl.ds(0, outer - 1), high])
    for kind in range(2, 8):
        drain(kind, pooled.at[:, 0, 0, 0, low if kind in (2, 4, 6) else high])
    drain(8, pooled.at[pl.ds(0, outer // 2)])
    drain(19, final.at[pl.ds(0, outer - 1)])

    @pl.when(deep)
    def _():
        drain(20, hidden_in)
        drain(21, parts_in)
        drain(22, from_both)

    @pl.when(jnp.logical_not(deep))
    def _():
        drain(12, half)
        drain(13, half.at[pl.ds(0, 3 * outer // 4)])

    def combine():
        copies = []
        for n in range(features // tile):
            at_n = pl.ds(n * tile, tile)
            slots = returned[:, :, at_n].reshape(GROUPS * cap, tile)
            combined = lax.dot_general(
                picker[...], slots, (((0,), (0,)), ((), ())), preferred_element_type=jnp.float32
            )
            ended[n] = (middle[:, at_n].astype(jnp.float32) + combined).astype(jnp.bfloat16)
            copies.append(pltpu.make_async_copy(ended.at[n], result.at[:, at_n], load.at[5 + n]))
            copies[-1].start()
        for copy in copies:
            copy.wait()

    combine()


def fast_body(
    residual,
    query_wide,
    key_wide,
    value_wide,
    query_narrow,
    key_narrow,
    value_narrow,
    gate_wide,
    gate_narrow,
    out_wide,
    out_narrow,
    norm_gain,
    routing,
    route_weight,
    gate_weight,
    up_weight,
    down_weight,
):
    inner = routing.shape[1]
    places = lax.axis_size("sp")
    outer = places // inner
    parts = lax.axis_size("tp")
    ys = parts // CORES
    own_rows, features = residual.shape
    rows, wide = query_wide.shape
    narrow = query_narrow.shape[1]
    heads = gate_wide.shape[1] + gate_narrow.shape[1]
    lines = pl.cdiv(heads + 2 * inner, 8) * 8
    cap = own_rows * GROUPS // places
    h = cap // 2
    units = down_weight.shape[1]
    tiles = features // math.gcd(features, 512)
    width = features + 128 * pl.cdiv(2 * inner, 128)
    kind, full = jnp.bfloat16, jnp.float32

    def vmem(*shape, dtype=kind):
        return pltpu.VMEM(shape, dtype)

    scratch = [
        vmem(places, rows, wide),
        vmem(places, rows, wide),
        vmem(places, rows, narrow),
        vmem(places, rows, narrow),
        vmem(places, lines, rows, dtype=full),
        vmem(lines, rows, dtype=full),
        vmem(lines, rows, dtype=full),
        vmem(lines, rows, dtype=full),
        vmem(wide, rows, dtype=full),
        vmem(narrow, rows, dtype=full),
        vmem(parts, own_rows, wide + narrow),
        vmem(parts, own_rows, wide + narrow),
        vmem(*out_wide.shape),
        vmem(*out_narrow.shape),
        vmem(*gate_weight.shape[1:]),
        vmem(*up_weight.shape[1:]),
        vmem(ys, units, features),
        vmem(own_rows, features),
        vmem(GROUPS, cap, width),
        vmem(outer, cap, features),
        vmem(outer, CORES, inner, ys, cap, width),
        vmem(outer, CORES, inner, ys, cap, features),
        vmem(outer, inner, ys, cap, features),
        vmem(outer, inner, ys, h, features),
        vmem(outer, ys, inner, h, features),
        vmem(outer, ys, h, features),
        vmem(outer, inner, h, features),
        vmem(outer, h, features),
        vmem(outer, h, features),
        vmem(outer, h, features),
        vmem(outer, h, features),
        vmem(outer, cap, features),
        vmem(GROUPS * cap, own_rows),
        vmem(lines, rows, dtype=full),
        vmem(own_rows, 1, dtype=full),
        vmem(outer, ys, CORES, inner, cap, units),
        vmem(outer, CORES, inner, cap, units),
        vmem(outer, CORES, inner, cap, features),
        vmem(outer, inner, cap, features),
        vmem(outer, inner, cap, features),
        vmem(outer, cap, features),
        vmem(tiles, own_rows, features // tiles),
        DMA((5 + tiles,)),
        DMA((outer - 1, 2)),
        DMA((outer - 1, 4)),
        DMA((outer, 2)),
        DMA((outer, 2)),
        DMA((1,)),
        DMA((1,)),
        DMA((1,)),
        DMA((1,)),
        DMA((1,)),
        DMA((1,)),
        DMA((1,)),
        DMA((1,)),
        DMA((1 + max(SENDS),)),
        DMA((1 + max(TAKES), outer)),
    ]
    anywhere = pl.BlockSpec(memory_space=pl.ANY)
    return pl.pallas_call(
        functools.partial(layer_kernel, outer, inner, ys),
        out_shape=jax.ShapeDtypeStruct(residual.shape, residual.dtype),
        in_specs=[VMEM] * 12 + [anywhere] * 5,
        out_specs=anywhere,
        scratch_shapes=scratch,
        compiler_params=pltpu.CompilerParams(
            collective_id=1, has_side_effects=True, vmem_limit_bytes=56 * 1024 * 1024
        ),
    )(
        gate_wide.T,
        gate_narrow.T,
        routing.T,
        route_weight.T,
        query_wide,
        key_wide,
        value_wide,
        query_narrow,
        key_narrow,
        value_narrow,
        residual,
        norm_gain[None, :],
        out_wide,
        out_narrow,
        gate_weight,
        up_weight,
        down_weight,
    )


def choose(*args):
    routing, gate_weight = args[12], args[14]
    experts = gate_weight.shape[0] * lax.axis_size("sp")
    paired = lax.axis_size("tp") == 2 * CORES and gate_weight.shape[0] == 1
    paired = paired and routing.shape[1] == 2
    if paired and experts == GROUPS * routing.shape[1]:
        return fast_body(*args)
    return body(*args)


def solution(mesh):
    placed = (
        P(("sp", "tp"), None),
        P("sp", "tp"),
        P("sp", "tp"),
        P("sp", "tp"),
        P("sp", "tp"),
        P("sp", "tp"),
        P("sp", "tp"),
        P("sp", "tp"),
        P("sp", "tp"),
        P(),
        P(),
        P(),
        P(("sp", "tp"), None),
        P(("sp", "tp"), None),
        P("sp", None, "tp"),
        P("sp", None, "tp"),
        P("sp", "tp", None),
    )
    return jax.shard_map(
        choose, mesh=mesh, in_specs=placed, out_specs=P(("sp", "tp"), None), check_vma=False
    )
```
